32 devices in a mesh: grp: 2 (over y), sp: 4 (over z), tp: 4 (over x, core).
Axes of the slice: x: 2, y: 2, z: 4, core: 2. Of those that a mesh axis runs over, the one named last changes fastest.
Arguments:
- query_rows: bfloat16 [1024, 1024], P(('grp', 'sp'), 'tp'), parts along dimension 0, may hold values from -12 to 12
- key_rows: bfloat16 [1024, 1024], P(('grp', 'sp'), 'tp'), parts along dimension 0, may hold values from -9 to 9
- value_rows: bfloat16 [1024, 1024], P(('grp', 'sp'), 'tp'), parts along dimension 0, may hold values from -6 to 6
- key_logit: bfloat16 [1024, 8], P(('grp', 'sp'), 'tp'), parts along dimension 0, as said below
- residual: bfloat16 [1024, 2048], P(('grp', 'sp')), parts along dimension 0, may hold values from -6 to 6
- out_weight: bfloat16 [1024, 2048], P('tp'), may hold values from -0.1875 to 0.1875
- mix_gain: float32 [2048], replicated, may hold values from 0.1 to 1.9
- ffn_gain: float32 [2048], replicated, may hold values from 0.1 to 1.9
- out_gain: float32 [2048], replicated, may hold values from 0.1 to 1.9
- gate_weight: bfloat16 [2048, 5120], P('sp', 'tp'), may hold values from -0.125 to 0.125
- up_weight: bfloat16 [2048, 5120], P('sp', 'tp'), may hold values from -0.125 to 0.125
- down_weight: bfloat16 [2048, 5120], P('sp', 'tp'), may hold values from -0.078125 to 0.078125
Outputs:
- layer_out: bfloat16 [1024, 2048], P(('grp', 'sp')), parts along dimension 0
The draws below stay inside these ranges and needn't reach their ends.
There are 2 independent parts, one for each index of `grp`. The reference program is written for one: setup_inputs(seed, part) draws one part's arguments, and reference() takes and returns one part's arrays. A program takes and returns all parts, laid end to end along the dimension named above; an argument that names none is the same for every part. Nothing has to cross between parts.
Inputs may be any that keep to these rules, and one draw needn't show every extreme that they name: `key_logit`: log-odds offsets of the keys, all negative.
All inputs are finite; a program needn't handle non-finite values.
Results may differ from the reference program's by a relative error of at most 0.018.
Values may be sent and summed in bfloat16 or wider, within the bound.
A program may use at most 64 MiB of HBM per device.

```python
import math
import jax
import jax.numpy as jnp
from jax import lax

D = 2048
ATTENTION_COUNT = 8
HEAD_DIM = 128
FF = 5120
TOK_DEV = 128
SEQUENCE_LENGTH = 512
HEAD_GROUP = 2
FF_GROUP = 1280
N_SP = 4
N_TP = 4


def draw_key_logit(key, part):
    flowing_entries = jax.random.split(key, 5)
    length_log = math.log(SEQUENCE_LENGTH)
    starting_shift = jax.random.uniform(flowing_entries[0], (ATTENTION_COUNT,), jnp.float32, -7.5 - length_log, -8.5)
    tile_spacing = jax.random.uniform(flowing_entries[1], (SEQUENCE_LENGTH // TOK_DEV, ATTENTION_COUNT), jnp.float32, -0.7, 0.7)
    tile_spacing = jnp.repeat(tile_spacing, TOK_DEV, axis=0)
    gaussian_perturbation = 0.3 * jax.random.normal(flowing_entries[2], (SEQUENCE_LENGTH, ATTENTION_COUNT), jnp.float32)
    spots = jax.random.randint(flowing_entries[3], (3, ATTENTION_COUNT), 0, SEQUENCE_LENGTH)
    places = jnp.arange(SEQUENCE_LENGTH, dtype=jnp.int32)[:, None, None]
    hit_entries = jnp.any(places == spots[None, :, :], axis=1)
    sudden_entries = jax.random.uniform(flowing_entries[4], (SEQUENCE_LENGTH, ATTENTION_COUNT), jnp.float32, -1.5, -0.5)
    payload_table = jnp.where(hit_entries, sudden_entries, starting_shift[None, :] + tile_spacing + gaussian_perturbation)
    return payload_table.astype(jnp.bfloat16)


def levels(own_key, shape, cuts, low, top_value):
    level, own = 1.0, jax.random.fold_in(own_key, 6)
    for dim, shards_of in cuts:
        draws = jnp.exp(jax.random.uniform(jax.random.fold_in(own, dim), (shards_of,), jnp.float32, low / len(cuts), top_value / len(cuts)))
        level = level * jnp.repeat(draws, shape[dim] // shards_of).reshape([-1 if axis == dim else 1 for axis in range(len(shape))])
    return level


def normal_values(key, dims, spread, reach, cuts=(), kind=jnp.bfloat16):
    array = spread * jax.random.normal(key, dims, jnp.float32)
    if cuts:
        array = array * levels(key, dims, cuts, -0.22, 0.18)
    return jnp.clip(array, -reach, reach).astype(kind)


def setup_inputs(seed: int = 0, part: int = 0) -> dict:
    key_list = jax.random.split(jax.random.key(seed), 13)
    part_keys = jax.random.split(jax.random.fold_in(key_list[12], part), 13)
    return {
        "query_rows": normal_values(part_keys[0], (SEQUENCE_LENGTH, ATTENTION_COUNT * HEAD_DIM), 2.0, 12.0, ((0, 4), (1, 4))),
        "key_rows": normal_values(part_keys[1], (SEQUENCE_LENGTH, ATTENTION_COUNT * HEAD_DIM), 1.5, 9.0, ((0, 4), (1, 4))),
        "value_rows": normal_values(part_keys[2], (SEQUENCE_LENGTH, ATTENTION_COUNT * HEAD_DIM), 1.0, 6.0, ((0, 4), (1, 4))),
        "key_logit": draw_key_logit(jax.random.fold_in(jax.random.fold_in(key_list[12], part), 71), part),
        "residual": normal_values(part_keys[4], (SEQUENCE_LENGTH, D), 1.0, 6.0, ((0, 4),)),
        "out_weight": normal_values(key_list[5], (ATTENTION_COUNT * HEAD_DIM, D), (ATTENTION_COUNT * HEAD_DIM) ** -0.5, 0.1875, ((0, 4),)),
        "mix_gain": jnp.clip(1.0 + 0.18 * jax.random.normal(key_list[6], (D,), jnp.float32), 0.1, 1.9),
        "ffn_gain": jnp.clip(1.0 + 0.18 * jax.random.normal(key_list[7], (D,), jnp.float32), 0.1, 1.9),
        "out_gain": jnp.clip(1.0 + 0.18 * jax.random.normal(key_list[8], (D,), jnp.float32), 0.1, 1.9),
        "gate_weight": normal_values(key_list[9], (D, FF), D ** -0.5, 0.125, ((0, 4), (1, 4))),
        "up_weight": normal_values(key_list[10], (D, FF), D ** -0.5, 0.125, ((0, 4), (1, 4))),
        "down_weight": normal_values(key_list[11], (D, FF), FF ** -0.5, 0.078125, ((0, 4), (1, 4))),
    }


epsilon = 1e-06

def normalize(payload_table):
    return payload_table * lax.rsqrt(lax.optimization_barrier(jnp.mean(payload_table * payload_table, axis=-1, keepdims=True)) + epsilon)

def block_terms(queries, key_part, value_part, logit_part, query_block, key_block):
    scores = jnp.einsum('hqd,khd->hqk', queries.astype(jnp.float32), key_part.astype(jnp.float32)) * HEAD_DIM ** (-0.5)
    scores = scores + jnp.transpose(logit_part.astype(jnp.float32))[:, None, :]
    query_pos = query_block * TOK_DEV + jnp.arange(TOK_DEV, dtype=jnp.int32)[:, None]
    key_pos = key_block * TOK_DEV + jnp.arange(TOK_DEV, dtype=jnp.int32)[None, :]
    causal = key_pos < query_pos
    keep_log = jnp.where(causal, jax.nn.log_sigmoid(-scores), 0.0)
    totals = lax.optimization_barrier(jnp.sum(keep_log, axis=2))
    within = lax.cumsum(keep_log, axis=2, reverse=True) - keep_log
    sticks = jnp.where(causal, jnp.exp(jax.nn.log_sigmoid(scores) + within), 0.0).astype(jnp.bfloat16)
    partials = jnp.einsum('hqk,khd->hqd', sticks.astype(jnp.float32), value_part.astype(jnp.float32))
    return (totals, partials)

def reference(query_rows, key_rows, value_rows, key_logit, residual, out_weight, mix_gain, ffn_gain, out_gain, gate_weight, up_weight, down_weight):

    def one_block(query_block):
        start = (query_block * TOK_DEV).astype(jnp.int32)
        queries = lax.dynamic_slice_in_dim(query_rows, start, TOK_DEV, 0).reshape(TOK_DEV, ATTENTION_COUNT, HEAD_DIM).transpose(1, 0, 2)

        def key_terms(key_block):
            key_start = (key_block * TOK_DEV).astype(jnp.int32)
            key_part = lax.dynamic_slice_in_dim(key_rows, key_start, TOK_DEV, 0).reshape(TOK_DEV, ATTENTION_COUNT, HEAD_DIM)
            value_part = lax.dynamic_slice_in_dim(value_rows, key_start, TOK_DEV, 0).reshape(TOK_DEV, ATTENTION_COUNT, HEAD_DIM)
            logit_part = lax.dynamic_slice_in_dim(key_logit, key_start, TOK_DEV, 0)

            def compute(unused):
                return block_terms(queries, key_part, value_part, logit_part, query_block, key_block)

            def skipped(unused):
                return (jnp.zeros((ATTENTION_COUNT, TOK_DEV), jnp.float32), jnp.zeros((ATTENTION_COUNT, TOK_DEV, HEAD_DIM), jnp.float32))
            return lax.cond(key_block <= query_block, compute, skipped, 0)
        totals, partials = lax.map(key_terms, jnp.arange(N_SP, dtype=jnp.int32))
        suffix = lax.cumsum(totals, axis=0, reverse=True) - totals
        attended = jnp.einsum('bhq,bhqd->qhd', jnp.exp(suffix), partials, precision=lax.Precision.HIGHEST)
        attended = attended.reshape(TOK_DEV, ATTENTION_COUNT * HEAD_DIM).astype(jnp.bfloat16)
        head_part = jnp.einsum('qgc,gcd->gqd', attended.reshape(TOK_DEV, N_TP, HEAD_GROUP * HEAD_DIM).astype(jnp.float32), out_weight.reshape(N_TP, HEAD_GROUP * HEAD_DIM, D).astype(jnp.float32)).astype(jnp.bfloat16)
        mixed_rows = lax.optimization_barrier(jnp.sum(head_part.astype(jnp.float32), axis=0)).astype(jnp.bfloat16)
        own_residual = lax.dynamic_slice_in_dim(residual, start, TOK_DEV, 0).astype(jnp.float32)
        middle = (own_residual + mix_gain * normalize(mixed_rows.astype(jnp.float32))).astype(jnp.bfloat16)
        normed = (ffn_gain * normalize(middle.astype(jnp.float32))).astype(jnp.bfloat16)
        gate_act = jnp.dot(normed, gate_weight, preferred_element_type=jnp.float32)
        up_act = jnp.dot(normed, up_weight, preferred_element_type=jnp.float32)
        hidden = (jax.nn.silu(gate_act) * up_act).astype(jnp.bfloat16)
        unit_part = jnp.einsum('qgf,dgf->gqd', hidden.reshape(TOK_DEV, N_TP, FF_GROUP).astype(jnp.float32), down_weight.reshape(D, N_TP, FF_GROUP).astype(jnp.float32)).astype(jnp.bfloat16)
        ffn_out = lax.optimization_barrier(jnp.sum(unit_part.astype(jnp.float32), axis=0)).astype(jnp.bfloat16)
        return (middle.astype(jnp.float32) + out_gain * normalize(ffn_out.astype(jnp.float32))).astype(jnp.bfloat16)
    blocks_out = lax.map(one_block, jnp.arange(N_SP, dtype=jnp.int32))
    return blocks_out.reshape(SEQUENCE_LENGTH, D)
```

```python
import functools

import jax
import jax.numpy as jnp
from jax import lax
from jax.experimental import pallas as pl
from jax.experimental.pallas import tpu as pltpu
from jax.sharding import PartitionSpec as P

epsilon = 1e-06
MESH = pl.DeviceIdType.MESH
F32 = jnp.float32
BF16 = jnp.bfloat16
LAG = 2
MOST_PIECES = 5
SPLIT_UP = 1
FIRST_DOWN = ((0, 0), (0, 1), (1, 0))


def EXTRA_ORDER(S):
    return list(range(S))


def normalize(rows):
    return rows * lax.rsqrt(jnp.mean(rows * rows, axis=-1, keepdims=True) + epsilon)


def each(count, body):
    if count <= 4:
        for i in range(count):
            body(i)
    else:

        def step(i, carry):
            body(i)
            return carry

        lax.fori_loop(0, count, step, 0)


def remote(src, dst, send, recv, axis, peer):
    return pltpu.make_async_remote_copy(
        src_ref=src,
        dst_ref=dst,
        send_sem=send,
        recv_sem=recv,
        device_id={axis: peer},
        device_id_type=MESH,
    )


def nt(a, b):
    return lax.dot_general(a, b, (((1,), (1,)), ((), ())), preferred_element_type=F32)


def kernel(
    S, TP, H, pieces,
    q, k, v, lg, mg, fg, og, res, ow, gw, uw, dw,
    out,
    kb, vb, lb, acc, run, owv, gwv, uwv, dwv, resv,
    hs, hr, mid, zs_sum, ns, na, tmp, gs, gr, hall, us, ur, zs, zr, oall,
    loc, kvs, kvr, hss, hrs, n1s, n1r, n2s, n2r, gss, grs, hars, hals, har,
    upss, upr, zss, zrs, oss, ors, outs,
):
    me, tp = lax.axis_index("sp"), lax.axis_index("tp")
    T = q.shape[0]
    hd = q.shape[1] // H
    D = out.shape[1]
    R, C = T // TP, D // S
    right, left = lax.rem(me + 1, S), lax.rem(me + S - 1, S)

    my_rows = pl.ds(pl.multiple_of(tp * R, R), R)
    loads = [
        pltpu.make_async_copy(a, b, loc.at[i])
        for i, (a, b) in enumerate(
            [(ow, owv), (res.at[my_rows], resv), (gw, gwv), (uw, uwv), (dw, dwv)]
        )
    ]
    for c in loads:
        c.start()

    barrier = pltpu.get_barrier_semaphore()
    for f in range(1, S):
        pl.semaphore_signal(barrier, inc=1, device_id={"sp": lax.rem(me + f, S)}, device_id_type=MESH)
    for f in range(1, TP):
        pl.semaphore_signal(barrier, inc=1, device_id={"tp": lax.rem(tp + f, TP)}, device_id_type=MESH)
    pl.semaphore_wait(barrier, S + TP - 2)

    def kv_copies(b, own):
        srcs = (k, v, lg) if own else (kb.at[b], vb.at[b], lb.at[b])
        return [
            remote(src, dst.at[b], kvs.at[b, i], kvr.at[b, i], "sp", right)
            for i, (src, dst) in enumerate(zip(srcs, (kb, vb, lb)))
        ]

    @pl.when(me < S - 1)
    def _():
        for c in kv_copies(me, True):
            c.start()

    rows = lax.broadcasted_iota(jnp.int32, (T, T), 0)
    cols = lax.broadcasted_iota(jnp.int32, (T, T), 1)
    causal = cols < rows
    later = (rows > cols).astype(F32)

    def block(kk, vv, ll, diag):
        for h in range(H):
            span = slice(h * hd, (h + 1) * hd)
            s = nt(q[:, span], kk[:, span]) * (hd**-0.5) + ll[h : h + 1, :]
            soft = jnp.log1p(jnp.exp(-jnp.abs(s)))
            keep = jnp.minimum(-s, 0.0) - soft
            logsig = jnp.minimum(s, 0.0) - soft
            if diag:
                keep = jnp.where(causal, keep, 0.0)
            within = jnp.dot(
                keep, later, preferred_element_type=F32, precision=lax.Precision.HIGHEST
            )
            stick = jnp.exp(logsig + within)
            if diag:
                stick = jnp.where(causal, stick, 0.0)
            part = jnp.dot(stick.astype(BF16), vv[:, span], preferred_element_type=F32)
            total = jnp.broadcast_to(jnp.sum(keep, axis=-1, keepdims=True), (T, hd))
            if diag:
                acc[h] = part
                run[h] = total
            else:
                acc[h] += jnp.exp(run[h]) * part
                run[h] += total

    block(k[...], v[...], lg[...], True)

    def earlier(i):
        b = me - 1 - i

        @pl.when(b >= 0)
        def _():
            for c in kv_copies(b, False):
                c.wait_recv()

            @pl.when(me < S - 1)
            def _():
                for c in kv_copies(b, False):
                    c.start()

            block(kb[b], vb[b], lb[b], False)

    each(S - 1, earlier)

    attended = jnp.concatenate([acc[h] for h in range(H)], axis=1).astype(BF16)
    loads[0].wait()
    width = 512 if D % 512 == 0 else D
    for c0 in range(0, D, width):
        piece = jnp.dot(attended, owv[:, c0 : c0 + width], preferred_element_type=F32)
        hs[:, :, c0 : c0 + width] = piece.astype(BF16).reshape(TP, R, width)

    def hp_copy(t, slot):
        return remote(hs.at[t], hr.at[slot], hss.at[t], hrs.at[slot], "tp", t)

    def others(count, own, body):
        def go(i):
            body(lax.rem(own + 1 + i, count))

        each(count - 1, go)

    others(TP, tp, lambda t: hp_copy(t, tp).start())
    mid[...] = hs[tp].astype(F32)

    def add_hp(t):
        hp_copy(t, t).wait_recv()
        mid[...] += hr[t].astype(F32)

    others(TP, tp, add_hp)
    loads[1].wait()
    mixed = mid[...].astype(BF16).astype(F32)
    middle = (resv[...].astype(F32) + mg[...] * normalize(mixed)).astype(BF16).astype(F32)
    mid[...] = middle
    normed = (fg[...] * normalize(middle)).astype(BF16)
    for j in range(S):
        ns[j] = normed[:, j * C : (j + 1) * C]

    def n1_copy(j, slot):
        return remote(ns.at[j], na.at[tp, slot], n1s.at[j], n1r.at[slot], "sp", j)

    def n2_copy(t, slot, s):
        return remote(na.at[tp, s], na.at[slot, s], n2s.at[t, s], n2r.at[slot, s], "tp", t)

    others(S, me, lambda j: n1_copy(j, me).start())
    na[tp, me] = ns[me]
    others(TP, tp, lambda t: n2_copy(t, tp, me).start())

    def pass_on(s):
        n1_copy(s, s).wait_recv()
        others(TP, tp, lambda t: n2_copy(t, tp, s).start())

    others(S, me, pass_on)
    for c in loads[2:4]:
        c.wait()

    def arrive(s):
        others(TP, tp, lambda t: remote(na.at[tp, s], na.at[t, s], n2s.at[t, s], n2r.at[t, s], "tp", t).wait_recv())

    W = gs.shape[-1]
    lag = LAG

    def partial(p, j):
        @pl.when(p == 0)
        def _():
            arrive(j)

        x = na[:, j].reshape(T, C)
        units = pl.ds(pl.multiple_of(p * W, W), W)
        tmp[0] = jnp.dot(x, gwv[:, units], preferred_element_type=F32)
        tmp[1] = jnp.dot(x, uwv[:, units], preferred_element_type=F32)

    def g_copy(p, j, slot, peer):
        return remote(gs.at[p, j], gr.at[p, slot], gss.at[p, j], grs.at[p, slot], "sp", peer)

    def chain(p, j, first, slot, peer):
        partial(p, j)

        @pl.when(first)
        def _():
            gs[p, j] = tmp[...].astype(BF16)

        @pl.when(jnp.logical_not(first))
        def _():
            g_copy(p, j, j, peer).wait_recv()
            gs[p, j] = (tmp[...] + gr[p, j].astype(F32)).astype(BF16)

        g_copy(p, j, slot, peer).start()

    def h_right(p, b):
        return remote(hall.at[p, b], hall.at[p, b], hars.at[p, b], har.at[p, b], "sp", right)

    def h_left(p, b):
        return remote(hall.at[p, b], hall.at[p, b], hals.at[p, b], har.at[p, b], "sp", left)

    def cut(at):
        return lax.div(at, S - 1), lax.rem(at, S - 1)

    def reduce_step(g):
        at_right = g - me * lag
        at_left = g - (S - 1 - me) * lag

        @pl.when((at_right >= 0) & (at_right < pieces * (S - 1)))
        def _():
            p, tau = cut(at_right)

            @pl.when(S - 1 - tau > me)
            def _():
                chain(p, S - 1 - tau, me == 0, S - 1 - tau, right)

        @pl.when((at_left >= 0) & (at_left < pieces * (S - 1)))
        def _():
            p, j = cut(at_left)

            @pl.when(j < me)
            def _():
                chain(p, j, me == S - 1, lax.select(j == me - 1, S, j), left)

    def finish(p):
        partial(p, me)

        @pl.when(me > 0)
        def _():
            g_copy(p, me, me, left).wait_recv()
            tmp[...] += gr[p, me].astype(F32)

        @pl.when(me < S - 1)
        def _():
            g_copy(p, me, S, right).wait_recv()
            tmp[...] += gr[p, S].astype(F32)

        gate = tmp[0]
        hall[p, me] = (gate / (1.0 + jnp.exp(-gate)) * tmp[1]).astype(BF16)

        @pl.when(me < S - 1)
        def _():
            h_right(p, me).start()

        @pl.when(me > 0)
        def _():
            h_left(p, me).start()

    def spread(p, i, then):
        lo, hi = me - 1 - i, me + 1 + i

        @pl.when(lo >= 0)
        def _():
            h_right(p, lo).wait_recv()

            @pl.when(me < S - 1)
            def _():
                h_right(p, lo).start()

            then(lo)

        @pl.when(hi < S)
        def _():
            h_left(p, hi).wait_recv()

            @pl.when(me > 0)
            def _():
                h_left(p, hi).start()

            then(hi)

    def step(g, carry):
        reduce_step(g)
        at = g - (S - 1) * lag
        p, tau = cut(at)

        @pl.when((at >= 0) & (tau == 0) & (p < pieces))
        def _():
            finish(p)

        def gather(i, carry):
            at_i = at - (i + 1) * lag
            p, tau = cut(at_i)

            @pl.when((at_i >= 0) & (tau == 0) & (p < pieces - 1))
            def _():
                spread(p, i, lambda b: None)

            return carry

        return lax.fori_loop(0, S - 1, gather, carry)

    steps = (S - 1) * (lag + max(pieces - 1, pieces - 2 + lag)) + 1
    lax.fori_loop(0, steps, step, 0)

    def up_copy(t, slot, b):
        return remote(us.at[t, b], ur.at[slot, b], upss.at[t, b], upr.at[slot, b], "tp", t)

    def down(b):
        rows_b = jnp.concatenate([hall[p, b] for p in range(pieces)], axis=1)
        us[:, b] = nt(rows_b, dwv[...]).astype(BF16).reshape(TP, R, C)
        others(TP, tp, lambda t: up_copy(t, tp, b).start())

    def z_copy(b, slot):
        return remote(zs.at[b], zr.at[slot], zss.at[b], zrs.at[slot], "sp", b)

    def settle(b):
        def add(t):
            up_copy(t, t, b).wait_recv()
            zs_sum[...] += ur[t, b].astype(F32)

        zs_sum[...] = us[tp, b].astype(F32)
        others(TP, tp, add)
        zs[b] = zs_sum[...].astype(BF16)

        @pl.when(b != me)
        def _():
            z_copy(b, me).start()

    loads[4].wait()
    down(me)

    def last(i, carry):
        spread(pieces - 1, i, down)
        return carry

    lax.fori_loop(0, S - 1, last, 0)
    others(S, me, settle)
    settle(me)
    zr[me] = zs[me]
    others(S, me, lambda s: z_copy(s, s).wait_recv())
    ffn = jnp.concatenate([zr[s] for s in range(S)], axis=1).astype(F32)
    oall[tp] = (mid[...] + og[...] * normalize(ffn)).astype(BF16)

    def o_copy(t, slot):
        return remote(oall.at[tp], oall.at[slot], oss.at[t], ors.at[slot], "tp", t)

    def o_out(t):
        return pltpu.make_async_copy(
            oall.at[t], out.at[pl.ds(pl.multiple_of(t * R, R), R)], outs.at[t]
        )

    others(TP, tp, lambda t: o_copy(t, tp).start())
    o_out(tp).start()

    def o_in(t):
        remote(oall.at[tp], oall.at[t], oss.at[t], ors.at[t], "tp", t).wait_recv()
        o_out(t).start()

    others(TP, tp, o_in)
    each(TP, lambda t: o_out(t).wait())

    @pl.when(me < S - 1)
    def _():
        def sent(b):
            @pl.when(b <= me)
            def _():
                for c in kv_copies(b, False):
                    c.wait_send()
                each(pieces, lambda p: h_right(p, b).wait_send())

        each(S, sent)

    @pl.when(me > 0)
    def _():
        def sent(b):
            @pl.when(b >= me)
            def _():
                each(pieces, lambda p: h_left(p, b).wait_send())

        each(S, sent)

    def sp_sent(j):
        n1_copy(j, me).wait_send()
        z_copy(j, me).wait_send()
        each(pieces, lambda p: g_copy(p, j, j, right).wait_send())

    others(S, me, sp_sent)

    def tp_sent(t):
        hp_copy(t, tp).wait_send()
        o_copy(t, tp).wait_send()

        def inner(s):
            n2_copy(t, tp, s).wait_send()
            up_copy(t, tp, s).wait_send()

        each(S, inner)

    others(TP, tp, tp_sent)


def gathered(
    S, TP, H, base, extras,
    q, k, v, lg, mg, fg, og, res, ow, gw, uw, dw,
    out,
    kb, vb, lb, acc, run, owv, resv, hs, hr, mid, xm, xn, gu, hid, dn, us, ur, zq, ov,
    loc, kvs, kvr, hss, hrs, azs, azr, axs, axr, acs, acr, afs, afr,
    gzs, gzr, gys, gyr, dzs, dzr, dys, dyr, hxs, hxr, hcs, hcr, hfs, hfr,
    rss, rsr, oxs, oxr, ocs, ocr, ofs, ofr, outs,
):
    me, tp, g = lax.axis_index("sp"), lax.axis_index("tp"), lax.axis_index("grp")
    T = q.shape[0]
    hd = q.shape[1] // H
    D = out.shape[1]
    R, C = T // TP, D // S
    NT = gu.shape[0]
    half, Q = C // 2, C // TP
    xpeer = lax.rem(tp + 2, TP)
    cpeer = tp + 1 - 2 * lax.rem(tp, 2)
    far = lax.rem(cpeer + 2, TP)

    def count(i):
        c = base
        for p in extras:
            c = c + jnp.where(i == p, 1, 0)
        return c

    def first(i):
        c = i * base
        for p in extras:
            c = c + jnp.where(i > p, 1, 0)
        return c

    def tiles_of(i, body):
        c = count(i)
        for m in sorted({base, base + 1} if extras else {base}):

            @pl.when(c == m)
            def _(m=m):
                body(m)

    n_me = count(me)
    my_rows = pl.ds(pl.multiple_of(tp * R, R), R)
    load_ow = pltpu.make_async_copy(ow, owv, loc.at[0])
    load_res = pltpu.make_async_copy(res.at[my_rows], resv, loc.at[1])
    load_ow.start()
    load_res.start()

    def own_gu(w, kk):
        lanes = pl.ds(pl.multiple_of((first(me) + kk) * 128, 128), 128)
        rows = pl.ds(pl.multiple_of(me * C, C), C)
        return pltpu.make_async_copy(
            (gw, uw)[w].at[:, lanes], gu.at[kk, rows, pl.ds(w * 128, 128)], loc.at[2 + w * NT + kk]
        )

    def own_dn(m):
        lanes = pl.ds(pl.multiple_of(first(me) * 128, 128), m * 128)
        rows = pl.ds(pl.multiple_of(tp * Q, Q), Q)
        to = pl.ds(pl.multiple_of(tp * (m * 128), 128), m * 128)
        return pltpu.make_async_copy(dw.at[rows, lanes], dn.at[me, :, to], loc.at[2 + 2 * NT])

    def with_tiles(body):
        for kk in range(NT):

            @pl.when(kk < n_me)
            def _(kk=kk):
                body(kk)

    def load_own(kk):
        own_gu(0, kk).start()
        own_gu(1, kk).start()

    with_tiles(load_own)
    tiles_of(me, lambda m: own_dn(m).start())

    barrier = pltpu.get_barrier_semaphore()

    def greet(i):
        for f in range(TP):

            @pl.when((i != 0) | (f != 0))
            def _(f=f):
                pl.semaphore_signal(
                    barrier,
                    inc=1,
                    device_id={"sp": lax.rem(me + i, S), "tp": lax.rem(tp + f, TP)},
                    device_id_type=MESH,
                )

    for i in range(S):
        greet(i)
    pl.semaphore_signal(barrier, inc=1, device_id={"grp": 1 - g}, device_id_type=MESH)
    pl.semaphore_wait(barrier, S * TP)

    def planes(body, up=True, down=True):
        for f in range(S - 1):
            if up:

                @pl.when(S - 1 - f > me)
                def _(f=f):
                    body(S - 1 - f)

            if down:

                @pl.when(f < me)
                def _(f=f):
                    body(f)

    def near(body):
        for d in range(1, S):

            @pl.when(me - d >= 0)
            def _(d=d):
                body(me - d)

            @pl.when(me + d < S)
            def _(d=d):
                body(me + d)

    def kv_copies(b, dst):
        return [
            remote(src, to.at[b], kvs.at[dst, i], kvr.at[b, i], "sp", dst)
            for i, (src, to) in enumerate(zip((k, v, lg), (kb, vb, lb)))
        ]

    def send_kv(i):
        for c in kv_copies(me, i):
            c.start()

    planes(send_kv, down=False)

    def gz_copy(w, i, kk, src, dst):
        lanes = pl.ds(pl.multiple_of((first(i) + kk) * 128, 128), 128)
        rows = pl.ds(pl.multiple_of(src * C + g * half, half), half)
        return remote(
            (gw, uw)[w].at[pl.ds(pl.multiple_of(g * half, half), half), lanes],
            gu.at[kk, rows, pl.ds(w * 128, 128)],
            gzs.at[w, i, kk],
            gzr.at[w, src, kk],
            "sp",
            dst,
        )

    def gy_copy(j, kk, h):
        r = gu.at[kk, pl.ds(pl.multiple_of(j * C + h * half, half), half)]
        return remote(r, r, gys.at[j, kk], gyr.at[j, kk], "grp", 1 - g)

    def send_gu(w, kk, **sides):
        def one(i):
            @pl.when(kk < count(i))
            def _():
                gz_copy(w, i, kk, me, i).start()

        planes(one, **sides)

    def dz_copy(i, t, src, st, m):
        lanes = pl.ds(pl.multiple_of(first(i) * 128, 128), m * 128)
        rows = pl.ds(pl.multiple_of(t * Q + g * (Q // 2), Q // 2), Q // 2)
        return pltpu.make_async_remote_copy(
            src_ref=dw.at[rows, lanes],
            dst_ref=dn.at[
                src,
                pl.ds(pl.multiple_of(g * (Q // 2), Q // 2), Q // 2),
                pl.ds(pl.multiple_of(st * (m * 128), 128), m * 128),
            ],
            send_sem=dzs.at[i, t],
            recv_sem=dzr.at[src, st],
            device_id={"sp": i, "tp": t},
            device_id_type=MESH,
        )

    def dp_copy(t, st, m):
        lanes = pl.ds(pl.multiple_of(first(me) * 128, 128), m * 128)
        rows = pl.ds(pl.multiple_of(t * Q, Q), Q)
        return remote(
            dw.at[rows, lanes],
            dn.at[me, :, pl.ds(pl.multiple_of(st * (m * 128), 128), m * 128)],
            dzs.at[me, t],
            dzr.at[me, st],
            "tp",
            t,
        )

    def dy_copy(j, h, m):
        r = dn.at[j, pl.ds(pl.multiple_of(h * (Q // 2), Q // 2), Q // 2), pl.ds(0, TP * m * 128)]
        return remote(r, r, dys.at[j], dyr.at[j], "grp", 1 - g)

    def peers(body):
        for f in range(1, TP):
            body(lax.rem(tp + f, TP))

    def send_dn(i):
        def some(m):
            for t in range(TP):
                dz_copy(i, t, me, tp, m).start()

        tiles_of(i, some)

    for kk in range(SPLIT_UP):
        for w in range(2):
            send_gu(w, kk, down=False)
    for kk, w in FIRST_DOWN:
        send_gu(w, kk, up=False)

    rows = lax.broadcasted_iota(jnp.int32, (T, T), 0)
    cols = lax.broadcasted_iota(jnp.int32, (T, T), 1)
    causal = cols < rows
    later = (rows > cols).astype(F32)

    def block(kk, vv, ll, diag):
        for h in range(H):
            span = slice(h * hd, (h + 1) * hd)
            s = nt(q[:, span], kk[:, span]) * (hd**-0.5) + ll[h : h + 1, :]
            soft = jnp.log1p(jnp.exp(-jnp.abs(s)))
            keep = jnp.minimum(-s, 0.0) - soft
            logsig = jnp.minimum(s, 0.0) - soft
            if diag:
                keep = jnp.where(causal, keep, 0.0)
            within = jnp.dot(
                keep, later, preferred_element_type=F32, precision=lax.Precision.HIGHEST
            )
            stick = jnp.exp(logsig + within)
            if diag:
                stick = jnp.where(causal, stick, 0.0)
            part = jnp.dot(stick.astype(BF16), vv[:, span], preferred_element_type=F32)
            total = jnp.broadcast_to(jnp.sum(keep, axis=-1, keepdims=True), (T, hd))
            if diag:
                acc[h] = part
                run[h] = total
            else:
                acc[h] += jnp.exp(run[h]) * part
                run[h] += total

    block(k[...], v[...], lg[...], True)

    def earlier(i):
        b = me - 1 - i

        @pl.when(b >= 0)
        def _():
            for c in kv_copies(b, me):
                c.wait_recv()
            block(kb[b], vb[b], lb[b], False)

    each(S - 1, earlier)

    attended = jnp.concatenate([acc[h] for h in range(H)], axis=1).astype(BF16)
    load_ow.wait()
    width = 512 if D % 512 == 0 else D
    for c0 in range(0, D, width):
        piece = jnp.dot(attended, owv[:, c0 : c0 + width], preferred_element_type=F32)
        hs[:, :, c0 : c0 + width] = piece.astype(BF16).reshape(TP, R, width)

    def hp_copy(t, slot):
        return remote(hs.at[t], hr.at[slot], hss.at[t], hrs.at[slot], "tp", t)

    peers(lambda t: hp_copy(t, tp).start())
    mid[...] = hs[tp].astype(F32)

    def add_hp(t):
        hp_copy(t, t).wait_recv()
        mid[...] += hr[t].astype(F32)

    peers(add_hp)
    load_res.wait()
    mixed = mid[...].astype(BF16).astype(F32)
    xm[me, my_rows] = (resv[...].astype(F32) + mg[...] * normalize(mixed)).astype(BF16)

    def piece_of(j, t):
        return xm.at[j, pl.ds(pl.multiple_of(t * R, R), R)]

    def az_copy(j, dst):
        return remote(piece_of(j, tp), piece_of(j, tp), azs.at[dst], azr.at[j], "sp", dst)

    def ax_copy(j, t):
        return remote(piece_of(j, t), piece_of(j, t), axs.at[j], axr.at[j], "tp", xpeer)

    def ac_copy(j, t):
        return remote(piece_of(j, t), piece_of(j, t), acs.at[j], acr.at[j], "tp", cpeer)

    def af_copy(j, t):
        return remote(piece_of(j, t), piece_of(j, t), afs.at[j], afr.at[j], "tp", cpeer)

    planes(lambda i: az_copy(me, i).start())
    ax_copy(me, tp).start()
    ac_copy(me, tp).start()

    for kk in range(NT):
        for w in range(2):
            if kk >= SPLIT_UP:
                send_gu(w, kk, down=False)
            if (kk, w) not in FIRST_DOWN:
                send_gu(w, kk, up=False)
    planes(send_dn)
    tiles_of(me, lambda m: peers(lambda t: dp_copy(t, tp, m).start()))

    def pass_gu(kk):
        def one(j):
            gz_copy(0, me, kk, j, j).wait_recv()
            gz_copy(1, me, kk, j, j).wait_recv()
            gy_copy(j, kk, g).start()

        planes(one)

    def spread(j):
        az_copy(j, j).wait_recv()
        ax_copy(j, tp).start()
        ac_copy(j, tp).start()

    def hand_on(j):
        ax_copy(j, xpeer).wait_recv()
        af_copy(j, xpeer).start()

    def ready(j):
        ac_copy(j, cpeer).wait_recv()
        af_copy(j, far).wait_recv()
        for r0 in range(0, T, R):
            rows_f = xm[j, pl.ds(r0, R)].astype(F32)
            at = pl.ds(pl.multiple_of(j * T + r0, R), R)
            xn[at] = (fg[...] * normalize(rows_f)).astype(BF16)

    pass_gu(0)
    hand_on(me)
    near(spread)
    near(hand_on)
    ready(me)
    near(ready)

    def hid_at(t, kk):
        return hid.at[t * NT + kk]

    def hx_copy(t, kk):
        return remote(hid_at(t, kk), hid_at(t, kk), hxs.at[kk], hxr.at[kk], "tp", xpeer)

    def hc_copy(t, kk):
        return remote(hid_at(t, kk), hid_at(t, kk), hcs.at[kk], hcr.at[kk], "tp", cpeer)

    def hf_copy(t, kk):
        return remote(hid_at(t, kk), hid_at(t, kk), hfs.at[kk], hfr.at[kk], "tp", cpeer)

    def tile(kk):
        if kk > 0:
            pass_gu(kk)
        own_gu(0, kk).wait()
        own_gu(1, kk).wait()
        planes(lambda j: gy_copy(j, kk, 1 - g).wait_recv())
        both = jnp.dot(xn[...], gu[kk], preferred_element_type=F32)
        gate, up = both[:, :128], both[:, 128:]
        hid[tp * NT + kk] = (gate / (1.0 + jnp.exp(-gate)) * up).astype(BF16)
        hx_copy(tp, kk).start()
        hc_copy(tp, kk).start()

    with_tiles(tile)

    def pass_tile(kk):
        hx_copy(xpeer, kk).wait_recv()
        hf_copy(xpeer, kk).start()

    with_tiles(pass_tile)

    def pass_dn(j):
        def some(m):
            for st in range(TP):
                dz_copy(me, tp, j, st, m).wait_recv()
            dy_copy(j, g, m).start()

        tiles_of(me, some)

    near(pass_dn)

    def hid_ready(kk):
        hc_copy(cpeer, kk).wait_recv()
        hf_copy(far, kk).wait_recv()

    with_tiles(hid_ready)

    def rs_copy(j, dst, src):
        return remote(us.at[j, dst], ur.at[j, src], rss.at[j, dst], rsr.at[j, src], "sp", dst)

    def down(j, own=False):
        def some(m):
            if own:
                own_dn(m).wait()
                peers(lambda t: dp_copy(tp, t, m).wait_recv())
            else:
                dy_copy(j, 1 - g, m).wait_recv()
            x = jnp.concatenate(
                [hid[t * NT + kk] for t in range(TP) for kk in range(m)], axis=1
            )
            us[j] = nt(x, dn[j, :, : TP * m * 128]).astype(BF16).reshape(S, T, Q)

        tiles_of(me, some)
        planes(lambda i: rs_copy(j, i, me).start())

    down(me, True)
    near(down)

    def ox_copy(j, t):
        return remote(zq.at[t, j], zq.at[t, j], oxs.at[j], oxr.at[j], "tp", xpeer)

    def oc_copy(j, t):
        return remote(zq.at[t, j], zq.at[t, j], ocs.at[j], ocr.at[j], "tp", cpeer)

    def of_copy(j, t):
        return remote(zq.at[t, j], zq.at[t, j], ofs.at[j], ofr.at[j], "tp", cpeer)

    def settle(j):
        planes(lambda i: rs_copy(j, i, i).wait_recv())
        total = us[j, me].astype(F32)
        for d in range(1, S):
            total += ur[j, lax.rem(me + d, S)].astype(F32)
        zq[tp, j] = total.astype(BF16)
        ox_copy(j, tp).start()
        oc_copy(j, tp).start()

    for j in range(S):
        settle(j)
    for j in range(S):
        ox_copy(j, xpeer).wait_recv()
        of_copy(j, xpeer).start()
    for j in range(S):
        oc_copy(j, cpeer).wait_recv()
        of_copy(j, far).wait_recv()

    def o_out(r):
        rows_r = pl.ds(r * R, R)
        return pltpu.make_async_copy(ov.at[rows_r], out.at[rows_r], outs.at[r])

    for r in range(TP):
        rows_r = pl.ds(r * R, R)
        ffn = jnp.concatenate(
            [zq[t, j, rows_r] for j in range(S) for t in range(TP)], axis=1
        ).astype(F32)
        ov[rows_r] = (xm[me, rows_r].astype(F32) + og[...] * normalize(ffn)).astype(BF16)
        o_out(r).start()

    planes(lambda i: [c.wait_send() for c in kv_copies(me, i)], down=False)
    peers(lambda t: hp_copy(t, tp).wait_send())
    for j in range(S):
        ax_copy(j, tp).wait_send()
        ac_copy(j, tp).wait_send()
        af_copy(j, xpeer).wait_send()
        ox_copy(j, tp).wait_send()
        oc_copy(j, tp).wait_send()
        of_copy(j, xpeer).wait_send()
        planes(lambda i: rs_copy(j, i, me).wait_send())

    def sent(i):
        az_copy(me, i).wait_send()
        for kk in range(NT):
            for w in range(2):

                @pl.when(kk < count(i))
                def _(kk=kk, w=w):
                    gz_copy(w, i, kk, me, i).wait_send()

        def some(m):
            for t in range(TP):
                dz_copy(i, t, me, tp, m).wait_send()

        tiles_of(i, some)
        tiles_of(me, lambda m: dy_copy(i, g, m).wait_send())

    planes(sent)

    def tile_sent(kk):
        planes(lambda j: gy_copy(j, kk, g).wait_send())
        hx_copy(tp, kk).wait_send()
        hc_copy(tp, kk).wait_send()
        hf_copy(xpeer, kk).wait_send()

    with_tiles(tile_sent)
    tiles_of(me, lambda m: peers(lambda t: dp_copy(t, tp, m).wait_send()))
    for r in range(TP):
        o_out(r).wait()


def gathered_call(S, TP, q, k, v, lgt, H, mg, fg, og, res, ow, gw, uw, dw):
    T, hw = q.shape
    D = res.shape[1]
    C, U = gw.shape
    R, Q = T // TP, C // TP
    base, extra = divmod(U // 128, S)
    extras = EXTRA_ORDER(S)[:extra]
    NT = base + (1 if extra else 0)
    vm = pl.BlockSpec(memory_space=pltpu.VMEM)
    hb = pl.BlockSpec(memory_space=pl.ANY)
    dma = pltpu.SemaphoreType.DMA
    pairs = lambda *shape: [dma(shape), dma(shape)]
    return pl.pallas_call(
        functools.partial(gathered, S, TP, H, base, extras),
        out_shape=jax.ShapeDtypeStruct((T, D), BF16),
        in_specs=[vm] * 7 + [hb] * 5,
        out_specs=hb,
        scratch_shapes=[
            pltpu.VMEM((S, T, hw), BF16),
            pltpu.VMEM((S, T, hw), BF16),
            pltpu.VMEM((S,) + lgt.shape, F32),
            pltpu.VMEM((H, T, hw // H), F32),
            pltpu.VMEM((H, T, hw // H), F32),
            pltpu.VMEM(ow.shape, BF16),
            pltpu.VMEM((R, D), BF16),
            pltpu.VMEM((TP, R, D), BF16),
            pltpu.VMEM((TP, R, D), BF16),
            pltpu.VMEM((R, D), F32),
            pltpu.VMEM((S, T, D), BF16),
            pltpu.VMEM((S * T, D), BF16),
            pltpu.VMEM((NT, D, 256), BF16),
            pltpu.VMEM((TP * NT, S * T, 128), BF16),
            pltpu.VMEM((S, Q, TP * NT * 128), BF16),
            pltpu.VMEM((S, S, T, Q), BF16),
            pltpu.VMEM((S, S, T, Q), BF16),
            pltpu.VMEM((TP, S, T, Q), BF16),
            pltpu.VMEM((T, D), BF16),
            dma((3 + 2 * NT,)),
            *pairs(S, 3),
            *pairs(TP),
            *pairs(S),
            *pairs(S),
            *pairs(S),
            *pairs(S),
            *pairs(2, S, NT),
            *pairs(S, NT),
            *pairs(S, TP),
            *pairs(S),
            *pairs(NT),
            *pairs(NT),
            *pairs(NT),
            *pairs(S, S),
            *pairs(S),
            *pairs(S),
            *pairs(S),
            dma((TP,)),
        ],
        compiler_params=pltpu.CompilerParams(
            collective_id=0, has_side_effects=True, vmem_limit_bytes=67043328 - 2**20
        ),
    )(q, k, v, lgt, mg[None], fg[None], og[None], res, ow, gw, uw, dw)


def solution(mesh):
    S, TP, G = mesh.shape["sp"], mesh.shape["tp"], mesh.shape["grp"]

    def shards(q, k, v, lg, res, ow, mg, fg, og, gw, uw, dw):
        T, H = lg.shape
        hw = q.shape[1]
        D = res.shape[1]
        C, U = gw.shape
        R = T // TP
        pieces = max([p for p in range(1, MOST_PIECES + 1) if U % (128 * p) == 0], default=1)
        W = U // pieces
        pad = -H % 8
        lgt = jnp.pad(lg.astype(F32).T, ((0, pad), (0, 0)))
        if U % 128 == 0 and U // 128 >= S and C % (128 * TP) == 0 and T % (16 * TP) == 0 and (TP, G) == (4, 2):
            return gathered_call(S, TP, q, k, v, lgt, H, mg, fg, og, res, ow, gw, uw, dw)
        vm = pl.BlockSpec(memory_space=pltpu.VMEM)
        hb = pl.BlockSpec(memory_space=pl.ANY)
        dma = pltpu.SemaphoreType.DMA
        return pl.pallas_call(
            functools.partial(kernel, S, TP, H, pieces),
            out_shape=jax.ShapeDtypeStruct((T, D), BF16),
            in_specs=[vm] * 7 + [hb] * 5,
            out_specs=hb,
            scratch_shapes=[
                pltpu.VMEM((S, T, hw), BF16),
                pltpu.VMEM((S, T, hw), BF16),
                pltpu.VMEM((S,) + lgt.shape, F32),
                pltpu.VMEM((H, T, hw // H), F32),
                pltpu.VMEM((H, T, hw // H), F32),
                pltpu.VMEM(ow.shape, BF16),
                pltpu.VMEM(gw.shape, BF16),
                pltpu.VMEM(uw.shape, BF16),
                pltpu.VMEM(dw.shape, BF16),
                pltpu.VMEM((R, D), BF16),
                pltpu.VMEM((TP, R, D), BF16),
                pltpu.VMEM((TP, R, D), BF16),
                pltpu.VMEM((R, D), F32),
                pltpu.VMEM((R, C), F32),
                pltpu.VMEM((S, R, C), BF16),
                pltpu.VMEM((TP, S, R, C), BF16),
                pltpu.VMEM((2, T, W), F32),
                pltpu.VMEM((pieces, S, 2, T, W), BF16),
                pltpu.VMEM((pieces, S + 1, 2, T, W), BF16),
                pltpu.VMEM((pieces, S, T, W), BF16),
                pltpu.VMEM((TP, S, R, C), BF16),
                pltpu.VMEM((TP, S, R, C), BF16),
                pltpu.VMEM((S, R, C), BF16),
                pltpu.VMEM((S, R, C), BF16),
                pltpu.VMEM((TP, R, D), BF16),
                dma((5,)),
                dma((S, 3)),
                dma((S, 3)),
                dma((TP,)),
                dma((TP,)),
                dma((S,)),
                dma((S,)),
                dma((TP, S)),
                dma((TP, S)),
                dma((pieces, S)),
                dma((pieces, S + 1)),
                dma((pieces, S)),
                dma((pieces, S)),
                dma((pieces, S)),
                dma((TP, S)),
                dma((TP, S)),
                dma((S,)),
                dma((S,)),
                dma((TP,)),
                dma((TP,)),
                dma((TP,)),
            ],
            compiler_params=pltpu.CompilerParams(
                collective_id=0, has_side_effects=True, vmem_limit_bytes=67043328 - 2**20
            ),
        )(q, k, v, lgt, mg[None], fg[None], og[None], res, ow, gw, uw, dw)

    placed = (
        P(("grp", "sp"), "tp"),
        P(("grp", "sp"), "tp"),
        P(("grp", "sp"), "tp"),
        P(("grp", "sp"), "tp"),
        P(("grp", "sp"), None),
        P("tp", None),
        P(),
        P(),
        P(),
        P("sp", "tp"),
        P("sp", "tp"),
        P("sp", "tp"),
    )
    return jax.shard_map(
        shards, mesh=mesh, in_specs=placed, out_specs=P(("grp", "sp"), None), check_vma=False
    )
```

```python
import functools

import jax
import jax.numpy as jnp
from jax import lax
from jax.experimental import pallas as pl
from jax.experimental.pallas import tpu as pltpu
from jax.sharding import PartitionSpec as P

epsilon = 1e-06
MESH = pl.DeviceIdType.MESH
F32 = jnp.float32
BF16 = jnp.bfloat16
LAG = 2
MOST_PIECES = 5
EARLY = 2


def EXTRA_ORDER(S):
    return list(range(S))


def normalize(rows):
    return rows * lax.rsqrt(jnp.mean(rows * rows, axis=-1, keepdims=True) + epsilon)


def each(count, body):
    if count <= 4:
        for i in range(count):
            body(i)
    else:

        def step(i, carry):
            body(i)
            return carry

        lax.fori_loop(0, count, step, 0)


def remote(src, dst, send, recv, axis, peer):
    return pltpu.make_async_remote_copy(
        src_ref=src,
        dst_ref=dst,
        send_sem=send,
        recv_sem=recv,
        device_id={axis: peer},
        device_id_type=MESH,
    )


def nt(a, b):
    return lax.dot_general(a, b, (((1,), (1,)), ((), ())), preferred_element_type=F32)


def kernel(
    S, TP, H, pieces,
    q, k, v, lg, mg, fg, og, res, ow, gw, uw, dw,
    out,
    kb, vb, lb, acc, run, owv, gwv, uwv, dwv, resv,
    hs, hr, mid, zs_sum, ns, na, tmp, gs, gr, hall, us, ur, zs, zr, oall,
    loc, kvs, kvr, hss, hrs, n1s, n1r, n2s, n2r, gss, grs, hars, hals, har,
    upss, upr, zss, zrs, oss, ors, outs,
):
    me, tp = lax.axis_index("sp"), lax.axis_index("tp")
    T = q.shape[0]
    hd = q.shape[1] // H
    D = out.shape[1]
    R, C = T // TP, D // S
    right, left = lax.rem(me + 1, S), lax.rem(me + S - 1, S)

    my_rows = pl.ds(pl.multiple_of(tp * R, R), R)
    loads = [
        pltpu.make_async_copy(a, b, loc.at[i])
        for i, (a, b) in enumerate(
            [(ow, owv), (res.at[my_rows], resv), (gw, gwv), (uw, uwv), (dw, dwv)]
        )
    ]
    for c in loads:
        c.start()

    barrier = pltpu.get_barrier_semaphore()
    for f in range(1, S):
        pl.semaphore_signal(barrier, inc=1, device_id={"sp": lax.rem(me + f, S)}, device_id_type=MESH)
    for f in range(1, TP):
        pl.semaphore_signal(barrier, inc=1, device_id={"tp": lax.rem(tp + f, TP)}, device_id_type=MESH)
    pl.semaphore_wait(barrier, S + TP - 2)

    def kv_copies(b, own):
        srcs = (k, v, lg) if own else (kb.at[b], vb.at[b], lb.at[b])
        return [
            remote(src, dst.at[b], kvs.at[b, i], kvr.at[b, i], "sp", right)
            for i, (src, dst) in enumerate(zip(srcs, (kb, vb, lb)))
        ]

    @pl.when(me < S - 1)
    def _():
        for c in kv_copies(me, True):
            c.start()

    rows = lax.broadcasted_iota(jnp.int32, (T, T), 0)
    cols = lax.broadcasted_iota(jnp.int32, (T, T), 1)
    causal = cols < rows
    later = (rows > cols).astype(F32)

    def block(kk, vv, ll, diag):
        for h in range(H):
            span = slice(h * hd, (h + 1) * hd)
            s = nt(q[:, span], kk[:, span]) * (hd**-0.5) + ll[h : h + 1, :]
            soft = jnp.log1p(jnp.exp(-jnp.abs(s)))
            keep = jnp.minimum(-s, 0.0) - soft
            logsig = jnp.minimum(s, 0.0) - soft
            if diag:
                keep = jnp.where(causal, keep, 0.0)
            within = jnp.dot(
                keep, later, preferred_element_type=F32, precision=lax.Precision.HIGHEST
            )
            stick = jnp.exp(logsig + within)
            if diag:
                stick = jnp.where(causal, stick, 0.0)
            part = jnp.dot(stick.astype(BF16), vv[:, span], preferred_element_type=F32)
            total = jnp.broadcast_to(jnp.sum(keep, axis=-1, keepdims=True), (T, hd))
            if diag:
                acc[h] = part
                run[h] = total
            else:
                acc[h] += jnp.exp(run[h]) * part
                run[h] += total

    block(k[...], v[...], lg[...], True)

    def earlier(i):
        b = me - 1 - i

        @pl.when(b >= 0)
        def _():
            for c in kv_copies(b, False):
                c.wait_recv()

            @pl.when(me < S - 1)
            def _():
                for c in kv_copies(b, False):
                    c.start()

            block(kb[b], vb[b], lb[b], False)

    each(S - 1, earlier)

    attended = jnp.concatenate([acc[h] for h in range(H)], axis=1).astype(BF16)
    loads[0].wait()
    width = 512 if D % 512 == 0 else D
    for c0 in range(0, D, width):
        piece = jnp.dot(attended, owv[:, c0 : c0 + width], preferred_element_type=F32)
        hs[:, :, c0 : c0 + width] = piece.astype(BF16).reshape(TP, R, width)

    def hp_copy(t, slot):
        return remote(hs.at[t], hr.at[slot], hss.at[t], hrs.at[slot], "tp", t)

    def others(count, own, body):
        def go(i):
            body(lax.rem(own + 1 + i, count))

        each(count - 1, go)

    others(TP, tp, lambda t: hp_copy(t, tp).start())
    mid[...] = hs[tp].astype(F32)

    def add_hp(t):
        hp_copy(t, t).wait_recv()
        mid[...] += hr[t].astype(F32)

    others(TP, tp, add_hp)
    loads[1].wait()
    mixed = mid[...].astype(BF16).astype(F32)
    middle = (resv[...].astype(F32) + mg[...] * normalize(mixed)).astype(BF16).astype(F32)
    mid[...] = middle
    normed = (fg[...] * normalize(middle)).astype(BF16)
    for j in range(S):
        ns[j] = normed[:, j * C : (j + 1) * C]

    def n1_copy(j, slot):
        return remote(ns.at[j], na.at[tp, slot], n1s.at[j], n1r.at[slot], "sp", j)

    def n2_copy(t, slot, s):
        return remote(na.at[tp, s], na.at[slot, s], n2s.at[t, s], n2r.at[slot, s], "tp", t)

    others(S, me, lambda j: n1_copy(j, me).start())
    na[tp, me] = ns[me]
    others(TP, tp, lambda t: n2_copy(t, tp, me).start())

    def pass_on(s):
        n1_copy(s, s).wait_recv()
        others(TP, tp, lambda t: n2_copy(t, tp, s).start())

    others(S, me, pass_on)
    for c in loads[2:4]:
        c.wait()

    def arrive(s):
        others(TP, tp, lambda t: remote(na.at[tp, s], na.at[t, s], n2s.at[t, s], n2r.at[t, s], "tp", t).wait_recv())

    W = gs.shape[-1]
    lag = LAG

    def partial(p, j):
        @pl.when(p == 0)
        def _():
            arrive(j)

        x = na[:, j].reshape(T, C)
        units = pl.ds(pl.multiple_of(p * W, W), W)
        tmp[0] = jnp.dot(x, gwv[:, units], preferred_element_type=F32)
        tmp[1] = jnp.dot(x, uwv[:, units], preferred_element_type=F32)

    def g_copy(p, j, slot, peer):
        return remote(gs.at[p, j], gr.at[p, slot], gss.at[p, j], grs.at[p, slot], "sp", peer)

    def chain(p, j, first, slot, peer):
        partial(p, j)

        @pl.when(first)
        def _():
            gs[p, j] = tmp[...].astype(BF16)

        @pl.when(jnp.logical_not(first))
        def _():
            g_copy(p, j, j, peer).wait_recv()
            gs[p, j] = (tmp[...] + gr[p, j].astype(F32)).astype(BF16)

        g_copy(p, j, slot, peer).start()

    def h_right(p, b):
        return remote(hall.at[p, b], hall.at[p, b], hars.at[p, b], har.at[p, b], "sp", right)

    def h_left(p, b):
        return remote(hall.at[p, b], hall.at[p, b], hals.at[p, b], har.at[p, b], "sp", left)

    def cut(at):
        return lax.div(at, S - 1), lax.rem(at, S - 1)

    def reduce_step(g):
        at_right = g - me * lag
        at_left = g - (S - 1 - me) * lag

        @pl.when((at_right >= 0) & (at_right < pieces * (S - 1)))
        def _():
            p, tau = cut(at_right)

            @pl.when(S - 1 - tau > me)
            def _():
                chain(p, S - 1 - tau, me == 0, S - 1 - tau, right)

        @pl.when((at_left >= 0) & (at_left < pieces * (S - 1)))
        def _():
            p, j = cut(at_left)

            @pl.when(j < me)
            def _():
                chain(p, j, me == S - 1, lax.select(j == me - 1, S, j), left)

    def finish(p):
        partial(p, me)

        @pl.when(me > 0)
        def _():
            g_copy(p, me, me, left).wait_recv()
            tmp[...] += gr[p, me].astype(F32)

        @pl.when(me < S - 1)
        def _():
            g_copy(p, me, S, right).wait_recv()
            tmp[...] += gr[p, S].astype(F32)

        gate = tmp[0]
        hall[p, me] = (gate / (1.0 + jnp.exp(-gate)) * tmp[1]).astype(BF16)

        @pl.when(me < S - 1)
        def _():
            h_right(p, me).start()

        @pl.when(me > 0)
        def _():
            h_left(p, me).start()

    def spread(p, i, then):
        lo, hi = me - 1 - i, me + 1 + i

        @pl.when(lo >= 0)
        def _():
            h_right(p, lo).wait_recv()

            @pl.when(me < S - 1)
            def _():
                h_right(p, lo).start()

            then(lo)

        @pl.when(hi < S)
        def _():
            h_left(p, hi).wait_recv()

            @pl.when(me > 0)
            def _():
                h_left(p, hi).start()

            then(hi)

    def step(g, carry):
        reduce_step(g)
        at = g - (S - 1) * lag
        p, tau = cut(at)

        @pl.when((at >= 0) & (tau == 0) & (p < pieces))
        def _():
            finish(p)

        def gather(i, carry):
            at_i = at - (i + 1) * lag
            p, tau = cut(at_i)

            @pl.when((at_i >= 0) & (tau == 0) & (p < pieces - 1))
            def _():
                spread(p, i, lambda b: None)

            return carry

        return lax.fori_loop(0, S - 1, gather, carry)

    steps = (S - 1) * (lag + max(pieces - 1, pieces - 2 + lag)) + 1
    lax.fori_loop(0, steps, step, 0)

    def up_copy(t, slot, b):
        return remote(us.at[t, b], ur.at[slot, b], upss.at[t, b], upr.at[slot, b], "tp", t)

    def down(b):
        rows_b = jnp.concatenate([hall[p, b] for p in range(pieces)], axis=1)
        us[:, b] = nt(rows_b, dwv[...]).astype(BF16).reshape(TP, R, C)
        others(TP, tp, lambda t: up_copy(t, tp, b).start())

    def z_copy(b, slot):
        return remote(zs.at[b], zr.at[slot], zss.at[b], zrs.at[slot], "sp", b)

    def settle(b):
        def add(t):
            up_copy(t, t, b).wait_recv()
            zs_sum[...] += ur[t, b].astype(F32)

        zs_sum[...] = us[tp, b].astype(F32)
        others(TP, tp, add)
        zs[b] = zs_sum[...].astype(BF16)

        @pl.when(b != me)
        def _():
            z_copy(b, me).start()

    loads[4].wait()
    down(me)

    def last(i, carry):
        spread(pieces - 1, i, down)
        return carry

    lax.fori_loop(0, S - 1, last, 0)
    others(S, me, settle)
    settle(me)
    zr[me] = zs[me]
    others(S, me, lambda s: z_copy(s, s).wait_recv())
    ffn = jnp.concatenate([zr[s] for s in range(S)], axis=1).astype(F32)
    oall[tp] = (mid[...] + og[...] * normalize(ffn)).astype(BF16)

    def o_copy(t, slot):
        return remote(oall.at[tp], oall.at[slot], oss.at[t], ors.at[slot], "tp", t)

    def o_out(t):
        return pltpu.make_async_copy(
            oall.at[t], out.at[pl.ds(pl.multiple_of(t * R, R), R)], outs.at[t]
        )

    others(TP, tp, lambda t: o_copy(t, tp).start())
    o_out(tp).start()

    def o_in(t):
        remote(oall.at[tp], oall.at[t], oss.at[t], ors.at[t], "tp", t).wait_recv()
        o_out(t).start()

    others(TP, tp, o_in)
    each(TP, lambda t: o_out(t).wait())

    @pl.when(me < S - 1)
    def _():
        def sent(b):
            @pl.when(b <= me)
            def _():
                for c in kv_copies(b, False):
                    c.wait_send()
                each(pieces, lambda p: h_right(p, b).wait_send())

        each(S, sent)

    @pl.when(me > 0)
    def _():
        def sent(b):
            @pl.when(b >= me)
            def _():
                each(pieces, lambda p: h_left(p, b).wait_send())

        each(S, sent)

    def sp_sent(j):
        n1_copy(j, me).wait_send()
        z_copy(j, me).wait_send()
        each(pieces, lambda p: g_copy(p, j, j, right).wait_send())

    others(S, me, sp_sent)

    def tp_sent(t):
        hp_copy(t, tp).wait_send()
        o_copy(t, tp).wait_send()

        def inner(s):
            n2_copy(t, tp, s).wait_send()
            up_copy(t, tp, s).wait_send()

        each(S, inner)

    others(TP, tp, tp_sent)


def gathered(
    S, TP, H, base, extras,
    q, k, v, lg, mg, fg, og, res, ow, gw, uw, dw,
    out,
    kb, vb, lb, acc, run, owv, resv, hs, hr, mid, xm, xn, gu, hid, dn, us, ur, zq, ov,
    loc, kvs, kvr, hss, hrs, azs, azr, axs, axr, acs, acr, afs, afr,
    gzs, gzr, gys, gyr, dzs, dzr, dys, dyr, hxs, hxr, hcs, hcr, hfs, hfr,
    rss, rsr, oxs, oxr, ocs, ocr, ofs, ofr, outs,
):
    me, tp, g = lax.axis_index("sp"), lax.axis_index("tp"), lax.axis_index("grp")
    T = q.shape[0]
    hd = q.shape[1] // H
    D = out.shape[1]
    R, C = T // TP, D // S
    NT = gu.shape[0]
    half, Q = C // 2, C // TP
    xpeer = lax.rem(tp + 2, TP)
    cpeer = tp + 1 - 2 * lax.rem(tp, 2)
    far = lax.rem(cpeer + 2, TP)

    def count(i):
        c = base
        for p in extras:
            c = c + jnp.where(i == p, 1, 0)
        return c

    def first(i):
        c = i * base
        for p in extras:
            c = c + jnp.where(i > p, 1, 0)
        return c

    def tiles_of(i, body):
        c = count(i)
        for m in sorted({base, base + 1} if extras else {base}):

            @pl.when(c == m)
            def _(m=m):
                body(m)

    n_me = count(me)
    my_rows = pl.ds(pl.multiple_of(tp * R, R), R)
    load_ow = pltpu.make_async_copy(ow, owv, loc.at[0])
    load_res = pltpu.make_async_copy(res.at[my_rows], resv, loc.at[1])
    load_ow.start()
    load_res.start()

    def own_gu(w, kk):
        lanes = pl.ds(pl.multiple_of((first(me) + kk) * 128, 128), 128)
        rows = pl.ds(pl.multiple_of(me * C, C), C)
        return pltpu.make_async_copy(
            (gw, uw)[w].at[:, lanes], gu.at[kk, rows, pl.ds(w * 128, 128)], loc.at[2 + w * NT + kk]
        )

    def own_dn(m):
        lanes = pl.ds(pl.multiple_of(first(me) * 128, 128), m * 128)
        rows = pl.ds(pl.multiple_of(tp * Q, Q), Q)
        to = pl.ds(pl.multiple_of(tp * (m * 128), 128), m * 128)
        return pltpu.make_async_copy(dw.at[rows, lanes], dn.at[me, :, to], loc.at[2 + 2 * NT])

    def with_tiles(body, at=range(NT)):
        for kk in at:

            @pl.when(kk < n_me)
            def _(kk=kk):
                body(kk)

    def load_own(kk):
        own_gu(0, kk).start()
        own_gu(1, kk).start()

    with_tiles(load_own)
    tiles_of(me, lambda m: own_dn(m).start())

    barrier = pltpu.get_barrier_semaphore()

    def greet(i):
        for f in range(TP):

            @pl.when((i != 0) | (f != 0))
            def _(f=f):
                pl.semaphore_signal(
                    barrier,
                    inc=1,
                    device_id={"sp": lax.rem(me + i, S), "tp": lax.rem(tp + f, TP)},
                    device_id_type=MESH,
                )

    for i in range(S):
        greet(i)
    pl.semaphore_signal(barrier, inc=1, device_id={"grp": 1 - g}, device_id_type=MESH)
    pl.semaphore_wait(barrier, S * TP)

    def planes(body, up=True, down=True, at=range(1, S)):
        for d in at:
            if down:

                @pl.when(me - d >= 0)
                def _(d=d):
                    body(me - d)

            if up:

                @pl.when(me + d < S)
                def _(d=d):
                    body(me + d)

    def kv_copies(b, dst):
        return [
            remote(src, to.at[b], kvs.at[dst, i], kvr.at[b, i], "sp", dst)
            for i, (src, to) in enumerate(zip((k, v, lg), (kb, vb, lb)))
        ]

    def send_kv(i):
        for c in kv_copies(me, i):
            c.start()

    planes(send_kv, down=False)

    def gz_copy(w, i, kk, src, dst):
        lanes = pl.ds(pl.multiple_of((first(i) + kk) * 128, 128), 128)
        rows = pl.ds(pl.multiple_of(src * C + g * half, half), half)
        return remote(
            (gw, uw)[w].at[pl.ds(pl.multiple_of(g * half, half), half), lanes],
            gu.at[kk, rows, pl.ds(w * 128, 128)],
            gzs.at[w, i, kk],
            gzr.at[w, src, kk],
            "sp",
            dst,
        )

    def gy_copy(j, kk, h):
        r = gu.at[kk, pl.ds(pl.multiple_of(j * C + h * half, half), half)]
        return remote(r, r, gys.at[j, kk], gyr.at[j, kk], "grp", 1 - g)

    def send_gu(w, kk, **sides):
        def one(i):
            @pl.when(kk < count(i))
            def _():
                gz_copy(w, i, kk, me, i).start()

        planes(one, **sides)

    def dz_copy(i, t, src, st, m):
        lanes = pl.ds(pl.multiple_of(first(i) * 128, 128), m * 128)
        rows = pl.ds(pl.multiple_of(t * Q + g * (Q // 2), Q // 2), Q // 2)
        return pltpu.make_async_remote_copy(
            src_ref=dw.at[rows, lanes],
            dst_ref=dn.at[
                src,
                pl.ds(pl.multiple_of(g * (Q // 2), Q // 2), Q // 2),
                pl.ds(pl.multiple_of(st * (m * 128), 128), m * 128),
            ],
            send_sem=dzs.at[i, t],
            recv_sem=dzr.at[src, st],
            device_id={"sp": i, "tp": t},
            device_id_type=MESH,
        )

    def dp_copy(t, st, m):
        lanes = pl.ds(pl.multiple_of(first(me) * 128, 128), m * 128)
        rows = pl.ds(pl.multiple_of(t * Q, Q), Q)
        return remote(
            dw.at[rows, lanes],
            dn.at[me, :, pl.ds(pl.multiple_of(st * (m * 128), 128), m * 128)],
            dzs.at[me, t],
            dzr.at[me, st],
            "tp",
            t,
        )

    def dy_copy(j, h, m):
        r = dn.at[j, pl.ds(pl.multiple_of(h * (Q // 2), Q // 2), Q // 2), pl.ds(0, TP * m * 128)]
        return remote(r, r, dys.at[j], dyr.at[j], "grp", 1 - g)

    def peers(body):
        for f in range(1, TP):
            body(lax.rem(tp + f, TP))

    def send_dn(i):
        def some(m):
            for t in range(TP):
                dz_copy(i, t, me, tp, m).start()

        tiles_of(i, some)

    for kk in range(min(EARLY, NT)):
        send_gu(0, kk, up=False)
        send_gu(1, kk, up=False)

    rows = lax.broadcasted_iota(jnp.int32, (T, T), 0)
    cols = lax.broadcasted_iota(jnp.int32, (T, T), 1)
    causal = cols < rows
    later = (rows > cols).astype(F32)

    def block(kk, vv, ll, diag):
        for h in range(H):
            span = slice(h * hd, (h + 1) * hd)
            s = nt(q[:, span], kk[:, span]) * (hd**-0.5) + ll[h : h + 1, :]
            soft = jnp.log1p(jnp.exp(-jnp.abs(s)))
            keep = jnp.minimum(-s, 0.0) - soft
            logsig = jnp.minimum(s, 0.0) - soft
            if diag:
                keep = jnp.where(causal, keep, 0.0)
            within = jnp.dot(
                keep, later, preferred_element_type=F32, precision=lax.Precision.HIGHEST
            )
            stick = jnp.exp(logsig + within)
            if diag:
                stick = jnp.where(causal, stick, 0.0)
            part = jnp.dot(stick.astype(BF16), vv[:, span], preferred_element_type=F32)
            total = jnp.broadcast_to(jnp.sum(keep, axis=-1, keepdims=True), (T, hd))
            if diag:
                acc[h] = part
                run[h] = total
            else:
                acc[h] += jnp.exp(run[h]) * part
                run[h] += total

    block(k[...], v[...], lg[...], True)

    def earlier(i):
        b = me - 1 - i

        @pl.when(b >= 0)
        def _():
            for c in kv_copies(b, me):
                c.wait_recv()
            block(kb[b], vb[b], lb[b], False)

    each(S - 1, earlier)

    attended = jnp.concatenate([acc[h] for h in range(H)], axis=1).astype(BF16)
    load_ow.wait()
    width = 512 if D % 512 == 0 else D
    for c0 in range(0, D, width):
        piece = jnp.dot(attended, owv[:, c0 : c0 + width], preferred_element_type=F32)
        hs[:, :, c0 : c0 + width] = piece.astype(BF16).reshape(TP, R, width)

    def hp_copy(t, slot):
        return remote(hs.at[t], hr.at[slot], hss.at[t], hrs.at[slot], "tp", t)

    peers(lambda t: hp_copy(t, tp).start())
    mid[...] = hs[tp].astype(F32)
    planes(lambda i: [c.wait_send() for c in kv_copies(me, i)], down=False)
    send_gu(0, 0, down=False)
    send_gu(1, 0, down=False)

    def add_hp(t):
        hp_copy(t, t).wait_recv()
        mid[...] += hr[t].astype(F32)

    peers(add_hp)
    load_res.wait()
    mixed = mid[...].astype(BF16).astype(F32)
    xm[me, my_rows] = (resv[...].astype(F32) + mg[...] * normalize(mixed)).astype(BF16)

    def piece_of(j, t):
        return xm.at[j, pl.ds(pl.multiple_of(t * R, R), R)]

    def az_copy(j, way):
        r = piece_of(j, tp)
        return remote(r, r, azs.at[way, j], azr.at[j], "sp", me + 1 if way else me - 1)

    def ends(j, body):
        @pl.when((j <= me) & (me < S - 1))
        def _():
            body(az_copy(j, 1))

        @pl.when((j >= me) & (me > 0))
        def _():
            body(az_copy(j, 0))

    def ax_copy(j, t):
        return remote(piece_of(j, t), piece_of(j, t), axs.at[j], axr.at[j], "tp", xpeer)

    def ac_copy(j, t):
        return remote(piece_of(j, t), piece_of(j, t), acs.at[j], acr.at[j], "tp", cpeer)

    def af_copy(j, t):
        return remote(piece_of(j, t), piece_of(j, t), afs.at[j], afr.at[j], "tp", cpeer)

    ends(me, lambda c: c.start())
    ax_copy(me, tp).start()
    ac_copy(me, tp).start()

    for w in range(2):
        for kk in range(1, NT):
            send_gu(w, kk, down=False)
        for kk in range(EARLY, NT):
            send_gu(w, kk, up=False)

    def pass_gu(kk, **sides):
        def one(j):
            gz_copy(0, me, kk, j, j).wait_recv()
            gz_copy(1, me, kk, j, j).wait_recv()
            gy_copy(j, kk, g).start()

        @pl.when(kk < n_me)
        def _():
            planes(one, **sides)

    def spread(j):
        az_copy(j, 0).wait_recv()
        ends(j, lambda c: c.start())
        ax_copy(j, tp).start()
        ac_copy(j, tp).start()

    def hand_on(j):
        ax_copy(j, xpeer).wait_recv()
        af_copy(j, xpeer).start()

    def ready(j):
        ac_copy(j, cpeer).wait_recv()
        af_copy(j, far).wait_recv()
        for r0 in range(0, T, R):
            rows_f = xm[j, pl.ds(r0, R)].astype(F32)
            at = pl.ds(pl.multiple_of(j * T + r0, R), R)
            xn[at] = (fg[...] * normalize(rows_f)).astype(BF16)

    pass_gu(0)
    pass_gu(1, down=False)
    hand_on(me)
    planes(spread, at=(1,))
    planes(hand_on, at=(1,))
    ready(me)
    planes(spread, at=(2,))
    planes(hand_on, at=(2,))
    planes(spread, at=range(3, S))
    planes(send_dn)
    tiles_of(me, lambda m: peers(lambda t: dp_copy(t, tp, m).start()))
    planes(hand_on, at=range(3, S))
    pass_gu(1, up=False)
    planes(ready)

    def hid_at(t, kk):
        return hid.at[t * NT + kk]

    def hx_copy(t, kk):
        return remote(hid_at(t, kk), hid_at(t, kk), hxs.at[kk], hxr.at[kk], "tp", xpeer)

    def hc_copy(t, kk):
        return remote(hid_at(t, kk), hid_at(t, kk), hcs.at[kk], hcr.at[kk], "tp", cpeer)

    def hf_copy(t, kk):
        return remote(hid_at(t, kk), hid_at(t, kk), hfs.at[kk], hfr.at[kk], "tp", cpeer)

    def tile(kk):
        own_gu(0, kk).wait()
        own_gu(1, kk).wait()
        planes(lambda j: gy_copy(j, kk, 1 - g).wait_recv())
        both = jnp.dot(xn[...], gu[kk], preferred_element_type=F32)
        gate, up = both[:, :128], both[:, 128:]
        hid[tp * NT + kk] = (gate / (1.0 + jnp.exp(-gate)) * up).astype(BF16)
        hx_copy(tp, kk).start()
        hc_copy(tp, kk).start()

    def pass_tile(kk):
        hx_copy(xpeer, kk).wait_recv()
        hf_copy(xpeer, kk).start()

    with_tiles(tile, at=(0,))
    for kk in range(2, NT):
        pass_gu(kk)
    with_tiles(tile, at=(1,))
    with_tiles(pass_tile, at=(0,))
    with_tiles(tile, at=range(2, NT))
    with_tiles(pass_tile, at=range(1, NT))

    def pass_dn(j):
        def some(m):
            for st in range(TP):
                dz_copy(me, tp, j, st, m).wait_recv()
            dy_copy(j, g, m).start()

        tiles_of(me, some)

    def hid_ready(kk):
        hc_copy(cpeer, kk).wait_recv()
        hf_copy(far, kk).wait_recv()

    def rs_copy(j, dst, src):
        return remote(us.at[j, dst], ur.at[j, src], rss.at[j, dst], rsr.at[j, src], "sp", dst)

    def down(j, own=False):
        def some(m):
            if own:
                own_dn(m).wait()
                peers(lambda t: dp_copy(tp, t, m).wait_recv())
            else:
                dy_copy(j, 1 - g, m).wait_recv()
            x = jnp.concatenate(
                [hid[t * NT + kk] for t in range(TP) for kk in range(m)], axis=1
            )
            us[j] = nt(x, dn[j, :, : TP * m * 128]).astype(BF16).reshape(S, T, Q)

        tiles_of(me, some)
        planes(lambda i: rs_copy(j, i, me).start())

    planes(pass_dn, at=(1,))
    with_tiles(hid_ready)
    down(me, True)
    for d in range(1, S):
        planes(pass_dn, at=range(d + 1, min(d + 2, S)))
        planes(down, at=(d,))

    def ox_copy(j, t):
        return remote(zq.at[t, j], zq.at[t, j], oxs.at[j], oxr.at[j], "tp", xpeer)

    def oc_copy(j, t):
        return remote(zq.at[t, j], zq.at[t, j], ocs.at[j], ocr.at[j], "tp", cpeer)

    def of_copy(j, t):
        return remote(zq.at[t, j], zq.at[t, j], ofs.at[j], ofr.at[j], "tp", cpeer)

    def settle(j):
        planes(lambda i: rs_copy(j, i, i).wait_recv())
        total = us[j, me].astype(F32)
        for d in range(1, S):
            total += ur[j, lax.rem(me + d, S)].astype(F32)
        zq[tp, j] = total.astype(BF16)
        ox_copy(j, tp).start()
        oc_copy(j, tp).start()

    for j in range(S):
        settle(j)
    for j in range(S):
        ox_copy(j, xpeer).wait_recv()
        of_copy(j, xpeer).start()
    for j in range(S):
        oc_copy(j, cpeer).wait_recv()
        of_copy(j, far).wait_recv()

    def o_out(r):
        rows_r = pl.ds(r * R, R)
        return pltpu.make_async_copy(ov.at[rows_r], out.at[rows_r], outs.at[r])

    for r in range(TP):
        rows_r = pl.ds(r * R, R)
        ffn = jnp.concatenate(
            [zq[t, j, rows_r] for j in range(S) for t in range(TP)], axis=1
        ).astype(F32)
        ov[rows_r] = (xm[me, rows_r].astype(F32) + og[...] * normalize(ffn)).astype(BF16)
        o_out(r).start()

    peers(lambda t: hp_copy(t, tp).wait_send())
    for j in range(S):
        ends(j, lambda c: c.wait_send())
        ax_copy(j, tp).wait_send()
        ac_copy(j, tp).wait_send()
        af_copy(j, xpeer).wait_send()
        ox_copy(j, tp).wait_send()
        oc_copy(j, tp).wait_send()
        of_copy(j, xpeer).wait_send()
        planes(lambda i: rs_copy(j, i, me).wait_send())

    def sent(i):
        for kk in range(NT):
            for w in range(2):

                @pl.when(kk < count(i))
                def _(kk=kk, w=w):
                    gz_copy(w, i, kk, me, i).wait_send()

        def some(m):
            for t in range(TP):
                dz_copy(i, t, me, tp, m).wait_send()

        tiles_of(i, some)
        tiles_of(me, lambda m: dy_copy(i, g, m).wait_send())

    planes(sent)

    def tile_sent(kk):
        planes(lambda j: gy_copy(j, kk, g).wait_send())
        hx_copy(tp, kk).wait_send()
        hc_copy(tp, kk).wait_send()
        hf_copy(xpeer, kk).wait_send()

    with_tiles(tile_sent)
    tiles_of(me, lambda m: peers(lambda t: dp_copy(t, tp, m).wait_send()))
    for r in range(TP):
        o_out(r).wait()


def gathered_call(S, TP, q, k, v, lgt, H, mg, fg, og, res, ow, gw, uw, dw):
    T, hw = q.shape
    D = res.shape[1]
    C, U = gw.shape
    R, Q = T // TP, C // TP
    base, extra = divmod(U // 128, S)
    extras = EXTRA_ORDER(S)[:extra]
    NT = base + (1 if extra else 0)
    vm = pl.BlockSpec(memory_space=pltpu.VMEM)
    hb = pl.BlockSpec(memory_space=pl.ANY)
    dma = pltpu.SemaphoreType.DMA
    pairs = lambda *shape: [dma(shape), dma(shape)]
    return pl.pallas_call(
        functools.partial(gathered, S, TP, H, base, extras),
        out_shape=jax.ShapeDtypeStruct((T, D), BF16),
        in_specs=[vm] * 7 + [hb] * 5,
        out_specs=hb,
        scratch_shapes=[
            pltpu.VMEM((S, T, hw), BF16),
            pltpu.VMEM((S, T, hw), BF16),
            pltpu.VMEM((S,) + lgt.shape, F32),
            pltpu.VMEM((H, T, hw // H), F32),
            pltpu.VMEM((H, T, hw // H), F32),
            pltpu.VMEM(ow.shape, BF16),
            pltpu.VMEM((R, D), BF16),
            pltpu.VMEM((TP, R, D), BF16),
            pltpu.VMEM((TP, R, D), BF16),
            pltpu.VMEM((R, D), F32),
            pltpu.VMEM((S, T, D), BF16),
            pltpu.VMEM((S * T, D), BF16),
            pltpu.VMEM((NT, D, 256), BF16),
            pltpu.VMEM((TP * NT, S * T, 128), BF16),
            pltpu.VMEM((S, Q, TP * NT * 128), BF16),
            pltpu.VMEM((S, S, T, Q), BF16),
            pltpu.VMEM((S, S, T, Q), BF16),
            pltpu.VMEM((TP, S, T, Q), BF16),
            pltpu.VMEM((T, D), BF16),
            dma((3 + 2 * NT,)),
            *pairs(S, 3),
            *pairs(TP),
            dma((2, S)),
            dma((S,)),
            *pairs(S),
            *pairs(S),
            *pairs(S),
            *pairs(2, S, NT),
            *pairs(S, NT),
            *pairs(S, TP),
            *pairs(S),
            *pairs(NT),
            *pairs(NT),
            *pairs(NT),
            *pairs(S, S),
            *pairs(S),
            *pairs(S),
            *pairs(S),
            dma((TP,)),
        ],
        compiler_params=pltpu.CompilerParams(
            collective_id=0, has_side_effects=True, vmem_limit_bytes=67043328 - 2**20
        ),
    )(q, k, v, lgt, mg[None], fg[None], og[None], res, ow, gw, uw, dw)


def solution(mesh):
    S, TP, G = mesh.shape["sp"], mesh.shape["tp"], mesh.shape["grp"]

    def shards(q, k, v, lg, res, ow, mg, fg, og, gw, uw, dw):
        T, H = lg.shape
        hw = q.shape[1]
        D = res.shape[1]
        C, U = gw.shape
        R = T // TP
        pieces = max([p for p in range(1, MOST_PIECES + 1) if U % (128 * p) == 0], default=1)
        W = U // pieces
        pad = -H % 8
        lgt = jnp.pad(lg.astype(F32).T, ((0, pad), (0, 0)))
        if U % 128 == 0 and U // 128 >= S and C % (128 * TP) == 0 and T % (16 * TP) == 0 and (TP, G) == (4, 2):
            return gathered_call(S, TP, q, k, v, lgt, H, mg, fg, og, res, ow, gw, uw, dw)
        vm = pl.BlockSpec(memory_space=pltpu.VMEM)
        hb = pl.BlockSpec(memory_space=pl.ANY)
        dma = pltpu.SemaphoreType.DMA
        return pl.pallas_call(
            functools.partial(kernel, S, TP, H, pieces),
            out_shape=jax.ShapeDtypeStruct((T, D), BF16),
            in_specs=[vm] * 7 + [hb] * 5,
            out_specs=hb,
            scratch_shapes=[
                pltpu.VMEM((S, T, hw), BF16),
                pltpu.VMEM((S, T, hw), BF16),
                pltpu.VMEM((S,) + lgt.shape, F32),
                pltpu.VMEM((H, T, hw // H), F32),
                pltpu.VMEM((H, T, hw // H), F32),
                pltpu.VMEM(ow.shape, BF16),
                pltpu.VMEM(gw.shape, BF16),
                pltpu.VMEM(uw.shape, BF16),
                pltpu.VMEM(dw.shape, BF16),
                pltpu.VMEM((R, D), BF16),
                pltpu.VMEM((TP, R, D), BF16),
                pltpu.VMEM((TP, R, D), BF16),
                pltpu.VMEM((R, D), F32),
                pltpu.VMEM((R, C), F32),
                pltpu.VMEM((S, R, C), BF16),
                pltpu.VMEM((TP, S, R, C), BF16),
                pltpu.VMEM((2, T, W), F32),
                pltpu.VMEM((pieces, S, 2, T, W), BF16),
                pltpu.VMEM((pieces, S + 1, 2, T, W), BF16),
                pltpu.VMEM((pieces, S, T, W), BF16),
                pltpu.VMEM((TP, S, R, C), BF16),
                pltpu.VMEM((TP, S, R, C), BF16),
                pltpu.VMEM((S, R, C), BF16),
                pltpu.VMEM((S, R, C), BF16),
                pltpu.VMEM((TP, R, D), BF16),
                dma((5,)),
                dma((S, 3)),
                dma((S, 3)),
                dma((TP,)),
                dma((TP,)),
                dma((S,)),
                dma((S,)),
                dma((TP, S)),
                dma((TP, S)),
                dma((pieces, S)),
                dma((pieces, S + 1)),
                dma((pieces, S)),
                dma((pieces, S)),
                dma((pieces, S)),
                dma((TP, S)),
                dma((TP, S)),
                dma((S,)),
                dma((S,)),
                dma((TP,)),
                dma((TP,)),
                dma((TP,)),
            ],
            compiler_params=pltpu.CompilerParams(
                collective_id=0, has_side_effects=True, vmem_limit_bytes=67043328 - 2**20
            ),
        )(q, k, v, lgt, mg[None], fg[None], og[None], res, ow, gw, uw, dw)

    placed = (
        P(("grp", "sp"), "tp"),
        P(("grp", "sp"), "tp"),
        P(("grp", "sp"), "tp"),
        P(("grp", "sp"), "tp"),
        P(("grp", "sp"), None),
        P("tp", None),
        P(),
        P(),
        P(),
        P("sp", "tp"),
        P("sp", "tp"),
        P("sp", "tp"),
    )
    return jax.shard_map(
        shards, mesh=mesh, in_specs=placed, out_specs=P(("grp", "sp"), None), check_vma=False
    )
```

```python
import functools

import jax
import jax.numpy as jnp
from jax import lax
from jax.experimental import pallas as pl
from jax.experimental.pallas import tpu as pltpu
from jax.sharding import PartitionSpec as P

epsilon = 1e-06
MESH = pl.DeviceIdType.MESH
F32 = jnp.float32
BF16 = jnp.bfloat16
LAG = 2
MOST_PIECES = 5
EARLY = 2


def KV_ORDER(S):
    return range(S - 1, 0, -1)


def EXTRA_ORDER(S):
    return list(range(S))


def normalize(rows):
    return rows * lax.rsqrt(jnp.mean(rows * rows, axis=-1, keepdims=True) + epsilon)


def each(count, body):
    if count <= 4:
        for i in range(count):
            body(i)
    else:

        def step(i, carry):
            body(i)
            return carry

        lax.fori_loop(0, count, step, 0)


def remote(src, dst, send, recv, axis, peer):
    return pltpu.make_async_remote_copy(
        src_ref=src,
        dst_ref=dst,
        send_sem=send,
        recv_sem=recv,
        device_id={axis: peer},
        device_id_type=MESH,
    )


def nt(a, b):
    return lax.dot_general(a, b, (((1,), (1,)), ((), ())), preferred_element_type=F32)


def kernel(
    S, TP, H, pieces,
    q, k, v, lg, mg, fg, og, res, ow, gw, uw, dw,
    out,
    kb, vb, lb, acc, run, owv, gwv, uwv, dwv, resv,
    hs, hr, mid, zs_sum, ns, na, tmp, gs, gr, hall, us, ur, zs, zr, oall,
    loc, kvs, kvr, hss, hrs, n1s, n1r, n2s, n2r, gss, grs, hars, hals, har,
    upss, upr, zss, zrs, oss, ors, outs,
):
    me, tp = lax.axis_index("sp"), lax.axis_index("tp")
    T = q.shape[0]
    hd = q.shape[1] // H
    D = out.shape[1]
    R, C = T // TP, D // S
    right, left = lax.rem(me + 1, S), lax.rem(me + S - 1, S)

    my_rows = pl.ds(pl.multiple_of(tp * R, R), R)
    loads = [
        pltpu.make_async_copy(a, b, loc.at[i])
        for i, (a, b) in enumerate(
            [(ow, owv), (res.at[my_rows], resv), (gw, gwv), (uw, uwv), (dw, dwv)]
        )
    ]
    for c in loads:
        c.start()

    barrier = pltpu.get_barrier_semaphore()
    for f in range(1, S):
        pl.semaphore_signal(barrier, inc=1, device_id={"sp": lax.rem(me + f, S)}, device_id_type=MESH)
    for f in range(1, TP):
        pl.semaphore_signal(barrier, inc=1, device_id={"tp": lax.rem(tp + f, TP)}, device_id_type=MESH)
    pl.semaphore_wait(barrier, S + TP - 2)

    def kv_copies(b, own):
        srcs = (k, v, lg) if own else (kb.at[b], vb.at[b], lb.at[b])
        return [
            remote(src, dst.at[b], kvs.at[b, i], kvr.at[b, i], "sp", right)
            for i, (src, dst) in enumerate(zip(srcs, (kb, vb, lb)))
        ]

    @pl.when(me < S - 1)
    def _():
        for c in kv_copies(me, True):
            c.start()

    rows = lax.broadcasted_iota(jnp.int32, (T, T), 0)
    cols = lax.broadcasted_iota(jnp.int32, (T, T), 1)
    causal = cols < rows
    later = (rows > cols).astype(F32)

    def block(kk, vv, ll, diag):
        for h in range(H):
            span = slice(h * hd, (h + 1) * hd)
            s = nt(q[:, span], kk[:, span]) * (hd**-0.5) + ll[h : h + 1, :]
            soft = jnp.log1p(jnp.exp(-jnp.abs(s)))
            keep = jnp.minimum(-s, 0.0) - soft
            logsig = jnp.minimum(s, 0.0) - soft
            if diag:
                keep = jnp.where(causal, keep, 0.0)
            within = jnp.dot(
                keep, later, preferred_element_type=F32, precision=lax.Precision.HIGHEST
            )
            stick = jnp.exp(logsig + within)
            if diag:
                stick = jnp.where(causal, stick, 0.0)
            part = jnp.dot(stick.astype(BF16), vv[:, span], preferred_element_type=F32)
            total = jnp.broadcast_to(jnp.sum(keep, axis=-1, keepdims=True), (T, hd))
            if diag:
                acc[h] = part
                run[h] = total
            else:
                acc[h] += jnp.exp(run[h]) * part
                run[h] += total

    block(k[...], v[...], lg[...], True)

    def earlier(i):
        b = me - 1 - i

        @pl.when(b >= 0)
        def _():
            for c in kv_copies(b, False):
                c.wait_recv()

            @pl.when(me < S - 1)
            def _():
                for c in kv_copies(b, False):
                    c.start()

            block(kb[b], vb[b], lb[b], False)

    each(S - 1, earlier)

    attended = jnp.concatenate([acc[h] for h in range(H)], axis=1).astype(BF16)
    loads[0].wait()
    width = 512 if D % 512 == 0 else D
    for c0 in range(0, D, width):
        piece = jnp.dot(attended, owv[:, c0 : c0 + width], preferred_element_type=F32)
        hs[:, :, c0 : c0 + width] = piece.astype(BF16).reshape(TP, R, width)

    def hp_copy(t, slot):
        return remote(hs.at[t], hr.at[slot], hss.at[t], hrs.at[slot], "tp", t)

    def others(count, own, body):
        def go(i):
            body(lax.rem(own + 1 + i, count))

        each(count - 1, go)

    others(TP, tp, lambda t: hp_copy(t, tp).start())
    mid[...] = hs[tp].astype(F32)

    def add_hp(t):
        hp_copy(t, t).wait_recv()
        mid[...] += hr[t].astype(F32)

    others(TP, tp, add_hp)
    loads[1].wait()
    mixed = mid[...].astype(BF16).astype(F32)
    middle = (resv[...].astype(F32) + mg[...] * normalize(mixed)).astype(BF16).astype(F32)
    mid[...] = middle
    normed = (fg[...] * normalize(middle)).astype(BF16)
    for j in range(S):
        ns[j] = normed[:, j * C : (j + 1) * C]

    def n1_copy(j, slot):
        return remote(ns.at[j], na.at[tp, slot], n1s.at[j], n1r.at[slot], "sp", j)

    def n2_copy(t, slot, s):
        return remote(na.at[tp, s], na.at[slot, s], n2s.at[t, s], n2r.at[slot, s], "tp", t)

    others(S, me, lambda j: n1_copy(j, me).start())
    na[tp, me] = ns[me]
    others(TP, tp, lambda t: n2_copy(t, tp, me).start())

    def pass_on(s):
        n1_copy(s, s).wait_recv()
        others(TP, tp, lambda t: n2_copy(t, tp, s).start())

    others(S, me, pass_on)
    for c in loads[2:4]:
        c.wait()

    def arrive(s):
        others(TP, tp, lambda t: remote(na.at[tp, s], na.at[t, s], n2s.at[t, s], n2r.at[t, s], "tp", t).wait_recv())

    W = gs.shape[-1]
    lag = LAG

    def partial(p, j):
        @pl.when(p == 0)
        def _():
            arrive(j)

        x = na[:, j].reshape(T, C)
        units = pl.ds(pl.multiple_of(p * W, W), W)
        tmp[0] = jnp.dot(x, gwv[:, units], preferred_element_type=F32)
        tmp[1] = jnp.dot(x, uwv[:, units], preferred_element_type=F32)

    def g_copy(p, j, slot, peer):
        return remote(gs.at[p, j], gr.at[p, slot], gss.at[p, j], grs.at[p, slot], "sp", peer)

    def chain(p, j, first, slot, peer):
        partial(p, j)

        @pl.when(first)
        def _():
            gs[p, j] = tmp[...].astype(BF16)

        @pl.when(jnp.logical_not(first))
        def _():
            g_copy(p, j, j, peer).wait_recv()
            gs[p, j] = (tmp[...] + gr[p, j].astype(F32)).astype(BF16)

        g_copy(p, j, slot, peer).start()

    def h_right(p, b):
        return remote(hall.at[p, b], hall.at[p, b], hars.at[p, b], har.at[p, b], "sp", right)

    def h_left(p, b):
        return remote(hall.at[p, b], hall.at[p, b], hals.at[p, b], har.at[p, b], "sp", left)

    def cut(at):
        return lax.div(at, S - 1), lax.rem(at, S - 1)

    def reduce_step(g):
        at_right = g - me * lag
        at_left = g - (S - 1 - me) * lag

        @pl.when((at_right >= 0) & (at_right < pieces * (S - 1)))
        def _():
            p, tau = cut(at_right)

            @pl.when(S - 1 - tau > me)
            def _():
                chain(p, S - 1 - tau, me == 0, S - 1 - tau, right)

        @pl.when((at_left >= 0) & (at_left < pieces * (S - 1)))
        def _():
            p, j = cut(at_left)

            @pl.when(j < me)
            def _():
                chain(p, j, me == S - 1, lax.select(j == me - 1, S, j), left)

    def finish(p):
        partial(p, me)

        @pl.when(me > 0)
        def _():
            g_copy(p, me, me, left).wait_recv()
            tmp[...] += gr[p, me].astype(F32)

        @pl.when(me < S - 1)
        def _():
            g_copy(p, me, S, right).wait_recv()
            tmp[...] += gr[p, S].astype(F32)

        gate = tmp[0]
        hall[p, me] = (gate / (1.0 + jnp.exp(-gate)) * tmp[1]).astype(BF16)

        @pl.when(me < S - 1)
        def _():
            h_right(p, me).start()

        @pl.when(me > 0)
        def _():
            h_left(p, me).start()

    def spread(p, i, then):
        lo, hi = me - 1 - i, me + 1 + i

        @pl.when(lo >= 0)
        def _():
            h_right(p, lo).wait_recv()

            @pl.when(me < S - 1)
            def _():
                h_right(p, lo).start()

            then(lo)

        @pl.when(hi < S)
        def _():
            h_left(p, hi).wait_recv()

            @pl.when(me > 0)
            def _():
                h_left(p, hi).start()

            then(hi)

    def step(g, carry):
        reduce_step(g)
        at = g - (S - 1) * lag
        p, tau = cut(at)

        @pl.when((at >= 0) & (tau == 0) & (p < pieces))
        def _():
            finish(p)

        def gather(i, carry):
            at_i = at - (i + 1) * lag
            p, tau = cut(at_i)

            @pl.when((at_i >= 0) & (tau == 0) & (p < pieces - 1))
            def _():
                spread(p, i, lambda b: None)

            return carry

        return lax.fori_loop(0, S - 1, gather, carry)

    steps = (S - 1) * (lag + max(pieces - 1, pieces - 2 + lag)) + 1
    lax.fori_loop(0, steps, step, 0)

    def up_copy(t, slot, b):
        return remote(us.at[t, b], ur.at[slot, b], upss.at[t, b], upr.at[slot, b], "tp", t)

    def down(b):
        rows_b = jnp.concatenate([hall[p, b] for p in range(pieces)], axis=1)
        us[:, b] = nt(rows_b, dwv[...]).astype(BF16).reshape(TP, R, C)
        others(TP, tp, lambda t: up_copy(t, tp, b).start())

    def z_copy(b, slot):
        return remote(zs.at[b], zr.at[slot], zss.at[b], zrs.at[slot], "sp", b)

    def settle(b):
        def add(t):
            up_copy(t, t, b).wait_recv()
            zs_sum[...] += ur[t, b].astype(F32)

        zs_sum[...] = us[tp, b].astype(F32)
        others(TP, tp, add)
        zs[b] = zs_sum[...].astype(BF16)

        @pl.when(b != me)
        def _():
            z_copy(b, me).start()

    loads[4].wait()
    down(me)

    def last(i, carry):
        spread(pieces - 1, i, down)
        return carry

    lax.fori_loop(0, S - 1, last, 0)
    others(S, me, settle)
    settle(me)
    zr[me] = zs[me]
    others(S, me, lambda s: z_copy(s, s).wait_recv())
    ffn = jnp.concatenate([zr[s] for s in range(S)], axis=1).astype(F32)
    oall[tp] = (mid[...] + og[...] * normalize(ffn)).astype(BF16)

    def o_copy(t, slot):
        return remote(oall.at[tp], oall.at[slot], oss.at[t], ors.at[slot], "tp", t)

    def o_out(t):
        return pltpu.make_async_copy(
            oall.at[t], out.at[pl.ds(pl.multiple_of(t * R, R), R)], outs.at[t]
        )

    others(TP, tp, lambda t: o_copy(t, tp).start())
    o_out(tp).start()

    def o_in(t):
        remote(oall.at[tp], oall.at[t], oss.at[t], ors.at[t], "tp", t).wait_recv()
        o_out(t).start()

    others(TP, tp, o_in)
    each(TP, lambda t: o_out(t).wait())

    @pl.when(me < S - 1)
    def _():
        def sent(b):
            @pl.when(b <= me)
            def _():
                for c in kv_copies(b, False):
                    c.wait_send()
                each(pieces, lambda p: h_right(p, b).wait_send())

        each(S, sent)

    @pl.when(me > 0)
    def _():
        def sent(b):
            @pl.when(b >= me)
            def _():
                each(pieces, lambda p: h_left(p, b).wait_send())

        each(S, sent)

    def sp_sent(j):
        n1_copy(j, me).wait_send()
        z_copy(j, me).wait_send()
        each(pieces, lambda p: g_copy(p, j, j, right).wait_send())

    others(S, me, sp_sent)

    def tp_sent(t):
        hp_copy(t, tp).wait_send()
        o_copy(t, tp).wait_send()

        def inner(s):
            n2_copy(t, tp, s).wait_send()
            up_copy(t, tp, s).wait_send()

        each(S, inner)

    others(TP, tp, tp_sent)


def gathered(
    S, TP, H, base, extras,
    q, k, v, lg, mg, fg, og, res, ow, gw, uw, dw,
    out,
    kb, vb, lb, acc, run, owv, resv, hs, hr, mid, xm, xn, gu, hid, dn, us, ur, zq, ov,
    loc, kvs, kvr, hss, hrs, azs, azr, axs, axr, acs, acr, afs, afr,
    gzs, gzr, gys, gyr, dzs, dzr, dys, dyr, hxs, hxr, hcs, hcr, hfs, hfr,
    rss, rsr, oxs, oxr, ocs, ocr, ofs, ofr, outs,
):
    me, tp, g = lax.axis_index("sp"), lax.axis_index("tp"), lax.axis_index("grp")
    T = q.shape[0]
    hd = q.shape[1] // H
    D = out.shape[1]
    R, C = T // TP, D // S
    NT = gu.shape[0]
    half, Q = C // 2, C // TP
    xpeer = lax.rem(tp + 2, TP)
    cpeer = tp + 1 - 2 * lax.rem(tp, 2)
    far = lax.rem(cpeer + 2, TP)

    def count(i):
        c = base
        for p in extras:
            c = c + jnp.where(i == p, 1, 0)
        return c

    def first(i):
        c = i * base
        for p in extras:
            c = c + jnp.where(i > p, 1, 0)
        return c

    def tiles_of(i, body):
        c = count(i)
        for m in sorted({base, base + 1} if extras else {base}):

            @pl.when(c == m)
            def _(m=m):
                body(m)

    n_me = count(me)
    my_rows = pl.ds(pl.multiple_of(tp * R, R), R)
    load_ow = pltpu.make_async_copy(ow, owv, loc.at[0])
    load_res = pltpu.make_async_copy(res.at[my_rows], resv, loc.at[1])
    load_ow.start()
    load_res.start()

    def own_gu(w, kk):
        lanes = pl.ds(pl.multiple_of((first(me) + kk) * 128, 128), 128)
        rows = pl.ds(pl.multiple_of(me * C, C), C)
        return pltpu.make_async_copy(
            (gw, uw)[w].at[:, lanes], gu.at[kk, rows, pl.ds(w * 128, 128)], loc.at[2 + w * NT + kk]
        )

    def own_dn(m):
        lanes = pl.ds(pl.multiple_of(first(me) * 128, 128), m * 128)
        rows = pl.ds(pl.multiple_of(tp * Q, Q), Q)
        to = pl.ds(pl.multiple_of(tp * (m * 128), 128), m * 128)
        return pltpu.make_async_copy(dw.at[rows, lanes], dn.at[me, :, to], loc.at[2 + 2 * NT])

    def with_tiles(body, at=range(NT)):
        for kk in at:

            @pl.when(kk < n_me)
            def _(kk=kk):
                body(kk)

    def load_own(kk):
        own_gu(0, kk).start()
        own_gu(1, kk).start()

    with_tiles(load_own)
    tiles_of(me, lambda m: own_dn(m).start())

    barrier = pltpu.get_barrier_semaphore()

    def greet(i):
        for f in range(TP):

            @pl.when((i != 0) | (f != 0))
            def _(f=f):
                pl.semaphore_signal(
                    barrier,
                    inc=1,
                    device_id={"sp": lax.rem(me + i, S), "tp": lax.rem(tp + f, TP)},
                    device_id_type=MESH,
                )

    for i in range(S):
        greet(i)
    pl.semaphore_signal(barrier, inc=1, device_id={"grp": 1 - g}, device_id_type=MESH)
    pl.semaphore_wait(barrier, S * TP)

    def planes(body, up=True, down=True, at=range(1, S)):
        for d in at:
            if down:

                @pl.when(me - d >= 0)
                def _(d=d):
                    body(me - d)

            if up:

                @pl.when(me + d < S)
                def _(d=d):
                    body(me + d)

    def kv_copies(b, dst):
        return [
            remote(src, to.at[b], kvs.at[dst, i], kvr.at[b, i], "sp", dst)
            for i, (src, to) in enumerate(zip((k, v, lg), (kb, vb, lb)))
        ]

    def send_kv(i):
        for c in kv_copies(me, i):
            c.start()

    planes(send_kv, down=False, at=KV_ORDER(S))

    def gz_copy(w, i, kk, src, dst):
        lanes = pl.ds(pl.multiple_of((first(i) + kk) * 128, 128), 128)
        rows = pl.ds(pl.multiple_of(src * C + g * half, half), half)
        return remote(
            (gw, uw)[w].at[pl.ds(pl.multiple_of(g * half, half), half), lanes],
            gu.at[kk, rows, pl.ds(w * 128, 128)],
            gzs.at[w, i, kk],
            gzr.at[w, src, kk],
            "sp",
            dst,
        )

    def gy_copy(j, kk, h):
        r = gu.at[kk, pl.ds(pl.multiple_of(j * C + h * half, half), half)]
        return remote(r, r, gys.at[j, kk], gyr.at[j, kk], "grp", 1 - g)

    def send_gu(w, kk, **sides):
        def one(i):
            @pl.when(kk < count(i))
            def _():
                gz_copy(w, i, kk, me, i).start()

        planes(one, **sides)

    def dz_copy(i, t, src, st, m):
        lanes = pl.ds(pl.multiple_of(first(i) * 128, 128), m * 128)
        rows = pl.ds(pl.multiple_of(t * Q + g * (Q // 2), Q // 2), Q // 2)
        return pltpu.make_async_remote_copy(
            src_ref=dw.at[rows, lanes],
            dst_ref=dn.at[
                src,
                pl.ds(pl.multiple_of(g * (Q // 2), Q // 2), Q // 2),
                pl.ds(pl.multiple_of(st * (m * 128), 128), m * 128),
            ],
            send_sem=dzs.at[i, t],
            recv_sem=dzr.at[src, st],
            device_id={"sp": i, "tp": t},
            device_id_type=MESH,
        )

    def dp_copy(t, st, m):
        lanes = pl.ds(pl.multiple_of(first(me) * 128, 128), m * 128)
        rows = pl.ds(pl.multiple_of(t * Q, Q), Q)
        return remote(
            dw.at[rows, lanes],
            dn.at[me, :, pl.ds(pl.multiple_of(st * (m * 128), 128), m * 128)],
            dzs.at[me, t],
            dzr.at[me, st],
            "tp",
            t,
        )

    def dy_copy(j, st, h, m):
        r = dn.at[
            j,
            pl.ds(pl.multiple_of(h * (Q // 2), Q // 2), Q // 2),
            pl.ds(pl.multiple_of(st * (m * 128), 128), m * 128),
        ]
        return remote(r, r, dys.at[j, st], dyr.at[j, st], "grp", 1 - g)

    def peers(body):
        for f in range(1, TP):
            body(lax.rem(tp + f, TP))

    def send_dn(i):
        def some(m):
            for f in range(TP):
                dz_copy(i, lax.rem(tp + f, TP), me, tp, m).start()

        tiles_of(i, some)

    tiles_of(me, lambda m: peers(lambda t: dp_copy(t, tp, m).start()))
    for kk in range(min(EARLY, NT)):
        send_gu(0, kk, up=False)
        send_gu(1, kk, up=False)

    rows = lax.broadcasted_iota(jnp.int32, (T, T), 0)
    cols = lax.broadcasted_iota(jnp.int32, (T, T), 1)
    causal = cols < rows
    later = (rows > cols).astype(F32)

    def block(kk, vv, ll, diag):
        for h in range(H):
            span = slice(h * hd, (h + 1) * hd)
            s = nt(q[:, span], kk[:, span]) * (hd**-0.5) + ll[h : h + 1, :].astype(F32)
            soft = jnp.log1p(jnp.exp(-jnp.abs(s)))
            keep = jnp.minimum(-s, 0.0) - soft
            logsig = jnp.minimum(s, 0.0) - soft
            if diag:
                keep = jnp.where(causal, keep, 0.0)
            within = jnp.dot(
                keep, later, preferred_element_type=F32, precision=lax.Precision.HIGHEST
            )
            stick = jnp.exp(logsig + within)
            if diag:
                stick = jnp.where(causal, stick, 0.0)
            part = jnp.dot(stick.astype(BF16), vv[:, span], preferred_element_type=F32)
            total = jnp.broadcast_to(jnp.sum(keep, axis=-1, keepdims=True), (T, hd))
            if diag:
                acc[h] = part
                run[h] = total
            else:
                acc[h] += jnp.exp(run[h]) * part
                run[h] += total

    block(k[...], v[...], lg[...], True)

    def earlier(i):
        b = me - 1 - i

        @pl.when(b >= 0)
        def _():
            for c in kv_copies(b, me):
                c.wait_recv()
            block(kb[b], vb[b], lb[b], False)

    each(S - 1, earlier)

    attended = jnp.concatenate([acc[h] for h in range(H)], axis=1).astype(BF16)
    load_ow.wait()
    width = 512 if D % 512 == 0 else D
    for c0 in range(0, D, width):
        piece = jnp.dot(attended, owv[:, c0 : c0 + width], preferred_element_type=F32)
        hs[:, :, c0 : c0 + width] = piece.astype(BF16).reshape(TP, R, width)

    def hp_copy(t, slot):
        return remote(hs.at[t], hr.at[slot], hss.at[t], hrs.at[slot], "tp", t)

    peers(lambda t: hp_copy(t, tp).start())
    mid[...] = hs[tp].astype(F32)
    planes(lambda i: [c.wait_send() for c in kv_copies(me, i)], down=False)
    send_gu(0, 0, down=False)
    send_gu(1, 0, down=False)

    def add_hp(t):
        hp_copy(t, t).wait_recv()
        mid[...] += hr[t].astype(F32)

    peers(add_hp)
    load_res.wait()
    mixed = mid[...].astype(BF16).astype(F32)
    xm[me, my_rows] = (resv[...].astype(F32) + mg[...] * normalize(mixed)).astype(BF16)

    def piece_of(j, t):
        return xm.at[j, pl.ds(pl.multiple_of(t * R, R), R)]

    def az_copy(j, way, dst):
        r = piece_of(j, tp)
        return remote(r, r, azs.at[way, j if way else dst], azr.at[j], "sp", dst)

    def ends(j, body):
        @pl.when((j <= me) & (me < S - 1))
        def _():
            body(az_copy(j, 1, me + 1))

    def ax_copy(j, t):
        return remote(piece_of(j, t), piece_of(j, t), axs.at[j], axr.at[j], "tp", xpeer)

    def ac_copy(j, t):
        return remote(piece_of(j, t), piece_of(j, t), acs.at[j], acr.at[j], "tp", cpeer)

    def af_copy(j, t):
        return remote(piece_of(j, t), piece_of(j, t), afs.at[j], afr.at[j], "tp", cpeer)

    ends(me, lambda c: c.start())
    planes(lambda i: az_copy(me, 0, i).start(), up=False, at=range(S - 1, 0, -1))
    ax_copy(me, tp).start()
    ac_copy(me, tp).start()

    def late_down():
        for w in range(2):
            for kk in range(EARLY, NT):
                send_gu(w, kk, up=False)

    for w in range(2):
        for kk in range(1, NT):
            send_gu(w, kk, down=False)
    pl.when(me < S - 1)(late_down)

    def pass_gu(kk, **sides):
        def one(j):
            gz_copy(0, me, kk, j, j).wait_recv()
            gz_copy(1, me, kk, j, j).wait_recv()
            gy_copy(j, kk, g).start()

        @pl.when(kk < n_me)
        def _():
            planes(one, **sides)

    def spread(j):
        az_copy(j, 1, me).wait_recv()
        ends(j, lambda c: c.start())
        ax_copy(j, tp).start()
        ac_copy(j, tp).start()

    def hand_on(j):
        ax_copy(j, xpeer).wait_recv()
        af_copy(j, xpeer).start()

    def ready(j):
        ac_copy(j, cpeer).wait_recv()
        af_copy(j, far).wait_recv()
        for r0 in range(0, T, R):
            rows_f = xm[j, pl.ds(r0, R)].astype(F32)
            at = pl.ds(pl.multiple_of(j * T + r0, R), R)
            xn[at] = (fg[...] * normalize(rows_f)).astype(BF16)

    def pass_late(at):
        for kk in range(2, NT):
            pass_gu(kk, at=at)

    pass_gu(0)
    pass_gu(1, down=False)
    hand_on(me)
    planes(spread, at=(1,))
    planes(hand_on, at=(1,))
    pl.when(me == S - 1)(late_down)
    ready(me)
    planes(spread, at=(2,))
    pass_late((1,))
    planes(hand_on, at=(2,))
    planes(spread, at=range(3, S))
    pass_late((2,))
    planes(send_dn)
    planes(hand_on, at=range(3, S))
    pass_gu(1, up=False)
    pass_late(range(3, S))
    planes(ready)

    def hid_at(t, kk):
        return hid.at[t * NT + kk]

    def hx_copy(t, kk):
        return remote(hid_at(t, kk), hid_at(t, kk), hxs.at[kk], hxr.at[kk], "tp", xpeer)

    def hc_copy(t, kk):
        return remote(hid_at(t, kk), hid_at(t, kk), hcs.at[kk], hcr.at[kk], "tp", cpeer)

    def hf_copy(t, kk):
        return remote(hid_at(t, kk), hid_at(t, kk), hfs.at[kk], hfr.at[kk], "tp", cpeer)

    def tile(kk):
        own_gu(0, kk).wait()
        own_gu(1, kk).wait()
        planes(lambda j: gy_copy(j, kk, 1 - g).wait_recv())
        both = jnp.dot(xn[...], gu[kk], preferred_element_type=F32)
        gate, up = both[:, :128], both[:, 128:]
        hid[tp * NT + kk] = (gate / (1.0 + jnp.exp(-gate)) * up).astype(BF16)
        hx_copy(tp, kk).start()
        hc_copy(tp, kk).start()

    def pass_tile(kk):
        hx_copy(xpeer, kk).wait_recv()
        hf_copy(xpeer, kk).start()

    def pass_dn(j, at=range(TP)):
        def some(m):
            for f in at:
                st = lax.rem(tp + TP - f, TP)
                dz_copy(me, tp, j, st, m).wait_recv()
                dy_copy(j, st, g, m).start()

        tiles_of(me, some)

    with_tiles(tile, at=(0,))
    with_tiles(tile, at=(1,))
    planes(pass_dn, at=(1,))
    with_tiles(pass_tile, at=(0,))
    with_tiles(tile, at=range(2, NT))
    for f in range(TP):
        if f == TP // 2:
            with_tiles(pass_tile, at=range(1, NT))
        planes(lambda j: pass_dn(j, (f,)), at=range(2, S))

    def hid_ready(kk):
        hc_copy(cpeer, kk).wait_recv()
        hf_copy(far, kk).wait_recv()

    def rs_copy(j, dst, src):
        return remote(us.at[j, dst], ur.at[j, src], rss.at[j, dst], rsr.at[j, src], "sp", dst)

    def down(j, own=False):
        def some(m):
            if own:
                own_dn(m).wait()
                peers(lambda t: dp_copy(tp, t, m).wait_recv())
            else:
                for t in range(TP):
                    dy_copy(j, t, 1 - g, m).wait_recv()
            x = jnp.concatenate(
                [hid[t * NT + kk] for t in range(TP) for kk in range(m)], axis=1
            )
            us[j] = nt(x, dn[j, :, : TP * m * 128]).astype(BF16).reshape(S, T, Q)

        tiles_of(me, some)
        planes(lambda i: rs_copy(j, i, me).start())

    with_tiles(hid_ready)
    down(me, True)
    for d in range(1, S):
        planes(down, at=(d,))

    def ox_copy(j, t):
        return remote(zq.at[t, j], zq.at[t, j], oxs.at[j], oxr.at[j], "tp", xpeer)

    def oc_copy(j, t):
        return remote(zq.at[t, j], zq.at[t, j], ocs.at[j], ocr.at[j], "tp", cpeer)

    def of_copy(j, t):
        return remote(zq.at[t, j], zq.at[t, j], ofs.at[j], ofr.at[j], "tp", cpeer)

    def settle(j):
        planes(lambda i: rs_copy(j, i, i).wait_recv())
        total = us[j, me].astype(F32)
        for d in range(1, S):
            total += ur[j, lax.rem(me + d, S)].astype(F32)
        zq[tp, j] = total.astype(BF16)
        ox_copy(j, tp).start()
        oc_copy(j, tp).start()

    for j in range(S):
        settle(j)
    for j in range(S):
        ox_copy(j, xpeer).wait_recv()
        of_copy(j, xpeer).start()
    for j in range(S):
        oc_copy(j, cpeer).wait_recv()
        of_copy(j, far).wait_recv()

    def o_out(r):
        rows_r = pl.ds(r * R, R)
        return pltpu.make_async_copy(ov.at[rows_r], out.at[rows_r], outs.at[r])

    for r in range(TP):
        rows_r = pl.ds(r * R, R)
        ffn = jnp.concatenate(
            [zq[t, j, rows_r] for j in range(S) for t in range(TP)], axis=1
        ).astype(F32)
        ov[rows_r] = (xm[me, rows_r].astype(F32) + og[...] * normalize(ffn)).astype(BF16)
        o_out(r).start()

    peers(lambda t: hp_copy(t, tp).wait_send())
    for j in range(S):
        pl.when(j <= me)(lambda: ends(j, lambda c: c.wait_send()))
        ax_copy(j, tp).wait_send()
        ac_copy(j, tp).wait_send()
        af_copy(j, xpeer).wait_send()
        ox_copy(j, tp).wait_send()
        oc_copy(j, tp).wait_send()
        of_copy(j, xpeer).wait_send()
        planes(lambda i: rs_copy(j, i, me).wait_send())

    planes(lambda i: az_copy(me, 0, i).wait_send(), up=False)

    def sent(i):
        for kk in range(NT):
            for w in range(2):

                @pl.when(kk < count(i))
                def _(kk=kk, w=w):
                    gz_copy(w, i, kk, me, i).wait_send()

        def some(m):
            for t in range(TP):
                dz_copy(i, t, me, tp, m).wait_send()

        tiles_of(i, some)
        tiles_of(me, lambda m: [dy_copy(i, t, g, m).wait_send() for t in range(TP)])

    planes(sent)

    def tile_sent(kk):
        planes(lambda j: gy_copy(j, kk, g).wait_send())
        hx_copy(tp, kk).wait_send()
        hc_copy(tp, kk).wait_send()
        hf_copy(xpeer, kk).wait_send()

    with_tiles(tile_sent)
    tiles_of(me, lambda m: peers(lambda t: dp_copy(t, tp, m).wait_send()))
    for r in range(TP):
        o_out(r).wait()


def gathered_call(S, TP, q, k, v, lgt, H, mg, fg, og, res, ow, gw, uw, dw):
    T, hw = q.shape
    D = res.shape[1]
    C, U = gw.shape
    R, Q = T // TP, C // TP
    base, extra = divmod(U // 128, S)
    extras = EXTRA_ORDER(S)[:extra]
    NT = base + (1 if extra else 0)
    vm = pl.BlockSpec(memory_space=pltpu.VMEM)
    hb = pl.BlockSpec(memory_space=pl.ANY)
    dma = pltpu.SemaphoreType.DMA
    pairs = lambda *shape: [dma(shape), dma(shape)]
    return pl.pallas_call(
        functools.partial(gathered, S, TP, H, base, extras),
        out_shape=jax.ShapeDtypeStruct((T, D), BF16),
        in_specs=[vm] * 7 + [hb] * 5,
        out_specs=hb,
        scratch_shapes=[
            pltpu.VMEM((S, T, hw), BF16),
            pltpu.VMEM((S, T, hw), BF16),
            pltpu.VMEM((S,) + lgt.shape, lgt.dtype),
            pltpu.VMEM((H, T, hw // H), F32),
            pltpu.VMEM((H, T, hw // H), F32),
            pltpu.VMEM(ow.shape, BF16),
            pltpu.VMEM((R, D), BF16),
            pltpu.VMEM((TP, R, D), BF16),
            pltpu.VMEM((TP, R, D), BF16),
            pltpu.VMEM((R, D), F32),
            pltpu.VMEM((S, T, D), BF16),
            pltpu.VMEM((S * T, D), BF16),
            pltpu.VMEM((NT, D, 256), BF16),
            pltpu.VMEM((TP * NT, S * T, 128), BF16),
            pltpu.VMEM((S, Q, TP * NT * 128), BF16),
            pltpu.VMEM((S, S, T, Q), BF16),
            pltpu.VMEM((S, S, T, Q), BF16),
            pltpu.VMEM((TP, S, T, Q), BF16),
            pltpu.VMEM((T, D), BF16),
            dma((3 + 2 * NT,)),
            *pairs(S, 3),
            *pairs(TP),
            dma((2, S)),
            dma((S,)),
            *pairs(S),
            *pairs(S),
            *pairs(S),
            *pairs(2, S, NT),
            *pairs(S, NT),
            *pairs(S, TP),
            *pairs(S, TP),
            *pairs(NT),
            *pairs(NT),
            *pairs(NT),
            *pairs(S, S),
            *pairs(S),
            *pairs(S),
            *pairs(S),
            dma((TP,)),
        ],
        compiler_params=pltpu.CompilerParams(
            collective_id=0, has_side_effects=True, vmem_limit_bytes=67043328 - 2**20
        ),
    )(q, k, v, lgt, mg[None], fg[None], og[None], res, ow, gw, uw, dw)


def solution(mesh):
    S, TP, G = mesh.shape["sp"], mesh.shape["tp"], mesh.shape["grp"]

    def shards(q, k, v, lg, res, ow, mg, fg, og, gw, uw, dw):
        T, H = lg.shape
        hw = q.shape[1]
        D = res.shape[1]
        C, U = gw.shape
        R = T // TP
        pieces = max([p for p in range(1, MOST_PIECES + 1) if U % (128 * p) == 0], default=1)
        W = U // pieces
        pad = -H % 8
        lgt = jnp.pad(lg.astype(F32).T, ((0, pad), (0, 0)))
        if U % 128 == 0 and U // 128 >= S and C % (128 * TP) == 0 and T % (16 * TP) == 0 and (TP, G) == (4, 2):
            return gathered_call(S, TP, q, k, v, lg.T, H, mg, fg, og, res, ow, gw, uw, dw)
        vm = pl.BlockSpec(memory_space=pltpu.VMEM)
        hb = pl.BlockSpec(memory_space=pl.ANY)
        dma = pltpu.SemaphoreType.DMA
        return pl.pallas_call(
            functools.partial(kernel, S, TP, H, pieces),
            out_shape=jax.ShapeDtypeStruct((T, D), BF16),
            in_specs=[vm] * 7 + [hb] * 5,
            out_specs=hb,
            scratch_shapes=[
                pltpu.VMEM((S, T, hw), BF16),
                pltpu.VMEM((S, T, hw), BF16),
                pltpu.VMEM((S,) + lgt.shape, F32),
                pltpu.VMEM((H, T, hw // H), F32),
                pltpu.VMEM((H, T, hw // H), F32),
                pltpu.VMEM(ow.shape, BF16),
                pltpu.VMEM(gw.shape, BF16),
                pltpu.VMEM(uw.shape, BF16),
                pltpu.VMEM(dw.shape, BF16),
                pltpu.VMEM((R, D), BF16),
                pltpu.VMEM((TP, R, D), BF16),
                pltpu.VMEM((TP, R, D), BF16),
                pltpu.VMEM((R, D), F32),
                pltpu.VMEM((R, C), F32),
                pltpu.VMEM((S, R, C), BF16),
                pltpu.VMEM((TP, S, R, C), BF16),
                pltpu.VMEM((2, T, W), F32),
                pltpu.VMEM((pieces, S, 2, T, W), BF16),
                pltpu.VMEM((pieces, S + 1, 2, T, W), BF16),
                pltpu.VMEM((pieces, S, T, W), BF16),
                pltpu.VMEM((TP, S, R, C), BF16),
                pltpu.VMEM((TP, S, R, C), BF16),
                pltpu.VMEM((S, R, C), BF16),
                pltpu.VMEM((S, R, C), BF16),
                pltpu.VMEM((TP, R, D), BF16),
                dma((5,)),
                dma((S, 3)),
                dma((S, 3)),
                dma((TP,)),
                dma((TP,)),
                dma((S,)),
                dma((S,)),
                dma((TP, S)),
                dma((TP, S)),
                dma((pieces, S)),
                dma((pieces, S + 1)),
                dma((pieces, S)),
                dma((pieces, S)),
                dma((pieces, S)),
                dma((TP, S)),
                dma((TP, S)),
                dma((S,)),
                dma((S,)),
                dma((TP,)),
                dma((TP,)),
                dma((TP,)),
            ],
            compiler_params=pltpu.CompilerParams(
                collective_id=0, has_side_effects=True, vmem_limit_bytes=67043328 - 2**20
            ),
        )(q, k, v, lgt, mg[None], fg[None], og[None], res, ow, gw, uw, dw)

    placed = (
        P(("grp", "sp"), "tp"),
        P(("grp", "sp"), "tp"),
        P(("grp", "sp"), "tp"),
        P(("grp", "sp"), "tp"),
        P(("grp", "sp"), None),
        P("tp", None),
        P(),
        P(),
        P(),
        P("sp", "tp"),
        P("sp", "tp"),
        P("sp", "tp"),
    )
    return jax.shard_map(
        shards, mesh=mesh, in_specs=placed, out_specs=P(("grp", "sp"), None), check_vma=False
    )
```

```python
import functools

import jax
import jax.numpy as jnp
from jax import lax
from jax.experimental import pallas as pl
from jax.experimental.pallas import tpu as pltpu
from jax.sharding import PartitionSpec as P

epsilon = 1e-06
MESH = pl.DeviceIdType.MESH
F32 = jnp.float32
BF16 = jnp.bfloat16
LAG = 2
MOST_PIECES = 5
EARLY = 2


def KV_ORDER(S):
    return range(S - 1, 0, -1)


def EXTRA_ORDER(S):
    return list(range(S))


def normalize(rows):
    return rows * lax.rsqrt(jnp.mean(rows * rows, axis=-1, keepdims=True) + epsilon)


def each(count, body):
    if count <= 4:
        for i in range(count):
            body(i)
    else:

        def step(i, carry):
            body(i)
            return carry

        lax.fori_loop(0, count, step, 0)


def remote(src, dst, send, recv, axis, peer):
    return pltpu.make_async_remote_copy(
        src_ref=src,
        dst_ref=dst,
        send_sem=send,
        recv_sem=recv,
        device_id={axis: peer},
        device_id_type=MESH,
    )


def nt(a, b):
    return lax.dot_general(a, b, (((1,), (1,)), ((), ())), preferred_element_type=F32)


def kernel(
    S, TP, H, pieces,
    q, k, v, lg, mg, fg, og, res, ow, gw, uw, dw,
    out,
    kb, vb, lb, acc, run, owv, gwv, uwv, dwv, resv,
    hs, hr, mid, zs_sum, ns, na, tmp, gs, gr, hall, us, ur, zs, zr, oall,
    loc, kvs, kvr, hss, hrs, n1s, n1r, n2s, n2r, gss, grs, hars, hals, har,
    upss, upr, zss, zrs, oss, ors, outs,
):
    me, tp = lax.axis_index("sp"), lax.axis_index("tp")
    T = q.shape[0]
    hd = q.shape[1] // H
    D = out.shape[1]
    R, C = T // TP, D // S
    right, left = lax.rem(me + 1, S), lax.rem(me + S - 1, S)

    my_rows = pl.ds(pl.multiple_of(tp * R, R), R)
    loads = [
        pltpu.make_async_copy(a, b, loc.at[i])
        for i, (a, b) in enumerate(
            [(ow, owv), (res.at[my_rows], resv), (gw, gwv), (uw, uwv), (dw, dwv)]
        )
    ]
    for c in loads:
        c.start()

    barrier = pltpu.get_barrier_semaphore()
    for f in range(1, S):
        pl.semaphore_signal(barrier, inc=1, device_id={"sp": lax.rem(me + f, S)}, device_id_type=MESH)
    for f in range(1, TP):
        pl.semaphore_signal(barrier, inc=1, device_id={"tp": lax.rem(tp + f, TP)}, device_id_type=MESH)
    pl.semaphore_wait(barrier, S + TP - 2)

    def kv_copies(b, own):
        srcs = (k, v, lg) if own else (kb.at[b], vb.at[b], lb.at[b])
        return [
            remote(src, dst.at[b], kvs.at[b, i], kvr.at[b, i], "sp", right)
            for i, (src, dst) in enumerate(zip(srcs, (kb, vb, lb)))
        ]

    @pl.when(me < S - 1)
    def _():
        for c in kv_copies(me, True):
            c.start()

    rows = lax.broadcasted_iota(jnp.int32, (T, T), 0)
    cols = lax.broadcasted_iota(jnp.int32, (T, T), 1)
    causal = cols < rows
    later = (rows > cols).astype(F32)

    def block(kk, vv, ll, diag):
        for h in range(H):
            span = slice(h * hd, (h + 1) * hd)
            s = nt(q[:, span], kk[:, span]) * (hd**-0.5) + ll[h : h + 1, :]
            soft = jnp.log1p(jnp.exp(-jnp.abs(s)))
            keep = jnp.minimum(-s, 0.0) - soft
            logsig = jnp.minimum(s, 0.0) - soft
            if diag:
                keep = jnp.where(causal, keep, 0.0)
            within = jnp.dot(
                keep, later, preferred_element_type=F32, precision=lax.Precision.HIGHEST
            )
            stick = jnp.exp(logsig + within)
            if diag:
                stick = jnp.where(causal, stick, 0.0)
            part = jnp.dot(stick.astype(BF16), vv[:, span], preferred_element_type=F32)
            total = jnp.broadcast_to(jnp.sum(keep, axis=-1, keepdims=True), (T, hd))
            if diag:
                acc[h] = part
                run[h] = total
            else:
                acc[h] += jnp.exp(run[h]) * part
                run[h] += total

    block(k[...], v[...], lg[...], True)

    def earlier(i):
        b = me - 1 - i

        @pl.when(b >= 0)
        def _():
            for c in kv_copies(b, False):
                c.wait_recv()

            @pl.when(me < S - 1)
            def _():
                for c in kv_copies(b, False):
                    c.start()

            block(kb[b], vb[b], lb[b], False)

    each(S - 1, earlier)

    attended = jnp.concatenate([acc[h] for h in range(H)], axis=1).astype(BF16)
    loads[0].wait()
    width = 512 if D % 512 == 0 else D
    for c0 in range(0, D, width):
        piece = jnp.dot(attended, owv[:, c0 : c0 + width], preferred_element_type=F32)
        hs[:, :, c0 : c0 + width] = piece.astype(BF16).reshape(TP, R, width)

    def hp_copy(t, slot):
        return remote(hs.at[t], hr.at[slot], hss.at[t], hrs.at[slot], "tp", t)

    def others(count, own, body):
        def go(i):
            body(lax.rem(own + 1 + i, count))

        each(count - 1, go)

    others(TP, tp, lambda t: hp_copy(t, tp).start())
    mid[...] = hs[tp].astype(F32)

    def add_hp(t):
        hp_copy(t, t).wait_recv()
        mid[...] += hr[t].astype(F32)

    others(TP, tp, add_hp)
    loads[1].wait()
    mixed = mid[...].astype(BF16).astype(F32)
    middle = (resv[...].astype(F32) + mg[...] * normalize(mixed)).astype(BF16).astype(F32)
    mid[...] = middle
    normed = (fg[...] * normalize(middle)).astype(BF16)
    for j in range(S):
        ns[j] = normed[:, j * C : (j + 1) * C]

    def n1_copy(j, slot):
        return remote(ns.at[j], na.at[tp, slot], n1s.at[j], n1r.at[slot], "sp", j)

    def n2_copy(t, slot, s):
        return remote(na.at[tp, s], na.at[slot, s], n2s.at[t, s], n2r.at[slot, s], "tp", t)

    others(S, me, lambda j: n1_copy(j, me).start())
    na[tp, me] = ns[me]
    others(TP, tp, lambda t: n2_copy(t, tp, me).start())

    def pass_on(s):
        n1_copy(s, s).wait_recv()
        others(TP, tp, lambda t: n2_copy(t, tp, s).start())

    others(S, me, pass_on)
    for c in loads[2:4]:
        c.wait()

    def arrive(s):
        others(TP, tp, lambda t: remote(na.at[tp, s], na.at[t, s], n2s.at[t, s], n2r.at[t, s], "tp", t).wait_recv())

    W = gs.shape[-1]
    lag = LAG

    def partial(p, j):
        @pl.when(p == 0)
        def _():
            arrive(j)

        x = na[:, j].reshape(T, C)
        units = pl.ds(pl.multiple_of(p * W, W), W)
        tmp[0] = jnp.dot(x, gwv[:, units], preferred_element_type=F32)
        tmp[1] = jnp.dot(x, uwv[:, units], preferred_element_type=F32)

    def g_copy(p, j, slot, peer):
        return remote(gs.at[p, j], gr.at[p, slot], gss.at[p, j], grs.at[p, slot], "sp", peer)

    def chain(p, j, first, slot, peer):
        partial(p, j)

        @pl.when(first)
        def _():
            gs[p, j] = tmp[...].astype(BF16)

        @pl.when(jnp.logical_not(first))
        def _():
            g_copy(p, j, j, peer).wait_recv()
            gs[p, j] = (tmp[...] + gr[p, j].astype(F32)).astype(BF16)

        g_copy(p, j, slot, peer).start()

    def h_right(p, b):
        return remote(hall.at[p, b], hall.at[p, b], hars.at[p, b], har.at[p, b], "sp", right)

    def h_left(p, b):
        return remote(hall.at[p, b], hall.at[p, b], hals.at[p, b], har.at[p, b], "sp", left)

    def cut(at):
        return lax.div(at, S - 1), lax.rem(at, S - 1)

    def reduce_step(g):
        at_right = g - me * lag
        at_left = g - (S - 1 - me) * lag

        @pl.when((at_right >= 0) & (at_right < pieces * (S - 1)))
        def _():
            p, tau = cut(at_right)

            @pl.when(S - 1 - tau > me)
            def _():
                chain(p, S - 1 - tau, me == 0, S - 1 - tau, right)

        @pl.when((at_left >= 0) & (at_left < pieces * (S - 1)))
        def _():
            p, j = cut(at_left)

            @pl.when(j < me)
            def _():
                chain(p, j, me == S - 1, lax.select(j == me - 1, S, j), left)

    def finish(p):
        partial(p, me)

        @pl.when(me > 0)
        def _():
            g_copy(p, me, me, left).wait_recv()
            tmp[...] += gr[p, me].astype(F32)

        @pl.when(me < S - 1)
        def _():
            g_copy(p, me, S, right).wait_recv()
            tmp[...] += gr[p, S].astype(F32)

        gate = tmp[0]
        hall[p, me] = (gate / (1.0 + jnp.exp(-gate)) * tmp[1]).astype(BF16)

        @pl.when(me < S - 1)
        def _():
            h_right(p, me).start()

        @pl.when(me > 0)
        def _():
            h_left(p, me).start()

    def spread(p, i, then):
        lo, hi = me - 1 - i, me + 1 + i

        @pl.when(lo >= 0)
        def _():
            h_right(p, lo).wait_recv()

            @pl.when(me < S - 1)
            def _():
                h_right(p, lo).start()

            then(lo)

        @pl.when(hi < S)
        def _():
            h_left(p, hi).wait_recv()

            @pl.when(me > 0)
            def _():
                h_left(p, hi).start()

            then(hi)

    def step(g, carry):
        reduce_step(g)
        at = g - (S - 1) * lag
        p, tau = cut(at)

        @pl.when((at >= 0) & (tau == 0) & (p < pieces))
        def _():
            finish(p)

        def gather(i, carry):
            at_i = at - (i + 1) * lag
            p, tau = cut(at_i)

            @pl.when((at_i >= 0) & (tau == 0) & (p < pieces - 1))
            def _():
                spread(p, i, lambda b: None)

            return carry

        return lax.fori_loop(0, S - 1, gather, carry)

    steps = (S - 1) * (lag + max(pieces - 1, pieces - 2 + lag)) + 1
    lax.fori_loop(0, steps, step, 0)

    def up_copy(t, slot, b):
        return remote(us.at[t, b], ur.at[slot, b], upss.at[t, b], upr.at[slot, b], "tp", t)

    def down(b):
        rows_b = jnp.concatenate([hall[p, b] for p in range(pieces)], axis=1)
        us[:, b] = nt(rows_b, dwv[...]).astype(BF16).reshape(TP, R, C)
        others(TP, tp, lambda t: up_copy(t, tp, b).start())

    def z_copy(b, slot):
        return remote(zs.at[b], zr.at[slot], zss.at[b], zrs.at[slot], "sp", b)

    def settle(b):
        def add(t):
            up_copy(t, t, b).wait_recv()
            zs_sum[...] += ur[t, b].astype(F32)

        zs_sum[...] = us[tp, b].astype(F32)
        others(TP, tp, add)
        zs[b] = zs_sum[...].astype(BF16)

        @pl.when(b != me)
        def _():
            z_copy(b, me).start()

    loads[4].wait()
    down(me)

    def last(i, carry):
        spread(pieces - 1, i, down)
        return carry

    lax.fori_loop(0, S - 1, last, 0)
    others(S, me, settle)
    settle(me)
    zr[me] = zs[me]
    others(S, me, lambda s: z_copy(s, s).wait_recv())
    ffn = jnp.concatenate([zr[s] for s in range(S)], axis=1).astype(F32)
    oall[tp] = (mid[...] + og[...] * normalize(ffn)).astype(BF16)

    def o_copy(t, slot):
        return remote(oall.at[tp], oall.at[slot], oss.at[t], ors.at[slot], "tp", t)

    def o_out(t):
        return pltpu.make_async_copy(
            oall.at[t], out.at[pl.ds(pl.multiple_of(t * R, R), R)], outs.at[t]
        )

    others(TP, tp, lambda t: o_copy(t, tp).start())
    o_out(tp).start()

    def o_in(t):
        remote(oall.at[tp], oall.at[t], oss.at[t], ors.at[t], "tp", t).wait_recv()
        o_out(t).start()

    others(TP, tp, o_in)
    each(TP, lambda t: o_out(t).wait())

    @pl.when(me < S - 1)
    def _():
        def sent(b):
            @pl.when(b <= me)
            def _():
                for c in kv_copies(b, False):
                    c.wait_send()
                each(pieces, lambda p: h_right(p, b).wait_send())

        each(S, sent)

    @pl.when(me > 0)
    def _():
        def sent(b):
            @pl.when(b >= me)
            def _():
                each(pieces, lambda p: h_left(p, b).wait_send())

        each(S, sent)

    def sp_sent(j):
        n1_copy(j, me).wait_send()
        z_copy(j, me).wait_send()
        each(pieces, lambda p: g_copy(p, j, j, right).wait_send())

    others(S, me, sp_sent)

    def tp_sent(t):
        hp_copy(t, tp).wait_send()
        o_copy(t, tp).wait_send()

        def inner(s):
            n2_copy(t, tp, s).wait_send()
            up_copy(t, tp, s).wait_send()

        each(S, inner)

    others(TP, tp, tp_sent)


def gathered(
    S, TP, H, base, extras,
    q, k, v, lg, mg, fg, og, res, ow, gw, uw, dw,
    out,
    kb, vb, lb, acc, run, owv, resv, hs, hr, mid, xm, xn, gu, hid, dn, us, ur, zq, ov,
    loc, kvs, kvr, hss, hrs, azs, azr, axs, axr, acs, acr,
    gzs, gzr, gys, gyr, dzs, dzr, dys, dyr, hxs, hxr, hcr,
    rss, rsr, oxs, oxr, ocs, ocr, outs,
):
    me, tp, g = lax.axis_index("sp"), lax.axis_index("tp"), lax.axis_index("grp")
    T = q.shape[0]
    hd = q.shape[1] // H
    D = out.shape[1]
    R, C = T // TP, D // S
    NT = gu.shape[0]
    half, Q = C // 2, C // TP
    xpeer = lax.rem(tp + 2, TP)
    cpeer = tp + 1 - 2 * lax.rem(tp, 2)
    far = lax.rem(cpeer + 2, TP)

    def count(i):
        c = base
        for p in extras:
            c = c + jnp.where(i == p, 1, 0)
        return c

    def first(i):
        c = i * base
        for p in extras:
            c = c + jnp.where(i > p, 1, 0)
        return c

    def tiles_of(i, body):
        c = count(i)
        for m in sorted({base, base + 1} if extras else {base}):

            @pl.when(c == m)
            def _(m=m):
                body(m)

    n_me = count(me)
    my_rows = pl.ds(pl.multiple_of(tp * R, R), R)
    load_ow = pltpu.make_async_copy(ow, owv, loc.at[0])
    load_res = pltpu.make_async_copy(res.at[my_rows], resv, loc.at[1])
    load_ow.start()
    load_res.start()

    def drain(ref, sem):
        remote(ref, ref, sem, sem, "tp", xpeer).wait_recv()

    def own_gu(w, kk):
        lanes = pl.ds(pl.multiple_of((first(me) + kk) * 128, 128), 128)
        rows = pl.ds(pl.multiple_of(me * C, C), C)
        return pltpu.make_async_copy(
            (gw, uw)[w].at[:, lanes], gu.at[kk, rows, pl.ds(w * 128, 128)], loc.at[3 + w * NT + kk]
        )

    def own_dn(m):
        lanes = pl.ds(pl.multiple_of(first(me) * 128, 128), m * 128)
        rows = pl.ds(pl.multiple_of(tp * Q, Q), Q)
        to = pl.ds(pl.multiple_of(tp * (m * 128), 128), m * 128)
        return pltpu.make_async_copy(dw.at[rows, lanes], dn.at[me, :, to], loc.at[2])

    def with_tiles(body, at=range(NT)):
        for kk in at:

            @pl.when(kk < n_me)
            def _(kk=kk):
                body(kk)

    def load_own(kk):
        own_gu(0, kk).start()
        own_gu(1, kk).start()

    with_tiles(load_own)
    tiles_of(me, lambda m: own_dn(m).start())

    barrier = pltpu.get_barrier_semaphore()

    def greet(i):
        for f in range(TP):

            @pl.when((i != 0) | (f != 0))
            def _(f=f):
                pl.semaphore_signal(
                    barrier,
                    inc=1,
                    device_id={"sp": lax.rem(me + i, S), "tp": lax.rem(tp + f, TP)},
                    device_id_type=MESH,
                )

    for i in range(S):
        greet(i)
    pl.semaphore_signal(barrier, inc=1, device_id={"grp": 1 - g}, device_id_type=MESH)
    pl.semaphore_wait(barrier, S * TP)

    def planes(body, up=True, down=True, at=range(1, S)):
        for d in at:
            if down:

                @pl.when(me - d >= 0)
                def _(d=d):
                    body(me - d)

            if up:

                @pl.when(me + d < S)
                def _(d=d):
                    body(me + d)

    def kv_copies(b, dst):
        return [
            remote(src, to.at[b], kvs.at[dst, i // 2], kvr.at[b, i // 2], "sp", dst)
            for i, (src, to) in enumerate(zip((k, v, lg), (kb, vb, lb)))
        ]

    def send_kv(i):
        for c in kv_copies(me, i):
            c.start()

    planes(send_kv, down=False, at=KV_ORDER(S))

    def gz_copy(w, i, kk, src, dst):
        lanes = pl.ds(pl.multiple_of((first(i) + kk) * 128, 128), 128)
        rows = pl.ds(pl.multiple_of(src * C + g * half, half), half)
        return remote(
            (gw, uw)[w].at[pl.ds(pl.multiple_of(g * half, half), half), lanes],
            gu.at[kk, rows, pl.ds(w * 128, 128)],
            gzs.at[i, kk],
            gzr.at[src, kk],
            "sp",
            dst,
        )

    def gy_copy(j, kk, h):
        r = gu.at[kk, pl.ds(pl.multiple_of(j * C + h * half, half), half)]
        return remote(r, r, gys.at[kk], gyr.at[kk], "grp", 1 - g)

    def send_gu(w, kk, **sides):
        def one(i):
            @pl.when(kk < count(i))
            def _():
                gz_copy(w, i, kk, me, i).start()

        planes(one, **sides)

    def dz_copy(i, t, src, st, m):
        lanes = pl.ds(pl.multiple_of(first(i) * 128, 128), m * 128)
        rows = pl.ds(pl.multiple_of(t * Q + g * (Q // 2), Q // 2), Q // 2)
        return pltpu.make_async_remote_copy(
            src_ref=dw.at[rows, lanes],
            dst_ref=dn.at[
                src,
                pl.ds(pl.multiple_of(g * (Q // 2), Q // 2), Q // 2),
                pl.ds(pl.multiple_of(st * (m * 128), 128), m * 128),
            ],
            send_sem=dzs.at[i],
            recv_sem=dzr.at[src, st],
            device_id={"sp": i, "tp": t},
            device_id_type=MESH,
        )

    def dp_copy(t, st, m):
        lanes = pl.ds(pl.multiple_of(first(me) * 128, 128), m * 128)
        rows = pl.ds(pl.multiple_of(t * Q, Q), Q)
        return remote(
            dw.at[rows, lanes],
            dn.at[me, :, pl.ds(pl.multiple_of(st * (m * 128), 128), m * 128)],
            dzs.at[me],
            dzr.at[me, 0],
            "tp",
            t,
        )

    def dy_copy(j, st, h, m):
        r = dn.at[
            j,
            pl.ds(pl.multiple_of(h * (Q // 2), Q // 2), Q // 2),
            pl.ds(pl.multiple_of(st * (m * 128), 128), m * 128),
        ]
        return remote(r, r, dys.at[j], dyr.at[j], "grp", 1 - g)

    def peers(body):
        for f in range(1, TP):
            body(lax.rem(tp + f, TP))

    def send_dn(i):
        def some(m):
            for t in (tp, cpeer, xpeer, far):
                dz_copy(i, t, me, tp, m).start()

        tiles_of(i, some)

    tiles_of(me, lambda m: peers(lambda t: dp_copy(t, tp, m).start()))
    for kk in range(min(EARLY, NT)):
        send_gu(0, kk, up=False)
        send_gu(1, kk, up=False)

    rows = lax.broadcasted_iota(jnp.int32, (T, T), 0)
    cols = lax.broadcasted_iota(jnp.int32, (T, T), 1)
    causal = cols < rows
    later = (rows > cols).astype(F32)

    def block(kk, vv, ll, diag):
        for h in range(H):
            span = slice(h * hd, (h + 1) * hd)
            s = nt(q[:, span], kk[:, span]) * (hd**-0.5) + ll[h : h + 1, :].astype(F32)
            soft = jnp.log1p(jnp.exp(-jnp.abs(s)))
            keep = jnp.minimum(-s, 0.0) - soft
            logsig = jnp.minimum(s, 0.0) - soft
            if diag:
                keep = jnp.where(causal, keep, 0.0)
            within = jnp.dot(
                keep, later, preferred_element_type=F32, precision=lax.Precision.HIGHEST
            )
            stick = jnp.exp(logsig + within)
            if diag:
                stick = jnp.where(causal, stick, 0.0)
            part = jnp.dot(stick.astype(BF16), vv[:, span], preferred_element_type=F32)
            total = jnp.broadcast_to(jnp.sum(keep, axis=-1, keepdims=True), (T, hd))
            if diag:
                acc[h] = part
                run[h] = total
            else:
                acc[h] += jnp.exp(run[h]) * part
                run[h] += total

    block(k[...], v[...], lg[...], True)

    def earlier(i):
        b = me - 1 - i

        @pl.when(b >= 0)
        def _():
            drain(kb.at[pl.ds(0, 2)], kvr.at[b, 0])
            drain(lb.at[0], kvr.at[b, 1])
            block(kb[b], vb[b], lb[b], False)

    each(S - 1, earlier)

    attended = jnp.concatenate([acc[h] for h in range(H)], axis=1).astype(BF16)
    load_ow.wait()
    width = 512 if D % 512 == 0 else D
    for c0 in range(0, D, width):
        piece = jnp.dot(attended, owv[:, c0 : c0 + width], preferred_element_type=F32)
        hs[:, :, c0 : c0 + width] = piece.astype(BF16).reshape(TP, R, width)

    def hp_copy(t, slot):
        return remote(hs.at[t], hr.at[slot], hss.at[0], hrs.at[0], "tp", t)

    peers(lambda t: hp_copy(t, tp).start())
    mid[...] = hs[tp].astype(F32)
    planes(
        lambda i: [drain(kb.at[pl.ds(0, 2)], kvs.at[i, 0]), drain(lb.at[0], kvs.at[i, 1])],
        down=False,
    )
    send_gu(0, 0, down=False)
    send_gu(1, 0, down=False)

    drain(hr.at[pl.ds(0, TP - 1)], hrs.at[0])

    def add_hp(t):
        mid[...] += hr[t].astype(F32)

    peers(add_hp)
    load_res.wait()
    mixed = mid[...].astype(BF16).astype(F32)
    xm[me, my_rows] = (resv[...].astype(F32) + mg[...] * normalize(mixed)).astype(BF16)

    def piece_of(j, t):
        return xm.at[j, pl.ds(pl.multiple_of(t * R, R), R)]

    def az_copy(j, way, dst):
        r = piece_of(j, tp)
        return remote(r, r, azs.at[way, j if way else dst], azr.at[j], "sp", dst)

    def ends(j, body):
        @pl.when((j <= me) & (me < S - 1))
        def _():
            body(az_copy(j, 1, me + 1))

    def ax_copy(j, t):
        return remote(piece_of(j, t), piece_of(j, t), axs.at[0], axr.at[j], "tp", xpeer)

    def ac_copy(j, t):
        return remote(piece_of(j, t), piece_of(j, t), acs.at[0], acr.at[j], "tp", cpeer)

    def af_copy(j, t):
        return remote(piece_of(j, t), piece_of(j, t), acs.at[0], acr.at[j], "tp", cpeer)

    ends(me, lambda c: c.start())
    planes(lambda i: az_copy(me, 0, i).start(), up=False, at=range(S - 1, 0, -1))
    ax_copy(me, tp).start()
    ac_copy(me, tp).start()

    def late_down():
        for w in range(2):
            for kk in range(EARLY, NT):
                send_gu(w, kk, up=False)

    pl.when(me < S - 1)(late_down)

    def pass_gu(kk, **sides):
        def one(j):
            drain(gu.at[kk, pl.ds(0, half)], gzr.at[j, kk])
            gy_copy(j, kk, g).start()

        @pl.when(kk < n_me)
        def _():
            planes(one, **sides)

    def spread(j):
        az_copy(j, 1, me).wait_recv()
        ends(j, lambda c: c.start())
        ax_copy(j, tp).start()
        ac_copy(j, tp).start()

    def hand_on(j):
        ax_copy(j, xpeer).wait_recv()
        af_copy(j, xpeer).start()

    def ready(j):
        drain(xm.at[j, pl.ds(0, 2 * R)], acr.at[j])
        for r0 in range(0, T, R):
            rows_f = xm[j, pl.ds(r0, R)].astype(F32)
            at = pl.ds(pl.multiple_of(j * T + r0, R), R)
            xn[at] = (fg[...] * normalize(rows_f)).astype(BF16)

    def pass_late(at):
        for kk in range(2, NT):
            pass_gu(kk, at=at)

    pass_gu(0)
    for kk in range(1, NT):
        send_gu(0, kk, down=False)
        send_gu(1, kk, down=False)
    pass_gu(1, down=False)
    hand_on(me)
    planes(spread, at=(1,))
    planes(hand_on, at=(1,))
    pl.when(me == S - 1)(late_down)
    ready(me)
    planes(spread, at=(2,))
    pass_late((1,))
    planes(hand_on, at=(2,))
    planes(spread, at=range(3, S))
    pass_late((2,))
    planes(send_dn)
    planes(hand_on, at=range(3, S))
    pass_gu(1, up=False)
    pass_late(range(3, S))
    planes(ready)

    def hid_at(t, kk):
        return hid.at[t * NT + kk]

    def hx_copy(t, kk):
        return remote(hid_at(t, kk), hid_at(t, kk), hxs.at[kk], hxr.at[kk], "tp", xpeer)

    def hc_copy(t, kk):
        return remote(hid_at(t, kk), hid_at(t, kk), hxs.at[kk], hcr.at[kk], "tp", cpeer)

    def hf_copy(t, kk):
        return remote(hid_at(t, kk), hid_at(t, kk), hxs.at[kk], hcr.at[kk], "tp", cpeer)

    def tile(kk):
        own_gu(0, kk).wait()
        own_gu(1, kk).wait()
        drain(gu.at[kk, pl.ds(0, (S - 1) * half)], gyr.at[kk])
        both = jnp.dot(xn[...], gu[kk], preferred_element_type=F32)
        gate, up = both[:, :128], both[:, 128:]
        hid[tp * NT + kk] = (gate / (1.0 + jnp.exp(-gate)) * up).astype(BF16)
        hx_copy(tp, kk).start()
        hc_copy(tp, kk).start()

    def pass_tile(kk):
        hx_copy(xpeer, kk).wait_recv()
        hf_copy(xpeer, kk).start()

    def pass_dn(j, at=range(TP)):
        def some(m):
            for f in at:
                st = (tp, cpeer, xpeer, far)[f]
                dz_copy(me, tp, j, st, m).wait_recv()
                dy_copy(j, st, g, m).start()

        tiles_of(me, some)

    with_tiles(tile, at=(0,))
    with_tiles(tile, at=(1,))
    planes(pass_dn, at=(1,))
    with_tiles(pass_tile, at=(0,))
    with_tiles(tile, at=range(2, NT))
    with_tiles(pass_tile, at=(1,))
    for f in range(TP):
        if f == TP - 1:
            with_tiles(pass_tile, at=range(2, NT))
        planes(lambda j: pass_dn(j, (f,)), at=range(2, S))

    def hid_ready(kk):
        drain(hid.at[pl.ds(0, 2)], hcr.at[kk])

    def rs_copy(j, dst, src):
        return remote(us.at[j, dst], ur.at[j, src], rss.at[0], rsr.at[j], "sp", dst)

    def down(j, own=False):
        def some(m):
            if own:
                own_dn(m).wait()
                drain(dn.at[me, :, pl.ds(0, (TP - 1) * m * 128)], dzr.at[me, 0])
            else:
                drain(dn.at[j, pl.ds(0, Q // 2), pl.ds(0, TP * m * 128)], dyr.at[j])
            x = jnp.concatenate(
                [hid[t * NT + kk] for t in range(TP) for kk in range(m)], axis=1
            )
            us[j] = nt(x, dn[j, :, : TP * m * 128]).astype(BF16).reshape(S, T, Q)

        tiles_of(me, some)
        planes(lambda i: rs_copy(j, i, me).start())

    with_tiles(hid_ready)
    down(me, True)
    for d in range(1, S):
        planes(down, at=(d,))

    def ox_copy(j, t):
        return remote(zq.at[t, j], zq.at[t, j], oxs.at[0], oxr.at[j], "tp", xpeer)

    def oc_copy(j, t):
        return remote(zq.at[t, j], zq.at[t, j], ocs.at[0], ocr.at[0], "tp", cpeer)

    def of_copy(j, t):
        return remote(zq.at[t, j], zq.at[t, j], ocs.at[0], ocr.at[0], "tp", cpeer)

    def settle(j):
        drain(ur.at[j, pl.ds(0, S - 1)], rsr.at[j])
        total = us[j, me].astype(F32)
        for d in range(1, S):
            total += ur[j, lax.rem(me + d, S)].astype(F32)
        zq[tp, j] = total.astype(BF16)
        ox_copy(j, tp).start()
        oc_copy(j, tp).start()

    order = sorted(range(S), key=lambda j: abs(2 * j + 1 - S))
    for j in order:
        settle(j)
    for j in order:
        ox_copy(j, xpeer).wait_recv()
        of_copy(j, xpeer).start()
    drain(zq.at[pl.ds(0, 2)], ocr.at[0])

    def o_out(r):
        rows_r = pl.ds(r * R, R)
        return pltpu.make_async_copy(ov.at[rows_r], out.at[rows_r], outs.at[0])

    for r in range(TP):
        rows_r = pl.ds(r * R, R)
        ffn = jnp.concatenate(
            [zq[t, j, rows_r] for j in range(S) for t in range(TP)], axis=1
        ).astype(F32)
        ov[rows_r] = (xm[me, rows_r].astype(F32) + og[...] * normalize(ffn)).astype(BF16)
        o_out(r).start()

    drain(hs.at[pl.ds(0, TP - 1)], hss.at[0])
    for j in range(S):
        pl.when(j <= me)(lambda: ends(j, lambda c: c.wait_send()))

    drain(xm.at[:, pl.ds(0, R)], axs.at[0])
    drain(xm.at[:, pl.ds(0, 2 * R)], acs.at[0])
    drain(zq.at[0], oxs.at[0])
    drain(zq.at[pl.ds(0, 2)], ocs.at[0])
    drain(us.at[pl.ds(0, S - 1)], rss.at[0])
    planes(lambda i: az_copy(me, 0, i).wait_send(), up=False)

    def sent(i):
        for kk in range(NT):

            @pl.when(kk < count(i))
            def _(kk=kk):
                drain(gu.at[kk, pl.ds(0, half)], gzs.at[i, kk])

        def some(m):
            drain(dn.at[0, pl.ds(0, Q // 2), pl.ds(0, TP * m * 128)], dzs.at[i])

        tiles_of(i, some)
        tiles_of(me, lambda m: drain(dn.at[i, pl.ds(0, Q // 2), pl.ds(0, TP * m * 128)], dys.at[i]))

    planes(sent)

    def tile_sent(kk):
        drain(gu.at[kk, pl.ds(0, (S - 1) * half)], gys.at[kk])
        drain(hid.at[pl.ds(0, 3)], hxs.at[kk])

    with_tiles(tile_sent)
    tiles_of(me, lambda m: drain(dn.at[me, :, pl.ds(0, (TP - 1) * m * 128)], dzs.at[me]))
    pltpu.make_async_copy(ov, out, outs.at[0]).wait()


def gathered_call(S, TP, q, k, v, lgt, H, mg, fg, og, res, ow, gw, uw, dw):
    T, hw = q.shape
    D = res.shape[1]
    C, U = gw.shape
    R, Q = T // TP, C // TP
    base, extra = divmod(U // 128, S)
    extras = EXTRA_ORDER(S)[:extra]
    NT = base + (1 if extra else 0)
    vm = pl.BlockSpec(memory_space=pltpu.VMEM)
    hb = pl.BlockSpec(memory_space=pl.ANY)
    dma = pltpu.SemaphoreType.DMA
    pairs = lambda *shape: [dma(shape), dma(shape)]
    return pl.pallas_call(
        functools.partial(gathered, S, TP, H, base, extras),
        out_shape=jax.ShapeDtypeStruct((T, D), BF16),
        in_specs=[vm] * 7 + [hb] * 5,
        out_specs=hb,
        scratch_shapes=[
            pltpu.VMEM((S, T, hw), BF16),
            pltpu.VMEM((S, T, hw), BF16),
            pltpu.VMEM((S,) + lgt.shape, lgt.dtype),
            pltpu.VMEM((H, T, hw // H), F32),
            pltpu.VMEM((H, T, hw // H), F32),
            pltpu.VMEM(ow.shape, BF16),
            pltpu.VMEM((R, D), BF16),
            pltpu.VMEM((TP, R, D), BF16),
            pltpu.VMEM((TP, R, D), BF16),
            pltpu.VMEM((R, D), F32),
            pltpu.VMEM((S, T, D), BF16),
            pltpu.VMEM((S * T, D), BF16),
            pltpu.VMEM((NT, D, 256), BF16),
            pltpu.VMEM((TP * NT, S * T, 128), BF16),
            pltpu.VMEM((S, Q, TP * NT * 128), BF16),
            pltpu.VMEM((S, S, T, Q), BF16),
            pltpu.VMEM((S, S, T, Q), BF16),
            pltpu.VMEM((TP, S, T, Q), BF16),
            pltpu.VMEM((T, D), BF16),
            dma((3 + 2 * NT,)),
            *pairs(S, 2),
            *pairs(1),
            dma((2, S)),
            dma((S,)),
            dma((1,)),
            dma((S,)),
            dma((1,)),
            dma((S,)),
            *pairs(S, NT),
            *pairs(NT),
            dma((S,)),
            dma((S, TP)),
            *pairs(S),
            dma((NT,)),
            dma((NT,)),
            dma((NT,)),
            dma((1,)),
            dma((S,)),
            dma((1,)),
            dma((S,)),
            *pairs(1),
            dma((1,)),
        ],
        compiler_params=pltpu.CompilerParams(
            collective_id=0, has_side_effects=True, vmem_limit_bytes=67043328 - 2**20
        ),
    )(q, k, v, lgt, mg[None], fg[None], og[None], res, ow, gw, uw, dw)


def solution(mesh):
    S, TP, G = mesh.shape["sp"], mesh.shape["tp"], mesh.shape["grp"]

    def shards(q, k, v, lg, res, ow, mg, fg, og, gw, uw, dw):
        T, H = lg.shape
        hw = q.shape[1]
        D = res.shape[1]
        C, U = gw.shape
        R = T // TP
        pieces = max([p for p in range(1, MOST_PIECES + 1) if U % (128 * p) == 0], default=1)
        W = U // pieces
        pad = -H % 8
        lgt = jnp.pad(lg.astype(F32).T, ((0, pad), (0, 0)))
        if U % 128 == 0 and U // 128 >= S and C % (128 * TP) == 0 and T % (16 * TP) == 0 and (TP, G) == (4, 2):
            return gathered_call(S, TP, q, k, v, lg.T, H, mg, fg, og, res, ow, gw, uw, dw)
        vm = pl.BlockSpec(memory_space=pltpu.VMEM)
        hb = pl.BlockSpec(memory_space=pl.ANY)
        dma = pltpu.SemaphoreType.DMA
        return pl.pallas_call(
            functools.partial(kernel, S, TP, H, pieces),
            out_shape=jax.ShapeDtypeStruct((T, D), BF16),
            in_specs=[vm] * 7 + [hb] * 5,
            out_specs=hb,
            scratch_shapes=[
                pltpu.VMEM((S, T, hw), BF16),
                pltpu.VMEM((S, T, hw), BF16),
                pltpu.VMEM((S,) + lgt.shape, F32),
                pltpu.VMEM((H, T, hw // H), F32),
                pltpu.VMEM((H, T, hw // H), F32),
                pltpu.VMEM(ow.shape, BF16),
                pltpu.VMEM(gw.shape, BF16),
                pltpu.VMEM(uw.shape, BF16),
                pltpu.VMEM(dw.shape, BF16),
                pltpu.VMEM((R, D), BF16),
                pltpu.VMEM((TP, R, D), BF16),
                pltpu.VMEM((TP, R, D), BF16),
                pltpu.VMEM((R, D), F32),
                pltpu.VMEM((R, C), F32),
                pltpu.VMEM((S, R, C), BF16),
                pltpu.VMEM((TP, S, R, C), BF16),
                pltpu.VMEM((2, T, W), F32),
                pltpu.VMEM((pieces, S, 2, T, W), BF16),
                pltpu.VMEM((pieces, S + 1, 2, T, W), BF16),
                pltpu.VMEM((pieces, S, T, W), BF16),
                pltpu.VMEM((TP, S, R, C), BF16),
                pltpu.VMEM((TP, S, R, C), BF16),
                pltpu.VMEM((S, R, C), BF16),
                pltpu.VMEM((S, R, C), BF16),
                pltpu.VMEM((TP, R, D), BF16),
                dma((5,)),
                dma((S, 3)),
                dma((S, 3)),
                dma((TP,)),
                dma((TP,)),
                dma((S,)),
                dma((S,)),
                dma((TP, S)),
                dma((TP, S)),
                dma((pieces, S)),
                dma((pieces, S + 1)),
                dma((pieces, S)),
                dma((pieces, S)),
                dma((pieces, S)),
                dma((TP, S)),
                dma((TP, S)),
                dma((S,)),
                dma((S,)),
                dma((TP,)),
                dma((TP,)),
                dma((TP,)),
            ],
            compiler_params=pltpu.CompilerParams(
                collective_id=0, has_side_effects=True, vmem_limit_bytes=67043328 - 2**20
            ),
        )(q, k, v, lgt, mg[None], fg[None], og[None], res, ow, gw, uw, dw)

    placed = (
        P(("grp", "sp"), "tp"),
        P(("grp", "sp"), "tp"),
        P(("grp", "sp"), "tp"),
        P(("grp", "sp"), "tp"),
        P(("grp", "sp"), None),
        P("tp", None),
        P(),
        P(),
        P(),
        P("sp", "tp"),
        P("sp", "tp"),
        P("sp", "tp"),
    )
    return jax.shard_map(
        shards, mesh=mesh, in_specs=placed, out_specs=P(("grp", "sp"), None), check_vma=False
    )
```

```python
import functools

import jax
import jax.numpy as jnp
from jax import lax
from jax.experimental import pallas as pl
from jax.experimental.pallas import tpu as pltpu
from jax.sharding import PartitionSpec as P

epsilon = 1e-06
MESH = pl.DeviceIdType.MESH
F32 = jnp.float32
BF16 = jnp.bfloat16
LAG = 2
MOST_PIECES = 5
EARLY = 2


def KV_ORDER(S):
    return range(S - 1, 0, -1)


def EXTRA_ORDER(S):
    return list(range(S))


def normalize(rows):
    return rows * lax.rsqrt(jnp.mean(rows * rows, axis=-1, keepdims=True) + epsilon)


def each(count, body):
    if count <= 4:
        for i in range(count):
            body(i)
    else:

        def step(i, carry):
            body(i)
            return carry

        lax.fori_loop(0, count, step, 0)


def remote(src, dst, send, recv, axis, peer):
    return pltpu.make_async_remote_copy(
        src_ref=src,
        dst_ref=dst,
        send_sem=send,
        recv_sem=recv,
        device_id={axis: peer},
        device_id_type=MESH,
    )


def nt(a, b):
    return lax.dot_general(a, b, (((1,), (1,)), ((), ())), preferred_element_type=F32)


def kernel(
    S, TP, H, pieces,
    q, k, v, lg, mg, fg, og, res, ow, gw, uw, dw,
    out,
    kb, vb, lb, acc, run, owv, gwv, uwv, dwv, resv,
    hs, hr, mid, zs_sum, ns, na, tmp, gs, gr, hall, us, ur, zs, zr, oall,
    loc, kvs, kvr, hss, hrs, n1s, n1r, n2s, n2r, gss, grs, hars, hals, har,
    upss, upr, zss, zrs, oss, ors, outs,
):
    me, tp = lax.axis_index("sp"), lax.axis_index("tp")
    T = q.shape[0]
    hd = q.shape[1] // H
    D = out.shape[1]
    R, C = T // TP, D // S
    right, left = lax.rem(me + 1, S), lax.rem(me + S - 1, S)

    my_rows = pl.ds(pl.multiple_of(tp * R, R), R)
    loads = [
        pltpu.make_async_copy(a, b, loc.at[i])
        for i, (a, b) in enumerate(
            [(ow, owv), (res.at[my_rows], resv), (gw, gwv), (uw, uwv), (dw, dwv)]
        )
    ]
    for c in loads:
        c.start()

    barrier = pltpu.get_barrier_semaphore()
    for f in range(1, S):
        pl.semaphore_signal(barrier, inc=1, device_id={"sp": lax.rem(me + f, S)}, device_id_type=MESH)
    for f in range(1, TP):
        pl.semaphore_signal(barrier, inc=1, device_id={"tp": lax.rem(tp + f, TP)}, device_id_type=MESH)
    pl.semaphore_wait(barrier, S + TP - 2)

    def kv_copies(b, own):
        srcs = (k, v, lg) if own else (kb.at[b], vb.at[b], lb.at[b])
        return [
            remote(src, dst.at[b], kvs.at[b, i], kvr.at[b, i], "sp", right)
            for i, (src, dst) in enumerate(zip(srcs, (kb, vb, lb)))
        ]

    @pl.when(me < S - 1)
    def _():
        for c in kv_copies(me, True):
            c.start()

    rows = lax.broadcasted_iota(jnp.int32, (T, T), 0)
    cols = lax.broadcasted_iota(jnp.int32, (T, T), 1)
    causal = cols < rows
    later = (rows > cols).astype(F32)

    def block(kk, vv, ll, diag):
        for h in range(H):
            span = slice(h * hd, (h + 1) * hd)
            s = nt(q[:, span], kk[:, span]) * (hd**-0.5) + ll[h : h + 1, :]
            soft = jnp.log1p(jnp.exp(-jnp.abs(s)))
            keep = jnp.minimum(-s, 0.0) - soft
            logsig = jnp.minimum(s, 0.0) - soft
            if diag:
                keep = jnp.where(causal, keep, 0.0)
            within = jnp.dot(
                keep, later, preferred_element_type=F32, precision=lax.Precision.HIGHEST
            )
            stick = jnp.exp(logsig + within)
            if diag:
                stick = jnp.where(causal, stick, 0.0)
            part = jnp.dot(stick.astype(BF16), vv[:, span], preferred_element_type=F32)
            total = jnp.broadcast_to(jnp.sum(keep, axis=-1, keepdims=True), (T, hd))
            if diag:
                acc[h] = part
                run[h] = total
            else:
                acc[h] += jnp.exp(run[h]) * part
                run[h] += total

    block(k[...], v[...], lg[...], True)

    def earlier(i):
        b = me - 1 - i

        @pl.when(b >= 0)
        def _():
            for c in kv_copies(b, False):
                c.wait_recv()

            @pl.when(me < S - 1)
            def _():
                for c in kv_copies(b, False):
                    c.start()

            block(kb[b], vb[b], lb[b], False)

    each(S - 1, earlier)

    attended = jnp.concatenate([acc[h] for h in range(H)], axis=1).astype(BF16)
    loads[0].wait()
    width = 512 if D % 512 == 0 else D
    for c0 in range(0, D, width):
        piece = jnp.dot(attended, owv[:, c0 : c0 + width], preferred_element_type=F32)
        hs[:, :, c0 : c0 + width] = piece.astype(BF16).reshape(TP, R, width)

    def hp_copy(t, slot):
        return remote(hs.at[t], hr.at[slot], hss.at[t], hrs.at[slot], "tp", t)

    def others(count, own, body):
        def go(i):
            body(lax.rem(own + 1 + i, count))

        each(count - 1, go)

    others(TP, tp, lambda t: hp_copy(t, tp).start())
    mid[...] = hs[tp].astype(F32)

    def add_hp(t):
        hp_copy(t, t).wait_recv()
        mid[...] += hr[t].astype(F32)

    others(TP, tp, add_hp)
    loads[1].wait()
    mixed = mid[...].astype(BF16).astype(F32)
    middle = (resv[...].astype(F32) + mg[...] * normalize(mixed)).astype(BF16).astype(F32)
    mid[...] = middle
    normed = (fg[...] * normalize(middle)).astype(BF16)
    for j in range(S):
        ns[j] = normed[:, j * C : (j + 1) * C]

    def n1_copy(j, slot):
        return remote(ns.at[j], na.at[tp, slot], n1s.at[j], n1r.at[slot], "sp", j)

    def n2_copy(t, slot, s):
        return remote(na.at[tp, s], na.at[slot, s], n2s.at[t, s], n2r.at[slot, s], "tp", t)

    others(S, me, lambda j: n1_copy(j, me).start())
    na[tp, me] = ns[me]
    others(TP, tp, lambda t: n2_copy(t, tp, me).start())

    def pass_on(s):
        n1_copy(s, s).wait_recv()
        others(TP, tp, lambda t: n2_copy(t, tp, s).start())

    others(S, me, pass_on)
    for c in loads[2:4]:
        c.wait()

    def arrive(s):
        others(TP, tp, lambda t: remote(na.at[tp, s], na.at[t, s], n2s.at[t, s], n2r.at[t, s], "tp", t).wait_recv())

    W = gs.shape[-1]
    lag = LAG

    def partial(p, j):
        @pl.when(p == 0)
        def _():
            arrive(j)

        x = na[:, j].reshape(T, C)
        units = pl.ds(pl.multiple_of(p * W, W), W)
        tmp[0] = jnp.dot(x, gwv[:, units], preferred_element_type=F32)
        tmp[1] = jnp.dot(x, uwv[:, units], preferred_element_type=F32)

    def g_copy(p, j, slot, peer):
        return remote(gs.at[p, j], gr.at[p, slot], gss.at[p, j], grs.at[p, slot], "sp", peer)

    def chain(p, j, first, slot, peer):
        partial(p, j)

        @pl.when(first)
        def _():
            gs[p, j] = tmp[...].astype(BF16)

        @pl.when(jnp.logical_not(first))
        def _():
            g_copy(p, j, j, peer).wait_recv()
            gs[p, j] = (tmp[...] + gr[p, j].astype(F32)).astype(BF16)

        g_copy(p, j, slot, peer).start()

    def h_right(p, b):
        return remote(hall.at[p, b], hall.at[p, b], hars.at[p, b], har.at[p, b], "sp", right)

    def h_left(p, b):
        return remote(hall.at[p, b], hall.at[p, b], hals.at[p, b], har.at[p, b], "sp", left)

    def cut(at):
        return lax.div(at, S - 1), lax.rem(at, S - 1)

    def reduce_step(g):
        at_right = g - me * lag
        at_left = g - (S - 1 - me) * lag

        @pl.when((at_right >= 0) & (at_right < pieces * (S - 1)))
        def _():
            p, tau = cut(at_right)

            @pl.when(S - 1 - tau > me)
            def _():
                chain(p, S - 1 - tau, me == 0, S - 1 - tau, right)

        @pl.when((at_left >= 0) & (at_left < pieces * (S - 1)))
        def _():
            p, j = cut(at_left)

            @pl.when(j < me)
            def _():
                chain(p, j, me == S - 1, lax.select(j == me - 1, S, j), left)

    def finish(p):
        partial(p, me)

        @pl.when(me > 0)
        def _():
            g_copy(p, me, me, left).wait_recv()
            tmp[...] += gr[p, me].astype(F32)

        @pl.when(me < S - 1)
        def _():
            g_copy(p, me, S, right).wait_recv()
            tmp[...] += gr[p, S].astype(F32)

        gate = tmp[0]
        hall[p, me] = (gate / (1.0 + jnp.exp(-gate)) * tmp[1]).astype(BF16)

        @pl.when(me < S - 1)
        def _():
            h_right(p, me).start()

        @pl.when(me > 0)
        def _():
            h_left(p, me).start()

    def spread(p, i, then):
        lo, hi = me - 1 - i, me + 1 + i

        @pl.when(lo >= 0)
        def _():
            h_right(p, lo).wait_recv()

            @pl.when(me < S - 1)
            def _():
                h_right(p, lo).start()

            then(lo)

        @pl.when(hi < S)
        def _():
            h_left(p, hi).wait_recv()

            @pl.when(me > 0)
            def _():
                h_left(p, hi).start()

            then(hi)

    def step(g, carry):
        reduce_step(g)
        at = g - (S - 1) * lag
        p, tau = cut(at)

        @pl.when((at >= 0) & (tau == 0) & (p < pieces))
        def _():
            finish(p)

        def gather(i, carry):
            at_i = at - (i + 1) * lag
            p, tau = cut(at_i)

            @pl.when((at_i >= 0) & (tau == 0) & (p < pieces - 1))
            def _():
                spread(p, i, lambda b: None)

            return carry

        return lax.fori_loop(0, S - 1, gather, carry)

    steps = (S - 1) * (lag + max(pieces - 1, pieces - 2 + lag)) + 1
    lax.fori_loop(0, steps, step, 0)

    def up_copy(t, slot, b):
        return remote(us.at[t, b], ur.at[slot, b], upss.at[t, b], upr.at[slot, b], "tp", t)

    def down(b):
        rows_b = jnp.concatenate([hall[p, b] for p in range(pieces)], axis=1)
        us[:, b] = nt(rows_b, dwv[...]).astype(BF16).reshape(TP, R, C)
        others(TP, tp, lambda t: up_copy(t, tp, b).start())

    def z_copy(b, slot):
        return remote(zs.at[b], zr.at[slot], zss.at[b], zrs.at[slot], "sp", b)

    def settle(b):
        def add(t):
            up_copy(t, t, b).wait_recv()
            zs_sum[...] += ur[t, b].astype(F32)

        zs_sum[...] = us[tp, b].astype(F32)
        others(TP, tp, add)
        zs[b] = zs_sum[...].astype(BF16)

        @pl.when(b != me)
        def _():
            z_copy(b, me).start()

    loads[4].wait()
    down(me)

    def last(i, carry):
        spread(pieces - 1, i, down)
        return carry

    lax.fori_loop(0, S - 1, last, 0)
    others(S, me, settle)
    settle(me)
    zr[me] = zs[me]
    others(S, me, lambda s: z_copy(s, s).wait_recv())
    ffn = jnp.concatenate([zr[s] for s in range(S)], axis=1).astype(F32)
    oall[tp] = (mid[...] + og[...] * normalize(ffn)).astype(BF16)

    def o_copy(t, slot):
        return remote(oall.at[tp], oall.at[slot], oss.at[t], ors.at[slot], "tp", t)

    def o_out(t):
        return pltpu.make_async_copy(
            oall.at[t], out.at[pl.ds(pl.multiple_of(t * R, R), R)], outs.at[t]
        )

    others(TP, tp, lambda t: o_copy(t, tp).start())
    o_out(tp).start()

    def o_in(t):
        remote(oall.at[tp], oall.at[t], oss.at[t], ors.at[t], "tp", t).wait_recv()
        o_out(t).start()

    others(TP, tp, o_in)
    each(TP, lambda t: o_out(t).wait())

    @pl.when(me < S - 1)
    def _():
        def sent(b):
            @pl.when(b <= me)
            def _():
                for c in kv_copies(b, False):
                    c.wait_send()
                each(pieces, lambda p: h_right(p, b).wait_send())

        each(S, sent)

    @pl.when(me > 0)
    def _():
        def sent(b):
            @pl.when(b >= me)
            def _():
                each(pieces, lambda p: h_left(p, b).wait_send())

        each(S, sent)

    def sp_sent(j):
        n1_copy(j, me).wait_send()
        z_copy(j, me).wait_send()
        each(pieces, lambda p: g_copy(p, j, j, right).wait_send())

    others(S, me, sp_sent)

    def tp_sent(t):
        hp_copy(t, tp).wait_send()
        o_copy(t, tp).wait_send()

        def inner(s):
            n2_copy(t, tp, s).wait_send()
            up_copy(t, tp, s).wait_send()

        each(S, inner)

    others(TP, tp, tp_sent)


def gathered(
    S, TP, H, base, extras,
    q, k, v, lg, mg, fg, og, res, ow, gw, uw, dw,
    out,
    kb, vb, lb, acc, run, owv, resv, hs, hr, mid, xm, xn, gu, hid, dn, us, ur, zq, ov,
    loc, kvs, kvr, hss, hrs, azs, azr, axs, axr, acs, acr,
    gzs, gzr, gys, gyr, dzs, dzr, dys, dyr, hxs, hxr, hcr,
    rss, rsr, oxs, oxr, ocs, ocr, outs,
):
    me, tp, g = lax.axis_index("sp"), lax.axis_index("tp"), lax.axis_index("grp")
    T = q.shape[0]
    hd = q.shape[1] // H
    D = out.shape[1]
    R, C = T // TP, D // S
    NT = gu.shape[0]
    half, Q = C // 2, C // TP
    xpeer = lax.rem(tp + 2, TP)
    cpeer = tp + 1 - 2 * lax.rem(tp, 2)
    far = lax.rem(cpeer + 2, TP)

    def count(i):
        c = base
        for p in extras:
            c = c + jnp.where(i == p, 1, 0)
        return c

    def first(i):
        c = i * base
        for p in extras:
            c = c + jnp.where(i > p, 1, 0)
        return c

    def tiles_of(i, body):
        c = count(i)
        for m in sorted({base, base + 1} if extras else {base}):

            @pl.when(c == m)
            def _(m=m):
                body(m)

    n_me = count(me)
    my_rows = pl.ds(pl.multiple_of(tp * R, R), R)
    load_ow = pltpu.make_async_copy(ow, owv, loc.at[0])
    load_res = pltpu.make_async_copy(res.at[my_rows], resv, loc.at[1])
    load_ow.start()
    load_res.start()

    def drain(ref, sem):
        remote(ref, ref, sem, sem, "tp", xpeer).wait_recv()

    def own_gu(w, kk):
        lanes = pl.ds(pl.multiple_of((first(me) + kk) * 128, 128), 128)
        rows = pl.ds(pl.multiple_of(me * C, C), C)
        return pltpu.make_async_copy(
            (gw, uw)[w].at[:, lanes], gu.at[kk, rows, pl.ds(w * 128, 128)], loc.at[3 + w * NT + kk]
        )

    def own_dn(m):
        lanes = pl.ds(pl.multiple_of(first(me) * 128, 128), m * 128)
        rows = pl.ds(pl.multiple_of(tp * Q, Q), Q)
        to = pl.ds(pl.multiple_of(tp * (m * 128), 128), m * 128)
        return pltpu.make_async_copy(dw.at[rows, lanes], dn.at[me, :, to], loc.at[2])

    def with_tiles(body, at=range(NT)):
        for kk in at:

            @pl.when(kk < n_me)
            def _(kk=kk):
                body(kk)

    def load_own(kk):
        own_gu(0, kk).start()
        own_gu(1, kk).start()

    with_tiles(load_own)
    tiles_of(me, lambda m: own_dn(m).start())

    barrier = pltpu.get_barrier_semaphore()

    def greet(i):
        for f in range(TP):

            @pl.when((i != 0) | (f != 0))
            def _(f=f):
                pl.semaphore_signal(
                    barrier,
                    inc=1,
                    device_id={"sp": lax.rem(me + i, S), "tp": lax.rem(tp + f, TP)},
                    device_id_type=MESH,
                )

    for i in range(S):
        greet(i)
    pl.semaphore_signal(barrier, inc=1, device_id={"grp": 1 - g}, device_id_type=MESH)
    pl.semaphore_wait(barrier, S * TP)

    def planes(body, up=True, down=True, at=range(1, S)):
        for d in at:
            if down:

                @pl.when(me - d >= 0)
                def _(d=d):
                    body(me - d)

            if up:

                @pl.when(me + d < S)
                def _(d=d):
                    body(me + d)

    def kv_copies(b, dst):
        return [
            remote(src, to.at[b], kvs.at[dst, i // 2], kvr.at[b, i // 2], "sp", dst)
            for i, (src, to) in enumerate(zip((k, v, lg), (kb, vb, lb)))
        ]

    def send_kv(i):
        for c in kv_copies(me, i):
            c.start()

    planes(send_kv, down=False, at=KV_ORDER(S))

    def gz_copy(w, i, kk, src, dst):
        lanes = pl.ds(pl.multiple_of((first(i) + kk) * 128, 128), 128)
        rows = pl.ds(pl.multiple_of(src * C + g * half, half), half)
        return remote(
            (gw, uw)[w].at[pl.ds(pl.multiple_of(g * half, half), half), lanes],
            gu.at[kk, rows, pl.ds(w * 128, 128)],
            gzs.at[i, kk],
            gzr.at[src, kk],
            "sp",
            dst,
        )

    def gy_copy(j, kk, h):
        r = gu.at[kk, pl.ds(pl.multiple_of(j * C + h * half, half), half)]
        return remote(r, r, gys.at[kk], gyr.at[kk], "grp", 1 - g)

    def send_gu(w, kk, **sides):
        def one(i):
            @pl.when(kk < count(i))
            def _():
                gz_copy(w, i, kk, me, i).start()

        planes(one, **sides)

    def dz_copy(i, t, src, st, m):
        lanes = pl.ds(pl.multiple_of(first(i) * 128, 128), m * 128)
        rows = pl.ds(pl.multiple_of(t * Q + g * (Q // 2), Q // 2), Q // 2)
        return pltpu.make_async_remote_copy(
            src_ref=dw.at[rows, lanes],
            dst_ref=dn.at[
                src,
                pl.ds(pl.multiple_of(g * (Q // 2), Q // 2), Q // 2),
                pl.ds(pl.multiple_of(st * (m * 128), 128), m * 128),
            ],
            send_sem=dzs.at[i],
            recv_sem=dzr.at[src, st],
            device_id={"sp": i, "tp": t},
            device_id_type=MESH,
        )

    def dp_copy(t, st, m):
        lanes = pl.ds(pl.multiple_of(first(me) * 128, 128), m * 128)
        rows = pl.ds(pl.multiple_of(t * Q, Q), Q)
        return remote(
            dw.at[rows, lanes],
            dn.at[me, :, pl.ds(pl.multiple_of(st * (m * 128), 128), m * 128)],
            dzs.at[me],
            dzr.at[me, 0],
            "tp",
            t,
        )

    def dy_copy(j, st, h, m):
        r = dn.at[
            j,
            pl.ds(pl.multiple_of(h * (Q // 2), Q // 2), Q // 2),
            pl.ds(pl.multiple_of(st * (m * 128), 128), m * 128),
        ]
        return remote(r, r, dys.at[j], dyr.at[j], "grp", 1 - g)

    def peers(body):
        for f in range(1, TP):
            body(lax.rem(tp + f, TP))

    def send_dn(i, to=(tp, cpeer, xpeer, far)):
        def some(m):
            for t in to:
                dz_copy(i, t, me, tp, m).start()

        tiles_of(i, some)

    tiles_of(me, lambda m: peers(lambda t: dp_copy(t, tp, m).start()))
    for kk in range(min(EARLY, NT)):
        send_gu(0, kk, up=False)
        send_gu(1, kk, up=False)

    rows = lax.broadcasted_iota(jnp.int32, (T, T), 0)
    cols = lax.broadcasted_iota(jnp.int32, (T, T), 1)
    causal = cols < rows
    later = (rows > cols).astype(F32)

    def block(kk, vv, ll, diag):
        for h in range(H):
            span = slice(h * hd, (h + 1) * hd)
            s = nt(q[:, span], kk[:, span]) * (hd**-0.5) + ll[h : h + 1, :].astype(F32)
            soft = jnp.log1p(jnp.exp(-jnp.abs(s)))
            keep = jnp.minimum(-s, 0.0) - soft
            logsig = jnp.minimum(s, 0.0) - soft
            if diag:
                keep = jnp.where(causal, keep, 0.0)
            within = jnp.dot(
                keep, later, preferred_element_type=F32, precision=lax.Precision.HIGHEST
            )
            stick = jnp.exp(logsig + within)
            if diag:
                stick = jnp.where(causal, stick, 0.0)
            part = jnp.dot(stick.astype(BF16), vv[:, span], preferred_element_type=F32)
            total = jnp.broadcast_to(jnp.sum(keep, axis=-1, keepdims=True), (T, hd))
            if diag:
                acc[h] = part
                run[h] = total
            else:
                acc[h] += jnp.exp(run[h]) * part
                run[h] += total

    block(k[...], v[...], lg[...], True)

    def earlier(i):
        b = me - 1 - i

        @pl.when(b >= 0)
        def _():
            drain(kb.at[pl.ds(0, 2)], kvr.at[b, 0])
            drain(lb.at[0], kvr.at[b, 1])
            block(kb[b], vb[b], lb[b], False)

    each(S - 1, earlier)

    attended = jnp.concatenate([acc[h] for h in range(H)], axis=1).astype(BF16)
    load_ow.wait()
    width = 512 if D % 512 == 0 else D
    for c0 in range(0, D, width):
        piece = jnp.dot(attended, owv[:, c0 : c0 + width], preferred_element_type=F32)
        hs[:, :, c0 : c0 + width] = piece.astype(BF16).reshape(TP, R, width)

    def hp_copy(t, slot):
        return remote(hs.at[t], hr.at[slot], hss.at[0], hrs.at[0], "tp", t)

    peers(lambda t: hp_copy(t, tp).start())
    mid[...] = hs[tp].astype(F32)
    planes(
        lambda i: [drain(kb.at[pl.ds(0, 2)], kvs.at[i, 0]), drain(lb.at[0], kvs.at[i, 1])],
        down=False,
    )
    send_gu(0, 0, down=False)
    send_gu(1, 0, down=False)

    drain(hr.at[pl.ds(0, TP - 1)], hrs.at[0])

    def add_hp(t):
        mid[...] += hr[t].astype(F32)

    peers(add_hp)
    load_res.wait()
    mixed = mid[...].astype(BF16).astype(F32)
    xm[me, my_rows] = (resv[...].astype(F32) + mg[...] * normalize(mixed)).astype(BF16)

    def piece_of(j, t):
        return xm.at[j, pl.ds(pl.multiple_of(t * R, R), R)]

    def az_copy(j, way, dst):
        r = piece_of(j, tp)
        return remote(r, r, azs.at[way, j if way else dst], azr.at[j], "sp", dst)

    def ends(j, body):
        @pl.when((j <= me) & (me < S - 1))
        def _():
            body(az_copy(j, 1, me + 1))

    def ax_copy(j, t):
        return remote(piece_of(j, t), piece_of(j, t), axs.at[0], axr.at[j], "tp", xpeer)

    def ac_copy(j, t):
        return remote(piece_of(j, t), piece_of(j, t), acs.at[0], acr.at[j], "tp", cpeer)

    def af_copy(j, t):
        return remote(piece_of(j, t), piece_of(j, t), acs.at[0], acr.at[j], "tp", cpeer)

    ends(me, lambda c: c.start())
    def own_left(body):
        @pl.when(me == S - 1)
        def _():
            for i in range(S - 1):
                body(az_copy(me, 0, i))

        @pl.when((me < S - 1) & (me > 0))
        def _():
            body(az_copy(me, 0, me - 1))

    def pass_left(j, body):
        @pl.when((j > me) & (j < S - 1) & (me > 0))
        def _():
            body(az_copy(j, 2, me - 1))

    own_left(lambda c: c.start())
    ax_copy(me, tp).start()
    ac_copy(me, tp).start()

    def late_down():
        for w in range(2):
            for kk in range(EARLY, NT):
                send_gu(w, kk, up=False)

    pl.when(me < S - 1)(late_down)

    def pass_gu(kk, **sides):
        def one(j):
            drain(gu.at[kk, pl.ds(0, half)], gzr.at[j, kk])
            gy_copy(j, kk, g).start()

        @pl.when(kk < n_me)
        def _():
            planes(one, **sides)

    def spread(j):
        az_copy(j, 1, me).wait_recv()
        ends(j, lambda c: c.start())
        pass_left(j, lambda c: c.start())
        ax_copy(j, tp).start()
        ac_copy(j, tp).start()

    def hand_on(j):
        ax_copy(j, xpeer).wait_recv()
        af_copy(j, xpeer).start()

    def ready(j):
        drain(xm.at[j, pl.ds(0, 2 * R)], acr.at[j])
        for r0 in range(0, T, R):
            rows_f = xm[j, pl.ds(r0, R)].astype(F32)
            at = pl.ds(pl.multiple_of(j * T + r0, R), R)
            xn[at] = (fg[...] * normalize(rows_f)).astype(BF16)

    def pass_late(at):
        for kk in range(2, NT):
            pass_gu(kk, at=at)

    pass_gu(0)
    for kk in range(1, NT):
        send_gu(0, kk, down=False)
        send_gu(1, kk, down=False)
    pass_gu(1, down=False)
    hand_on(me)
    planes(spread, at=(1,))
    planes(hand_on, at=(1,))
    pl.when(me == S - 1)(late_down)
    ready(me)
    planes(spread, at=(2,))
    pl.when(2 * me >= S)(lambda: planes(lambda i: send_dn(i, (tp, cpeer))))
    pass_late((1,))
    planes(hand_on, at=(2,))
    planes(spread, at=range(3, S))
    pass_late((2,))
    pl.when(2 * me < S)(lambda: planes(send_dn))
    pl.when(2 * me >= S)(lambda: planes(lambda i: send_dn(i, (xpeer, far))))
    planes(hand_on, at=range(3, S))
    pass_gu(1, up=False)
    pass_late(range(3, S))
    planes(ready)

    def hid_at(t, kk):
        return hid.at[t * NT + kk]

    def hx_copy(t, kk):
        return remote(hid_at(t, kk), hid_at(t, kk), hxs.at[kk], hxr.at[kk], "tp", xpeer)

    def hc_copy(t, kk):
        return remote(hid_at(t, kk), hid_at(t, kk), hxs.at[kk], hcr.at[kk], "tp", cpeer)

    def hf_copy(t, kk):
        return remote(hid_at(t, kk), hid_at(t, kk), hxs.at[kk], hcr.at[kk], "tp", cpeer)

    def tile(kk):
        own_gu(0, kk).wait()
        own_gu(1, kk).wait()
        drain(gu.at[kk, pl.ds(0, (S - 1) * half)], gyr.at[kk])
        both = jnp.dot(xn[...], gu[kk], preferred_element_type=F32)
        gate, up = both[:, :128], both[:, 128:]
        hid[tp * NT + kk] = (gate / (1.0 + jnp.exp(-gate)) * up).astype(BF16)
        hx_copy(tp, kk).start()
        hc_copy(tp, kk).start()

    def pass_tile(kk):
        hx_copy(xpeer, kk).wait_recv()
        hf_copy(xpeer, kk).start()

    def pass_dn(j, at=range(TP)):
        def some(m):
            for f in at:
                st = (tp, cpeer, xpeer, far)[f]
                dz_copy(me, tp, j, st, m).wait_recv()
                dy_copy(j, st, g, m).start()

        tiles_of(me, some)

    with_tiles(tile, at=(0,))
    with_tiles(tile, at=(1,))
    planes(pass_dn, at=(1,))
    with_tiles(pass_tile, at=(0,))
    with_tiles(tile, at=range(2, NT))
    with_tiles(pass_tile, at=(1,))
    for f in range(TP):
        if f == TP - 1:
            with_tiles(pass_tile, at=range(2, NT))
        planes(lambda j: pass_dn(j, (f,)), at=range(2, S))

    def hid_ready(kk):
        drain(hid.at[pl.ds(0, 2)], hcr.at[kk])

    def rs_copy(j, dst, src):
        return remote(us.at[j, dst], ur.at[j, src], rss.at[0], rsr.at[j], "sp", dst)

    def down(j, own=False):
        def some(m):
            if own:
                own_dn(m).wait()
                drain(dn.at[me, :, pl.ds(0, (TP - 1) * m * 128)], dzr.at[me, 0])
            else:
                drain(dn.at[j, pl.ds(0, Q // 2), pl.ds(0, TP * m * 128)], dyr.at[j])
            x = jnp.concatenate(
                [hid[t * NT + kk] for t in range(TP) for kk in range(m)], axis=1
            )
            us[j] = nt(x, dn[j, :, : TP * m * 128]).astype(BF16).reshape(S, T, Q)

        tiles_of(me, some)
        planes(lambda i: rs_copy(j, i, me).start())

    with_tiles(hid_ready)
    down(me, True)
    for d in range(1, S):
        planes(down, at=(d,))

    def ox_copy(j, t):
        return remote(zq.at[t, j], zq.at[t, j], oxs.at[0], oxr.at[j], "tp", xpeer)

    def oc_copy(j, t):
        return remote(zq.at[t, j], zq.at[t, j], ocs.at[0], ocr.at[0], "tp", cpeer)

    def of_copy(j, t):
        return remote(zq.at[t, j], zq.at[t, j], ocs.at[0], ocr.at[0], "tp", cpeer)

    def settle(j):
        drain(ur.at[j, pl.ds(0, S - 1)], rsr.at[j])
        total = us[j, me].astype(F32)
        for d in range(1, S):
            total += ur[j, lax.rem(me + d, S)].astype(F32)
        zq[tp, j] = total.astype(BF16)
        ox_copy(j, tp).start()
        oc_copy(j, tp).start()

    order = sorted(range(S), key=lambda j: abs(2 * j + 1 - S))
    for j in order:
        settle(j)
    for j in order:
        ox_copy(j, xpeer).wait_recv()
        of_copy(j, xpeer).start()
    drain(zq.at[pl.ds(0, 2)], ocr.at[0])

    def o_out(r):
        rows_r = pl.ds(r * R, R)
        return pltpu.make_async_copy(ov.at[rows_r], out.at[rows_r], outs.at[0])

    for r in range(TP):
        rows_r = pl.ds(r * R, R)
        ffn = jnp.concatenate(
            [zq[t, j, rows_r] for j in range(S) for t in range(TP)], axis=1
        ).astype(F32)
        ov[rows_r] = (xm[me, rows_r].astype(F32) + og[...] * normalize(ffn)).astype(BF16)
        o_out(r).start()

    drain(hs.at[pl.ds(0, TP - 1)], hss.at[0])
    for j in range(S):
        pl.when(j <= me)(lambda: ends(j, lambda c: c.wait_send()))

    drain(xm.at[:, pl.ds(0, R)], axs.at[0])
    drain(xm.at[:, pl.ds(0, 2 * R)], acs.at[0])
    drain(zq.at[0], oxs.at[0])
    drain(zq.at[pl.ds(0, 2)], ocs.at[0])
    drain(us.at[pl.ds(0, S - 1)], rss.at[0])
    own_left(lambda c: c.wait_send())
    planes(lambda j: pass_left(j, lambda c: c.wait_send()), down=False)

    def sent(i):
        for kk in range(NT):

            @pl.when(kk < count(i))
            def _(kk=kk):
                drain(gu.at[kk, pl.ds(0, half)], gzs.at[i, kk])

        def some(m):
            drain(dn.at[0, pl.ds(0, Q // 2), pl.ds(0, TP * m * 128)], dzs.at[i])

        tiles_of(i, some)
        tiles_of(me, lambda m: drain(dn.at[i, pl.ds(0, Q // 2), pl.ds(0, TP * m * 128)], dys.at[i]))

    planes(sent)

    def tile_sent(kk):
        drain(gu.at[kk, pl.ds(0, (S - 1) * half)], gys.at[kk])
        drain(hid.at[pl.ds(0, 3)], hxs.at[kk])

    with_tiles(tile_sent)
    tiles_of(me, lambda m: drain(dn.at[me, :, pl.ds(0, (TP - 1) * m * 128)], dzs.at[me]))
    pltpu.make_async_copy(ov, out, outs.at[0]).wait()


def gathered_call(S, TP, q, k, v, lgt, H, mg, fg, og, res, ow, gw, uw, dw):
    T, hw = q.shape
    D = res.shape[1]
    C, U = gw.shape
    R, Q = T // TP, C // TP
    base, extra = divmod(U // 128, S)
    extras = EXTRA_ORDER(S)[:extra]
    NT = base + (1 if extra else 0)
    vm = pl.BlockSpec(memory_space=pltpu.VMEM)
    hb = pl.BlockSpec(memory_space=pl.ANY)
    dma = pltpu.SemaphoreType.DMA
    pairs = lambda *shape: [dma(shape), dma(shape)]
    return pl.pallas_call(
        functools.partial(gathered, S, TP, H, base, extras),
        out_shape=jax.ShapeDtypeStruct((T, D), BF16),
        in_specs=[vm] * 7 + [hb] * 5,
        out_specs=hb,
        scratch_shapes=[
            pltpu.VMEM((S, T, hw), BF16),
            pltpu.VMEM((S, T, hw), BF16),
            pltpu.VMEM((S,) + lgt.shape, lgt.dtype),
            pltpu.VMEM((H, T, hw // H), F32),
            pltpu.VMEM((H, T, hw // H), F32),
            pltpu.VMEM(ow.shape, BF16),
            pltpu.VMEM((R, D), BF16),
            pltpu.VMEM((TP, R, D), BF16),
            pltpu.VMEM((TP, R, D), BF16),
            pltpu.VMEM((R, D), F32),
            pltpu.VMEM((S, T, D), BF16),
            pltpu.VMEM((S * T, D), BF16),
            pltpu.VMEM((NT, D, 256), BF16),
            pltpu.VMEM((TP * NT, S * T, 128), BF16),
            pltpu.VMEM((S, Q, TP * NT * 128), BF16),
            pltpu.VMEM((S, S, T, Q), BF16),
            pltpu.VMEM((S, S, T, Q), BF16),
            pltpu.VMEM((TP, S, T, Q), BF16),
            pltpu.VMEM((T, D), BF16),
            dma((3 + 2 * NT,)),
            *pairs(S, 2),
            *pairs(1),
            dma((3, S)),
            dma((S,)),
            dma((1,)),
            dma((S,)),
            dma((1,)),
            dma((S,)),
            *pairs(S, NT),
            *pairs(NT),
            dma((S,)),
            dma((S, TP)),
            *pairs(S),
            dma((NT,)),
            dma((NT,)),
            dma((NT,)),
            dma((1,)),
            dma((S,)),
            dma((1,)),
            dma((S,)),
            *pairs(1),
            dma((1,)),
        ],
        compiler_params=pltpu.CompilerParams(
            collective_id=0, has_side_effects=True, vmem_limit_bytes=67043328 - 2**20
        ),
    )(q, k, v, lgt, mg[None], fg[None], og[None], res, ow, gw, uw, dw)


def solution(mesh):
    S, TP, G = mesh.shape["sp"], mesh.shape["tp"], mesh.shape["grp"]

    def shards(q, k, v, lg, res, ow, mg, fg, og, gw, uw, dw):
        T, H = lg.shape
        hw = q.shape[1]
        D = res.shape[1]
        C, U = gw.shape
        R = T // TP
        pieces = max([p for p in range(1, MOST_PIECES + 1) if U % (128 * p) == 0], default=1)
        W = U // pieces
        pad = -H % 8
        lgt = jnp.pad(lg.astype(F32).T, ((0, pad), (0, 0)))
        if U % 128 == 0 and U // 128 >= S and C % (128 * TP) == 0 and T % (16 * TP) == 0 and (TP, G) == (4, 2):
            return gathered_call(S, TP, q, k, v, lg.T, H, mg, fg, og, res, ow, gw, uw, dw)
        vm = pl.BlockSpec(memory_space=pltpu.VMEM)
        hb = pl.BlockSpec(memory_space=pl.ANY)
        dma = pltpu.SemaphoreType.DMA
        return pl.pallas_call(
            functools.partial(kernel, S, TP, H, pieces),
            out_shape=jax.ShapeDtypeStruct((T, D), BF16),
            in_specs=[vm] * 7 + [hb] * 5,
            out_specs=hb,
            scratch_shapes=[
                pltpu.VMEM((S, T, hw), BF16),
                pltpu.VMEM((S, T, hw), BF16),
                pltpu.VMEM((S,) + lgt.shape, F32),
                pltpu.VMEM((H, T, hw // H), F32),
                pltpu.VMEM((H, T, hw // H), F32),
                pltpu.VMEM(ow.shape, BF16),
                pltpu.VMEM(gw.shape, BF16),
                pltpu.VMEM(uw.shape, BF16),
                pltpu.VMEM(dw.shape, BF16),
                pltpu.VMEM((R, D), BF16),
                pltpu.VMEM((TP, R, D), BF16),
                pltpu.VMEM((TP, R, D), BF16),
                pltpu.VMEM((R, D), F32),
                pltpu.VMEM((R, C), F32),
                pltpu.VMEM((S, R, C), BF16),
                pltpu.VMEM((TP, S, R, C), BF16),
                pltpu.VMEM((2, T, W), F32),
                pltpu.VMEM((pieces, S, 2, T, W), BF16),
                pltpu.VMEM((pieces, S + 1, 2, T, W), BF16),
                pltpu.VMEM((pieces, S, T, W), BF16),
                pltpu.VMEM((TP, S, R, C), BF16),
                pltpu.VMEM((TP, S, R, C), BF16),
                pltpu.VMEM((S, R, C), BF16),
                pltpu.VMEM((S, R, C), BF16),
                pltpu.VMEM((TP, R, D), BF16),
                dma((5,)),
                dma((S, 3)),
                dma((S, 3)),
                dma((TP,)),
                dma((TP,)),
                dma((S,)),
                dma((S,)),
                dma((TP, S)),
                dma((TP, S)),
                dma((pieces, S)),
                dma((pieces, S + 1)),
                dma((pieces, S)),
                dma((pieces, S)),
                dma((pieces, S)),
                dma((TP, S)),
                dma((TP, S)),
                dma((S,)),
                dma((S,)),
                dma((TP,)),
                dma((TP,)),
                dma((TP,)),
            ],
            compiler_params=pltpu.CompilerParams(
                collective_id=0, has_side_effects=True, vmem_limit_bytes=67043328 - 2**20
            ),
        )(q, k, v, lgt, mg[None], fg[None], og[None], res, ow, gw, uw, dw)

    placed = (
        P(("grp", "sp"), "tp"),
        P(("grp", "sp"), "tp"),
        P(("grp", "sp"), "tp"),
        P(("grp", "sp"), "tp"),
        P(("grp", "sp"), None),
        P("tp", None),
        P(),
        P(),
        P(),
        P("sp", "tp"),
        P("sp", "tp"),
        P("sp", "tp"),
    )
    return jax.shard_map(
        shards, mesh=mesh, in_specs=placed, out_specs=P(("grp", "sp"), None), check_vma=False
    )
```

```python
import functools

import jax
import jax.numpy as jnp
from jax import lax
from jax.experimental import pallas as pl
from jax.experimental.pallas import tpu as pltpu
from jax.sharding import PartitionSpec as P

epsilon = 1e-06
MESH = pl.DeviceIdType.MESH
F32 = jnp.float32
BF16 = jnp.bfloat16
LAG = 2
MOST_PIECES = 5
EARLY = 2


def KV_ORDER(S):
    return range(S - 1, 0, -1)


def EXTRA_ORDER(S):
    return list(range(S))


def normalize(rows):
    return rows * lax.rsqrt(jnp.mean(rows * rows, axis=-1, keepdims=True) + epsilon)


def each(count, body):
    if count <= 4:
        for i in range(count):
            body(i)
    else:

        def step(i, carry):
            body(i)
            return carry

        lax.fori_loop(0, count, step, 0)


def remote(src, dst, send, recv, axis, peer):
    return pltpu.make_async_remote_copy(
        src_ref=src,
        dst_ref=dst,
        send_sem=send,
        recv_sem=recv,
        device_id={axis: peer},
        device_id_type=MESH,
    )


def nt(a, b):
    return lax.dot_general(a, b, (((1,), (1,)), ((), ())), preferred_element_type=F32)


def kernel(
    S, TP, H, pieces,
    q, k, v, lg, mg, fg, og, res, ow, gw, uw, dw,
    out,
    kb, vb, lb, acc, run, owv, gwv, uwv, dwv, resv,
    hs, hr, mid, zs_sum, ns, na, tmp, gs, gr, hall, us, ur, zs, zr, oall,
    loc, kvs, kvr, hss, hrs, n1s, n1r, n2s, n2r, gss, grs, hars, hals, har,
    upss, upr, zss, zrs, oss, ors, outs,
):
    me, tp = lax.axis_index("sp"), lax.axis_index("tp")
    T = q.shape[0]
    hd = q.shape[1] // H
    D = out.shape[1]
    R, C = T // TP, D // S
    right, left = lax.rem(me + 1, S), lax.rem(me + S - 1, S)

    my_rows = pl.ds(pl.multiple_of(tp * R, R), R)
    loads = [
        pltpu.make_async_copy(a, b, loc.at[i])
        for i, (a, b) in enumerate(
            [(ow, owv), (res.at[my_rows], resv), (gw, gwv), (uw, uwv), (dw, dwv)]
        )
    ]
    for c in loads:
        c.start()

    barrier = pltpu.get_barrier_semaphore()
    for f in range(1, S):
        pl.semaphore_signal(barrier, inc=1, device_id={"sp": lax.rem(me + f, S)}, device_id_type=MESH)
    for f in range(1, TP):
        pl.semaphore_signal(barrier, inc=1, device_id={"tp": lax.rem(tp + f, TP)}, device_id_type=MESH)
    pl.semaphore_wait(barrier, S + TP - 2)

    def kv_copies(b, own):
        srcs = (k, v, lg) if own else (kb.at[b], vb.at[b], lb.at[b])
        return [
            remote(src, dst.at[b], kvs.at[b, i], kvr.at[b, i], "sp", right)
            for i, (src, dst) in enumerate(zip(srcs, (kb, vb, lb)))
        ]

    @pl.when(me < S - 1)
    def _():
        for c in kv_copies(me, True):
            c.start()

    rows = lax.broadcasted_iota(jnp.int32, (T, T), 0)
    cols = lax.broadcasted_iota(jnp.int32, (T, T), 1)
    causal = cols < rows
    later = (rows > cols).astype(F32)

    def block(kk, vv, ll, diag):
        for h in range(H):
            span = slice(h * hd, (h + 1) * hd)
            s = nt(q[:, span], kk[:, span]) * (hd**-0.5) + ll[h : h + 1, :]
            soft = jnp.log1p(jnp.exp(-jnp.abs(s)))
            keep = jnp.minimum(-s, 0.0) - soft
            logsig = jnp.minimum(s, 0.0) - soft
            if diag:
                keep = jnp.where(causal, keep, 0.0)
            within = jnp.dot(
                keep, later, preferred_element_type=F32, precision=lax.Precision.HIGHEST
            )
            stick = jnp.exp(logsig + within)
            if diag:
                stick = jnp.where(causal, stick, 0.0)
            part = jnp.dot(stick.astype(BF16), vv[:, span], preferred_element_type=F32)
            total = jnp.broadcast_to(jnp.sum(keep, axis=-1, keepdims=True), (T, hd))
            if diag:
                acc[h] = part
                run[h] = total
            else:
                acc[h] += jnp.exp(run[h]) * part
                run[h] += total

    block(k[...], v[...], lg[...], True)

    def earlier(i):
        b = me - 1 - i

        @pl.when(b >= 0)
        def _():
            for c in kv_copies(b, False):
                c.wait_recv()

            @pl.when(me < S - 1)
            def _():
                for c in kv_copies(b, False):
                    c.start()

            block(kb[b], vb[b], lb[b], False)

    each(S - 1, earlier)

    attended = jnp.concatenate([acc[h] for h in range(H)], axis=1).astype(BF16)
    loads[0].wait()
    width = 512 if D % 512 == 0 else D
    for c0 in range(0, D, width):
        piece = jnp.dot(attended, owv[:, c0 : c0 + width], preferred_element_type=F32)
        hs[:, :, c0 : c0 + width] = piece.astype(BF16).reshape(TP, R, width)

    def hp_copy(t, slot):
        return remote(hs.at[t], hr.at[slot], hss.at[t], hrs.at[slot], "tp", t)

    def others(count, own, body):
        def go(i):
            body(lax.rem(own + 1 + i, count))

        each(count - 1, go)

    others(TP, tp, lambda t: hp_copy(t, tp).start())
    mid[...] = hs[tp].astype(F32)

    def add_hp(t):
        hp_copy(t, t).wait_recv()
        mid[...] += hr[t].astype(F32)

    others(TP, tp, add_hp)
    loads[1].wait()
    mixed = mid[...].astype(BF16).astype(F32)
    middle = (resv[...].astype(F32) + mg[...] * normalize(mixed)).astype(BF16).astype(F32)
    mid[...] = middle
    normed = (fg[...] * normalize(middle)).astype(BF16)
    for j in range(S):
        ns[j] = normed[:, j * C : (j + 1) * C]

    def n1_copy(j, slot):
        return remote(ns.at[j], na.at[tp, slot], n1s.at[j], n1r.at[slot], "sp", j)

    def n2_copy(t, slot, s):
        return remote(na.at[tp, s], na.at[slot, s], n2s.at[t, s], n2r.at[slot, s], "tp", t)

    others(S, me, lambda j: n1_copy(j, me).start())
    na[tp, me] = ns[me]
    others(TP, tp, lambda t: n2_copy(t, tp, me).start())

    def pass_on(s):
        n1_copy(s, s).wait_recv()
        others(TP, tp, lambda t: n2_copy(t, tp, s).start())

    others(S, me, pass_on)
    for c in loads[2:4]:
        c.wait()

    def arrive(s):
        others(TP, tp, lambda t: remote(na.at[tp, s], na.at[t, s], n2s.at[t, s], n2r.at[t, s], "tp", t).wait_recv())

    W = gs.shape[-1]
    lag = LAG

    def partial(p, j):
        @pl.when(p == 0)
        def _():
            arrive(j)

        x = na[:, j].reshape(T, C)
        units = pl.ds(pl.multiple_of(p * W, W), W)
        tmp[0] = jnp.dot(x, gwv[:, units], preferred_element_type=F32)
        tmp[1] = jnp.dot(x, uwv[:, units], preferred_element_type=F32)

    def g_copy(p, j, slot, peer):
        return remote(gs.at[p, j], gr.at[p, slot], gss.at[p, j], grs.at[p, slot], "sp", peer)

    def chain(p, j, first, slot, peer):
        partial(p, j)

        @pl.when(first)
        def _():
            gs[p, j] = tmp[...].astype(BF16)

        @pl.when(jnp.logical_not(first))
        def _():
            g_copy(p, j, j, peer).wait_recv()
            gs[p, j] = (tmp[...] + gr[p, j].astype(F32)).astype(BF16)

        g_copy(p, j, slot, peer).start()

    def h_right(p, b):
        return remote(hall.at[p, b], hall.at[p, b], hars.at[p, b], har.at[p, b], "sp", right)

    def h_left(p, b):
        return remote(hall.at[p, b], hall.at[p, b], hals.at[p, b], har.at[p, b], "sp", left)

    def cut(at):
        return lax.div(at, S - 1), lax.rem(at, S - 1)

    def reduce_step(g):
        at_right = g - me * lag
        at_left = g - (S - 1 - me) * lag

        @pl.when((at_right >= 0) & (at_right < pieces * (S - 1)))
        def _():
            p, tau = cut(at_right)

            @pl.when(S - 1 - tau > me)
            def _():
                chain(p, S - 1 - tau, me == 0, S - 1 - tau, right)

        @pl.when((at_left >= 0) & (at_left < pieces * (S - 1)))
        def _():
            p, j = cut(at_left)

            @pl.when(j < me)
            def _():
                chain(p, j, me == S - 1, lax.select(j == me - 1, S, j), left)

    def finish(p):
        partial(p, me)

        @pl.when(me > 0)
        def _():
            g_copy(p, me, me, left).wait_recv()
            tmp[...] += gr[p, me].astype(F32)

        @pl.when(me < S - 1)
        def _():
            g_copy(p, me, S, right).wait_recv()
            tmp[...] += gr[p, S].astype(F32)

        gate = tmp[0]
        hall[p, me] = (gate / (1.0 + jnp.exp(-gate)) * tmp[1]).astype(BF16)

        @pl.when(me < S - 1)
        def _():
            h_right(p, me).start()

        @pl.when(me > 0)
        def _():
            h_left(p, me).start()

    def spread(p, i, then):
        lo, hi = me - 1 - i, me + 1 + i

        @pl.when(lo >= 0)
        def _():
            h_right(p, lo).wait_recv()

            @pl.when(me < S - 1)
            def _():
                h_right(p, lo).start()

            then(lo)

        @pl.when(hi < S)
        def _():
            h_left(p, hi).wait_recv()

            @pl.when(me > 0)
            def _():
                h_left(p, hi).start()

            then(hi)

    def step(g, carry):
        reduce_step(g)
        at = g - (S - 1) * lag
        p, tau = cut(at)

        @pl.when((at >= 0) & (tau == 0) & (p < pieces))
        def _():
            finish(p)

        def gather(i, carry):
            at_i = at - (i + 1) * lag
            p, tau = cut(at_i)

            @pl.when((at_i >= 0) & (tau == 0) & (p < pieces - 1))
            def _():
                spread(p, i, lambda b: None)

            return carry

        return lax.fori_loop(0, S - 1, gather, carry)

    steps = (S - 1) * (lag + max(pieces - 1, pieces - 2 + lag)) + 1
    lax.fori_loop(0, steps, step, 0)

    def up_copy(t, slot, b):
        return remote(us.at[t, b], ur.at[slot, b], upss.at[t, b], upr.at[slot, b], "tp", t)

    def down(b):
        rows_b = jnp.concatenate([hall[p, b] for p in range(pieces)], axis=1)
        us[:, b] = nt(rows_b, dwv[...]).astype(BF16).reshape(TP, R, C)
        others(TP, tp, lambda t: up_copy(t, tp, b).start())

    def z_copy(b, slot):
        return remote(zs.at[b], zr.at[slot], zss.at[b], zrs.at[slot], "sp", b)

    def settle(b):
        def add(t):
            up_copy(t, t, b).wait_recv()
            zs_sum[...] += ur[t, b].astype(F32)

        zs_sum[...] = us[tp, b].astype(F32)
        others(TP, tp, add)
        zs[b] = zs_sum[...].astype(BF16)

        @pl.when(b != me)
        def _():
            z_copy(b, me).start()

    loads[4].wait()
    down(me)

    def last(i, carry):
        spread(pieces - 1, i, down)
        return carry

    lax.fori_loop(0, S - 1, last, 0)
    others(S, me, settle)
    settle(me)
    zr[me] = zs[me]
    others(S, me, lambda s: z_copy(s, s).wait_recv())
    ffn = jnp.concatenate([zr[s] for s in range(S)], axis=1).astype(F32)
    oall[tp] = (mid[...] + og[...] * normalize(ffn)).astype(BF16)

    def o_copy(t, slot):
        return remote(oall.at[tp], oall.at[slot], oss.at[t], ors.at[slot], "tp", t)

    def o_out(t):
        return pltpu.make_async_copy(
            oall.at[t], out.at[pl.ds(pl.multiple_of(t * R, R), R)], outs.at[t]
        )

    others(TP, tp, lambda t: o_copy(t, tp).start())
    o_out(tp).start()

    def o_in(t):
        remote(oall.at[tp], oall.at[t], oss.at[t], ors.at[t], "tp", t).wait_recv()
        o_out(t).start()

    others(TP, tp, o_in)
    each(TP, lambda t: o_out(t).wait())

    @pl.when(me < S - 1)
    def _():
        def sent(b):
            @pl.when(b <= me)
            def _():
                for c in kv_copies(b, False):
                    c.wait_send()
                each(pieces, lambda p: h_right(p, b).wait_send())

        each(S, sent)

    @pl.when(me > 0)
    def _():
        def sent(b):
            @pl.when(b >= me)
            def _():
                each(pieces, lambda p: h_left(p, b).wait_send())

        each(S, sent)

    def sp_sent(j):
        n1_copy(j, me).wait_send()
        z_copy(j, me).wait_send()
        each(pieces, lambda p: g_copy(p, j, j, right).wait_send())

    others(S, me, sp_sent)

    def tp_sent(t):
        hp_copy(t, tp).wait_send()
        o_copy(t, tp).wait_send()

        def inner(s):
            n2_copy(t, tp, s).wait_send()
            up_copy(t, tp, s).wait_send()

        each(S, inner)

    others(TP, tp, tp_sent)


def gathered(
    S, TP, H, base, extras,
    q, k, v, lg, mg, fg, og, res, ow, gw, uw, dw,
    out,
    kb, vb, lb, acc, run, owv, resv, hs, hr, mid, xm, xn, gu, hid, dn, us, ur, zq, ov,
    loc, kvs, kvr, hss, hrs, azs, azr, axs, axr, acs, acr,
    gzs, gzr, gys, gyr, dzs, dzr, dys, dyr, hxs, hxr, hcr,
    rss, rsr, oxs, oxr, ocs, ocr, outs,
):
    me, tp, g = lax.axis_index("sp"), lax.axis_index("tp"), lax.axis_index("grp")
    T = q.shape[0]
    hd = q.shape[1] // H
    D = out.shape[1]
    R, C = T // TP, D // S
    NT = gu.shape[0]
    half, Q = C // 2, C // TP
    xpeer = lax.rem(tp + 2, TP)
    cpeer = tp + 1 - 2 * lax.rem(tp, 2)
    far = lax.rem(cpeer + 2, TP)

    def count(i):
        c = base
        for p in extras:
            c = c + jnp.where(i == p, 1, 0)
        return c

    def first(i):
        c = i * base
        for p in extras:
            c = c + jnp.where(i > p, 1, 0)
        return c

    def tiles_of(i, body):
        c = count(i)
        for m in sorted({base, base + 1} if extras else {base}):

            @pl.when(c == m)
            def _(m=m):
                body(m)

    n_me = count(me)
    my_rows = pl.ds(pl.multiple_of(tp * R, R), R)
    load_ow = pltpu.make_async_copy(ow, owv, loc.at[0])
    load_res = pltpu.make_async_copy(res.at[my_rows], resv, loc.at[1])
    load_ow.start()
    load_res.start()

    def drain(ref, sem):
        remote(ref, ref, sem, sem, "tp", xpeer).wait_recv()

    def own_gu(w, kk):
        lanes = pl.ds(pl.multiple_of((first(me) + kk) * 128, 128), 128)
        rows = pl.ds(pl.multiple_of(me * C, C), C)
        return pltpu.make_async_copy(
            (gw, uw)[w].at[:, lanes], gu.at[kk, rows, pl.ds(w * 128, 128)], loc.at[3 + w * NT + kk]
        )

    def own_dn(m):
        lanes = pl.ds(pl.multiple_of(first(me) * 128, 128), m * 128)
        rows = pl.ds(pl.multiple_of(tp * Q, Q), Q)
        to = pl.ds(pl.multiple_of(tp * (m * 128), 128), m * 128)
        return pltpu.make_async_copy(dw.at[rows, lanes], dn.at[me, :, to], loc.at[2])

    def with_tiles(body, at=range(NT)):
        for kk in at:

            @pl.when(kk < n_me)
            def _(kk=kk):
                body(kk)

    def load_own(kk):
        own_gu(0, kk).start()
        own_gu(1, kk).start()

    with_tiles(load_own)
    tiles_of(me, lambda m: own_dn(m).start())

    barrier = pltpu.get_barrier_semaphore()

    def greet(i):
        for f in range(TP):

            @pl.when((i != 0) | (f != 0))
            def _(f=f):
                pl.semaphore_signal(
                    barrier,
                    inc=1,
                    device_id={"sp": lax.rem(me + i, S), "tp": lax.rem(tp + f, TP)},
                    device_id_type=MESH,
                )

    for i in range(S):
        greet(i)
    pl.semaphore_signal(barrier, inc=1, device_id={"grp": 1 - g}, device_id_type=MESH)
    pl.semaphore_wait(barrier, S * TP)

    def planes(body, up=True, down=True, at=range(1, S)):
        for d in at:
            if down:

                @pl.when(me - d >= 0)
                def _(d=d):
                    body(me - d)

            if up:

                @pl.when(me + d < S)
                def _(d=d):
                    body(me + d)

    def kv_copies(b, dst):
        return [
            remote(src, to.at[b], kvs.at[dst, i // 2], kvr.at[b, i // 2], "sp", dst)
            for i, (src, to) in enumerate(zip((k, v, lg), (kb, vb, lb)))
        ]

    def send_kv(i):
        for c in kv_copies(me, i):
            c.start()

    planes(send_kv, down=False, at=KV_ORDER(S))

    def gz_copy(w, i, kk, src, dst):
        lanes = pl.ds(pl.multiple_of((first(i) + kk) * 128, 128), 128)
        rows = pl.ds(pl.multiple_of(src * C + g * half, half), half)
        return remote(
            (gw, uw)[w].at[pl.ds(pl.multiple_of(g * half, half), half), lanes],
            gu.at[kk, rows, pl.ds(w * 128, 128)],
            gzs.at[i, kk],
            gzr.at[src, kk],
            "sp",
            dst,
        )

    def gy_copy(j, kk, h):
        r = gu.at[kk, pl.ds(pl.multiple_of(j * C + h * half, half), half)]
        return remote(r, r, gys.at[kk], gyr.at[kk], "grp", 1 - g)

    def send_gu(w, kk, **sides):
        def one(i):
            @pl.when(kk < count(i))
            def _():
                gz_copy(w, i, kk, me, i).start()

        planes(one, **sides)

    def dz_copy(i, t, src, st, m):
        lanes = pl.ds(pl.multiple_of(first(i) * 128, 128), m * 128)
        rows = pl.ds(pl.multiple_of(t * Q + g * (Q // 2), Q // 2), Q // 2)
        return pltpu.make_async_remote_copy(
            src_ref=dw.at[rows, lanes],
            dst_ref=dn.at[
                src,
                pl.ds(pl.multiple_of(g * (Q // 2), Q // 2), Q // 2),
                pl.ds(pl.multiple_of(st * (m * 128), 128), m * 128),
            ],
            send_sem=dzs.at[i],
            recv_sem=dzr.at[src, st],
            device_id={"sp": i, "tp": t},
            device_id_type=MESH,
        )

    def dp_copy(t, st, m):
        lanes = pl.ds(pl.multiple_of(first(me) * 128, 128), m * 128)
        rows = pl.ds(pl.multiple_of(t * Q, Q), Q)
        return remote(
            dw.at[rows, lanes],
            dn.at[me, :, pl.ds(pl.multiple_of(st * (m * 128), 128), m * 128)],
            dzs.at[me],
            dzr.at[me, 0],
            "tp",
            t,
        )

    def dy_copy(j, st, h, m):
        r = dn.at[
            j,
            pl.ds(pl.multiple_of(h * (Q // 2), Q // 2), Q // 2),
            pl.ds(pl.multiple_of(st * (m * 128), 128), m * 128),
        ]
        return remote(r, r, dys.at[j], dyr.at[j], "grp", 1 - g)

    def peers(body):
        for f in range(1, TP):
            body(lax.rem(tp + f, TP))

    def send_dn(i, to=(tp, cpeer, xpeer, far)):
        def some(m):
            for t in to:
                dz_copy(i, t, me, tp, m).start()

        tiles_of(i, some)

    tiles_of(me, lambda m: peers(lambda t: dp_copy(t, tp, m).start()))
    for kk in range(min(EARLY, NT)):
        send_gu(0, kk, up=False)
        send_gu(1, kk, up=False)

    rows = lax.broadcasted_iota(jnp.int32, (T, T), 0)
    cols = lax.broadcasted_iota(jnp.int32, (T, T), 1)
    causal = cols < rows
    later = (rows > cols).astype(F32)

    def block(kk, vv, ll, diag):
        for h in range(H):
            span = slice(h * hd, (h + 1) * hd)
            s = nt(q[:, span], kk[:, span]) * (hd**-0.5) + ll[h : h + 1, :].astype(F32)
            soft = jnp.log1p(jnp.exp(-jnp.abs(s)))
            keep = jnp.minimum(-s, 0.0) - soft
            logsig = jnp.minimum(s, 0.0) - soft
            if diag:
                keep = jnp.where(causal, keep, 0.0)
            within = jnp.dot(
                keep, later, preferred_element_type=F32, precision=lax.Precision.HIGHEST
            )
            stick = jnp.exp(logsig + within)
            if diag:
                stick = jnp.where(causal, stick, 0.0)
            part = jnp.dot(stick.astype(BF16), vv[:, span], preferred_element_type=F32)
            total = jnp.broadcast_to(jnp.sum(keep, axis=-1, keepdims=True), (T, hd))
            if diag:
                acc[h] = part
                run[h] = total
            else:
                acc[h] += jnp.exp(run[h]) * part
                run[h] += total

    block(k[...], v[...], lg[...], True)

    def earlier(i):
        b = me - 1 - i

        @pl.when(b >= 0)
        def _():
            drain(kb.at[pl.ds(0, 2)], kvr.at[b, 0])
            drain(lb.at[0], kvr.at[b, 1])
            block(kb[b], vb[b], lb[b], False)

    each(S - 1, earlier)

    attended = jnp.concatenate([acc[h] for h in range(H)], axis=1).astype(BF16)
    load_ow.wait()
    width = 512 if D % 512 == 0 else D
    for c0 in range(0, D, width):
        piece = jnp.dot(attended, owv[:, c0 : c0 + width], preferred_element_type=F32)
        hs[:, :, c0 : c0 + width] = piece.astype(BF16).reshape(TP, R, width)

    def hp_copy(t, slot):
        return remote(hs.at[t], hr.at[slot], hss.at[0], hrs.at[0], "tp", t)

    peers(lambda t: hp_copy(t, tp).start())
    mid[...] = hs[tp].astype(F32)
    planes(
        lambda i: [drain(kb.at[pl.ds(0, 2)], kvs.at[i, 0]), drain(lb.at[0], kvs.at[i, 1])],
        down=False,
    )
    send_gu(0, 0, down=False)
    send_gu(1, 0, down=False)

    drain(hr.at[pl.ds(0, TP - 1)], hrs.at[0])

    def add_hp(t):
        mid[...] += hr[t].astype(F32)

    peers(add_hp)
    load_res.wait()
    mixed = mid[...].astype(BF16).astype(F32)
    xm[me, my_rows] = (resv[...].astype(F32) + mg[...] * normalize(mixed)).astype(BF16)

    def piece_of(j, t):
        return xm.at[j, pl.ds(pl.multiple_of(t * R, R), R)]

    def az_copy(j, way, dst):
        r = piece_of(j, tp)
        return remote(r, r, azs.at[way, j if way else dst], azr.at[j], "sp", dst)

    def ends(j, body):
        @pl.when((j <= me) & (me < S - 1))
        def _():
            body(az_copy(j, 1, me + 1))

    def ax_copy(j, t):
        return remote(piece_of(j, t), piece_of(j, t), axs.at[0], axr.at[j], "tp", xpeer)

    def ac_copy(j, t):
        return remote(piece_of(j, t), piece_of(j, t), acs.at[0], acr.at[j], "tp", cpeer)

    def af_copy(j, t):
        return remote(piece_of(j, t), piece_of(j, t), acs.at[0], acr.at[j], "tp", cpeer)

    ends(me, lambda c: c.start())
    def own_left(body):
        @pl.when(me == S - 1)
        def _():
            for i in range(S - 1):
                body(az_copy(me, 0, i))

        @pl.when((me < S - 1) & (me > 0))
        def _():
            body(az_copy(me, 0, me - 1))

    def pass_left(j, body):
        @pl.when((j > me) & (j < S - 1) & (me > 0))
        def _():
            body(az_copy(j, 2, me - 1))

    own_left(lambda c: c.start())
    ax_copy(me, tp).start()
    ac_copy(me, tp).start()

    def late_down():
        for w in range(2):
            for kk in range(EARLY, NT):
                send_gu(w, kk, up=False)

    pl.when(me < S - 1)(late_down)

    def pass_gu(kk, **sides):
        def one(j):
            drain(gu.at[kk, pl.ds(0, half)], gzr.at[j, kk])
            gy_copy(j, kk, g).start()

        @pl.when(kk < n_me)
        def _():
            planes(one, **sides)

    def spread(j):
        az_copy(j, 1, me).wait_recv()
        ends(j, lambda c: c.start())
        pass_left(j, lambda c: c.start())
        ax_copy(j, tp).start()
        ac_copy(j, tp).start()

    def hand_on(j):
        ax_copy(j, xpeer).wait_recv()
        af_copy(j, xpeer).start()

    def ready(j):
        drain(xm.at[j, pl.ds(0, 2 * R)], acr.at[j])
        for r0 in range(0, T, R):
            rows_f = xm[j, pl.ds(r0, R)].astype(F32)
            at = pl.ds(pl.multiple_of(j * T + r0, R), R)
            xn[at] = (fg[...] * normalize(rows_f)).astype(BF16)

    def pass_late(at):
        for kk in range(2, NT):
            pass_gu(kk, at=at)

    pass_gu(0)
    for kk in range(1, NT):
        send_gu(0, kk, down=False)
        send_gu(1, kk, down=False)
    planes(spread, up=False, at=(1,))
    pass_gu(1, down=False)
    hand_on(me)
    planes(spread, down=False, at=(1,))
    planes(hand_on, at=(1,))
    pl.when(me == S - 1)(late_down)
    ready(me)
    planes(spread, at=(2,))
    pl.when(2 * me >= S)(lambda: planes(lambda i: send_dn(i, (tp, cpeer))))
    pass_late((1,))
    planes(hand_on, at=(2,))
    planes(spread, at=range(3, S))
    pass_late((2,))
    pl.when(2 * me < S)(lambda: planes(send_dn))
    pl.when(2 * me >= S)(lambda: planes(lambda i: send_dn(i, (xpeer, far))))
    planes(hand_on, at=range(3, S))
    pass_gu(1, up=False)
    pass_late(range(3, S))
    planes(ready)

    def hid_at(t, kk):
        return hid.at[t * NT + kk]

    def hx_copy(t, kk):
        return remote(hid_at(t, kk), hid_at(t, kk), hxs.at[kk], hxr.at[kk], "tp", xpeer)

    def hc_copy(t, kk):
        return remote(hid_at(t, kk), hid_at(t, kk), hxs.at[kk], hcr.at[kk], "tp", cpeer)

    def hf_copy(t, kk):
        return remote(hid_at(t, kk), hid_at(t, kk), hxs.at[kk], hcr.at[kk], "tp", cpeer)

    def tile(kk):
        own_gu(0, kk).wait()
        own_gu(1, kk).wait()
        drain(gu.at[kk, pl.ds(0, (S - 1) * half)], gyr.at[kk])
        both = jnp.dot(xn[...], gu[kk], preferred_element_type=F32)
        gate, up = both[:, :128], both[:, 128:]
        hid[tp * NT + kk] = (gate / (1.0 + jnp.exp(-gate)) * up).astype(BF16)
        hx_copy(tp, kk).start()
        hc_copy(tp, kk).start()

    def pass_tile(kk):
        hx_copy(xpeer, kk).wait_recv()
        hf_copy(xpeer, kk).start()

    def pass_dn(j, at=range(TP)):
        def some(m):
            for f in at:
                st = (tp, cpeer, xpeer, far)[f]
                dz_copy(me, tp, j, st, m).wait_recv()
                dy_copy(j, st, g, m).start()

        tiles_of(me, some)

    with_tiles(tile, at=(0,))
    with_tiles(tile, at=(1,))
    planes(pass_dn, at=(1,))
    with_tiles(pass_tile, at=(0,))
    with_tiles(tile, at=range(2, NT))
    with_tiles(pass_tile, at=(1,))
    for f in range(TP):
        if f == TP - 1:
            with_tiles(pass_tile, at=range(2, NT))
        planes(lambda j: pass_dn(j, (f,)), at=range(2, S))

    def hid_ready(kk):
        drain(hid.at[pl.ds(0, 2)], hcr.at[kk])

    def rs_copy(j, dst, src):
        return remote(us.at[j, dst], ur.at[j, src], rss.at[0], rsr.at[j], "sp", dst)

    def down(j, own=False):
        def some(m):
            if own:
                own_dn(m).wait()
                drain(dn.at[me, :, pl.ds(0, (TP - 1) * m * 128)], dzr.at[me, 0])
            else:
                drain(dn.at[j, pl.ds(0, Q // 2), pl.ds(0, TP * m * 128)], dyr.at[j])
            x = jnp.concatenate(
                [hid[t * NT + kk] for t in range(TP) for kk in range(m)], axis=1
            )
            us[j] = nt(x, dn[j, :, : TP * m * 128]).astype(BF16).reshape(S, T, Q)

        tiles_of(me, some)
        planes(lambda i: rs_copy(j, i, me).start())

    with_tiles(hid_ready)
    down(me, True)
    for d in range(1, S):
        planes(down, at=(d,))

    def ox_copy(j, t):
        return remote(zq.at[t, j], zq.at[t, j], oxs.at[0], oxr.at[j], "tp", xpeer)

    def oc_copy(j, t):
        return remote(zq.at[t, j], zq.at[t, j], ocs.at[0], ocr.at[0], "tp", cpeer)

    def of_copy(j, t):
        return remote(zq.at[t, j], zq.at[t, j], ocs.at[0], ocr.at[0], "tp", cpeer)

    def settle(j):
        drain(ur.at[j, pl.ds(0, S - 1)], rsr.at[j])
        total = us[j, me].astype(F32)
        for d in range(1, S):
            total += ur[j, lax.rem(me + d, S)].astype(F32)
        zq[tp, j] = total.astype(BF16)
        ox_copy(j, tp).start()
        oc_copy(j, tp).start()

    order = sorted(range(S), key=lambda j: abs(2 * j + 1 - S))
    for j in order:
        settle(j)
    for j in order:
        ox_copy(j, xpeer).wait_recv()
        of_copy(j, xpeer).start()
    drain(zq.at[pl.ds(0, 2)], ocr.at[0])

    def o_out(r):
        rows_r = pl.ds(r * R, R)
        return pltpu.make_async_copy(ov.at[rows_r], out.at[rows_r], outs.at[0])

    for r in range(TP):
        rows_r = pl.ds(r * R, R)
        ffn = jnp.concatenate(
            [zq[t, j, rows_r] for j in range(S) for t in range(TP)], axis=1
        ).astype(F32)
        ov[rows_r] = (xm[me, rows_r].astype(F32) + og[...] * normalize(ffn)).astype(BF16)
        o_out(r).start()

    drain(hs.at[pl.ds(0, TP - 1)], hss.at[0])
    for j in range(S):
        pl.when(j <= me)(lambda: ends(j, lambda c: c.wait_send()))

    drain(xm.at[:, pl.ds(0, R)], axs.at[0])
    drain(xm.at[:, pl.ds(0, 2 * R)], acs.at[0])
    drain(zq.at[0], oxs.at[0])
    drain(zq.at[pl.ds(0, 2)], ocs.at[0])
    drain(us.at[pl.ds(0, S - 1)], rss.at[0])
    own_left(lambda c: c.wait_send())
    planes(lambda j: pass_left(j, lambda c: c.wait_send()), down=False)

    def sent(i):
        for kk in range(NT):

            @pl.when(kk < count(i))
            def _(kk=kk):
                drain(gu.at[kk, pl.ds(0, half)], gzs.at[i, kk])

        def some(m):
            drain(dn.at[0, pl.ds(0, Q // 2), pl.ds(0, TP * m * 128)], dzs.at[i])

        tiles_of(i, some)
        tiles_of(me, lambda m: drain(dn.at[i, pl.ds(0, Q // 2), pl.ds(0, TP * m * 128)], dys.at[i]))

    planes(sent)

    def tile_sent(kk):
        drain(gu.at[kk, pl.ds(0, (S - 1) * half)], gys.at[kk])
        drain(hid.at[pl.ds(0, 3)], hxs.at[kk])

    with_tiles(tile_sent)
    tiles_of(me, lambda m: drain(dn.at[me, :, pl.ds(0, (TP - 1) * m * 128)], dzs.at[me]))
    pltpu.make_async_copy(ov, out, outs.at[0]).wait()


def gathered_call(S, TP, q, k, v, lgt, H, mg, fg, og, res, ow, gw, uw, dw):
    T, hw = q.shape
    D = res.shape[1]
    C, U = gw.shape
    R, Q = T // TP, C // TP
    base, extra = divmod(U // 128, S)
    extras = EXTRA_ORDER(S)[:extra]
    NT = base + (1 if extra else 0)
    vm = pl.BlockSpec(memory_space=pltpu.VMEM)
    hb = pl.BlockSpec(memory_space=pl.ANY)
    dma = pltpu.SemaphoreType.DMA
    pairs = lambda *shape: [dma(shape), dma(shape)]
    return pl.pallas_call(
        functools.partial(gathered, S, TP, H, base, extras),
        out_shape=jax.ShapeDtypeStruct((T, D), BF16),
        in_specs=[vm] * 7 + [hb] * 5,
        out_specs=hb,
        scratch_shapes=[
            pltpu.VMEM((S, T, hw), BF16),
            pltpu.VMEM((S, T, hw), BF16),
            pltpu.VMEM((S,) + lgt.shape, lgt.dtype),
            pltpu.VMEM((H, T, hw // H), F32),
            pltpu.VMEM((H, T, hw // H), F32),
            pltpu.VMEM(ow.shape, BF16),
            pltpu.VMEM((R, D), BF16),
            pltpu.VMEM((TP, R, D), BF16),
            pltpu.VMEM((TP, R, D), BF16),
            pltpu.VMEM((R, D), F32),
            pltpu.VMEM((S, T, D), BF16),
            pltpu.VMEM((S * T, D), BF16),
            pltpu.VMEM((NT, D, 256), BF16),
            pltpu.VMEM((TP * NT, S * T, 128), BF16),
            pltpu.VMEM((S, Q, TP * NT * 128), BF16),
            pltpu.VMEM((S, S, T, Q), BF16),
            pltpu.VMEM((S, S, T, Q), BF16),
            pltpu.VMEM((TP, S, T, Q), BF16),
            pltpu.VMEM((T, D), BF16),
            dma((3 + 2 * NT,)),
            *pairs(S, 2),
            *pairs(1),
            dma((3, S)),
            dma((S,)),
            dma((1,)),
            dma((S,)),
            dma((1,)),
            dma((S,)),
            *pairs(S, NT),
            *pairs(NT),
            dma((S,)),
            dma((S, TP)),
            *pairs(S),
            dma((NT,)),
            dma((NT,)),
            dma((NT,)),
            dma((1,)),
            dma((S,)),
            dma((1,)),
            dma((S,)),
            *pairs(1),
            dma((1,)),
        ],
        compiler_params=pltpu.CompilerParams(
            collective_id=0, has_side_effects=True, vmem_limit_bytes=67043328 - 2**20
        ),
    )(q, k, v, lgt, mg[None], fg[None], og[None], res, ow, gw, uw, dw)


def solution(mesh):
    S, TP, G = mesh.shape["sp"], mesh.shape["tp"], mesh.shape["grp"]

    def shards(q, k, v, lg, res, ow, mg, fg, og, gw, uw, dw):
        T, H = lg.shape
        hw = q.shape[1]
        D = res.shape[1]
        C, U = gw.shape
        R = T // TP
        pieces = max([p for p in range(1, MOST_PIECES + 1) if U % (128 * p) == 0], default=1)
        W = U // pieces
        pad = -H % 8
        lgt = jnp.pad(lg.astype(F32).T, ((0, pad), (0, 0)))
        if U % 128 == 0 and U // 128 >= S and C % (128 * TP) == 0 and T % (16 * TP) == 0 and (TP, G) == (4, 2):
            return gathered_call(S, TP, q, k, v, lg.T, H, mg, fg, og, res, ow, gw, uw, dw)
        vm = pl.BlockSpec(memory_space=pltpu.VMEM)
        hb = pl.BlockSpec(memory_space=pl.ANY)
        dma = pltpu.SemaphoreType.DMA
        return pl.pallas_call(
            functools.partial(kernel, S, TP, H, pieces),
            out_shape=jax.ShapeDtypeStruct((T, D), BF16),
            in_specs=[vm] * 7 + [hb] * 5,
            out_specs=hb,
            scratch_shapes=[
                pltpu.VMEM((S, T, hw), BF16),
                pltpu.VMEM((S, T, hw), BF16),
                pltpu.VMEM((S,) + lgt.shape, F32),
                pltpu.VMEM((H, T, hw // H), F32),
                pltpu.VMEM((H, T, hw // H), F32),
                pltpu.VMEM(ow.shape, BF16),
                pltpu.VMEM(gw.shape, BF16),
                pltpu.VMEM(uw.shape, BF16),
                pltpu.VMEM(dw.shape, BF16),
                pltpu.VMEM((R, D), BF16),
                pltpu.VMEM((TP, R, D), BF16),
                pltpu.VMEM((TP, R, D), BF16),
                pltpu.VMEM((R, D), F32),
                pltpu.VMEM((R, C), F32),
                pltpu.VMEM((S, R, C), BF16),
                pltpu.VMEM((TP, S, R, C), BF16),
                pltpu.VMEM((2, T, W), F32),
                pltpu.VMEM((pieces, S, 2, T, W), BF16),
                pltpu.VMEM((pieces, S + 1, 2, T, W), BF16),
                pltpu.VMEM((pieces, S, T, W), BF16),
                pltpu.VMEM((TP, S, R, C), BF16),
                pltpu.VMEM((TP, S, R, C), BF16),
                pltpu.VMEM((S, R, C), BF16),
                pltpu.VMEM((S, R, C), BF16),
                pltpu.VMEM((TP, R, D), BF16),
                dma((5,)),
                dma((S, 3)),
                dma((S, 3)),
                dma((TP,)),
                dma((TP,)),
                dma((S,)),
                dma((S,)),
                dma((TP, S)),
                dma((TP, S)),
                dma((pieces, S)),
                dma((pieces, S + 1)),
                dma((pieces, S)),
                dma((pieces, S)),
                dma((pieces, S)),
                dma((TP, S)),
                dma((TP, S)),
                dma((S,)),
                dma((S,)),
                dma((TP,)),
                dma((TP,)),
                dma((TP,)),
            ],
            compiler_params=pltpu.CompilerParams(
                collective_id=0, has_side_effects=True, vmem_limit_bytes=67043328 - 2**20
            ),
        )(q, k, v, lgt, mg[None], fg[None], og[None], res, ow, gw, uw, dw)

    placed = (
        P(("grp", "sp"), "tp"),
        P(("grp", "sp"), "tp"),
        P(("grp", "sp"), "tp"),
        P(("grp", "sp"), "tp"),
        P(("grp", "sp"), None),
        P("tp", None),
        P(),
        P(),
        P(),
        P("sp", "tp"),
        P("sp", "tp"),
        P("sp", "tp"),
    )
    return jax.shard_map(
        shards, mesh=mesh, in_specs=placed, out_specs=P(("grp", "sp"), None), check_vma=False
    )
```
